128 devices in a mesh: sp: 32 (over z, y, core), tp: 4 (over x).
Axes of the slice: x: 4, y: 4, z: 4, core: 2. Of those that a mesh axis runs over, the one named last changes fastest.
Arguments:
- query_narrow: bfloat16 [4096, 2048], P('sp', 'tp'), may hold values from -48 to 48
- key_narrow: bfloat16 [4096, 512], P('sp', 'tp'), may hold values from -15 to 15
- value_narrow: bfloat16 [4096, 512], P('sp', 'tp'), may hold values from -6 to 6
- gates_narrow: float32 [4096, 16], P(None, 'tp'), may hold values from -514 to 0, as said below
- query_broad: bfloat16 [4096, 2048], P('sp', 'tp'), may hold values from -48 to 48
- key_broad: bfloat16 [4096, 1024], P('sp', 'tp'), may hold values from -15 to 15
- value_broad: bfloat16 [4096, 1024], P('sp', 'tp'), may hold values from -6 to 6
- gates_broad: float32 [4096, 8], P(None, 'tp'), may hold values from -514 to 0, as said below
- project_narrow: bfloat16 [2048, 4096], P('tp'), may hold values from -0.1875 to 0.1875
- project_broad: bfloat16 [2048, 4096], P('tp'), may hold values from -0.1875 to 0.1875
- residual: bfloat16 [4096, 4096], P('sp'), may hold values from -6 to 6
- norm_gain: float32 [4096], replicated, may hold values from 0.1 to 1.9
- route_ids: int32 [4096, 4], P(('sp', 'tp')), may hold values from 0 to 127, all different within a row; in each aligned block of 32 rows (0 to 31, 32 to 63, ...) at most 2 rows name the same one
- route_weight: float32 [4096, 4], P(('sp', 'tp')), may hold values from 0.2 to 1.2
- expert_gate: bfloat16 [128, 4096, 256], P(('sp', 'tp')), may hold values from -0.09375 to 0.09375
- expert_up: bfloat16 [128, 4096, 256], P(('sp', 'tp')), may hold values from -0.09375 to 0.09375
- expert_down: bfloat16 [128, 256, 4096], P(('sp', 'tp')), may hold values from -0.375 to 0.375
- shared_gate: bfloat16 [4096, 1024], P(None, 'tp'), may hold values from -0.09375 to 0.09375
- shared_up: bfloat16 [4096, 1024], P(None, 'tp'), may hold values from -0.09375 to 0.09375
- shared_down: bfloat16 [1024, 4096], P('tp'), may hold values from -0.1875 to 0.1875
Outputs:
- layer_out: bfloat16 [4096, 4096], P(('sp', 'tp'))
The draws below stay inside these ranges and needn't reach their ends.
Inputs may be any that keep to these rules, and one draw needn't show every extreme that they name: `gates_narrow`: Non-increasing along positions in each head. `gates_broad`: Non-increasing along positions in each head. `route_ids`: each row names 4 different experts; among the rows of one device no expert is named by more than 2 rows, and that number is reached.
All inputs are finite; a program needn't handle non-finite values.
Results may differ from the reference program's by a relative error of at most 0.014.
Values may be sent and summed in bfloat16 or wider, within the bound.
No kernel may reach another device: no remote copies, remote signals or barrier semaphores. Data moves between devices by JAX's collectives and lax.ppermute only.
A program may use at most 128 MiB of HBM per device.

```python
import math
import jax
import jax.numpy as jnp
import numpy as np
from jax import lax

D = 4096
NARROW_HEADS = 16
NARROW_SIZE = 128
NARROW_KV = 4
BROAD_HEADS = 8
BROAD_SIZE = 256
BROAD_KV = 4
EXPERT_WIDTH = 256
SHARED_WIDTH = 1024
TOP = 4
TOK_DEV = 128
SEQUENCE_LENGTH = 4096
TOK_SUB = 32
EXPERTS = 128
CAP = 2
ATT_W = 4096
N_SP = 32
N_TP = 4


def plant_pairs(key, head_count, kv_heads, head_size, salt):
    base = jax.random.fold_in(key, salt)
    sequence_lanes = jax.random.split(base, 7)
    key_rows = 2.5 * jnp.clip(jax.random.normal(sequence_lanes[5], (SEQUENCE_LENGTH, kv_heads * head_size), jnp.float32), -6.0, 6.0)
    query_rows = jnp.clip(jax.random.normal(sequence_lanes[6], (SEQUENCE_LENGTH, head_count * head_size), jnp.float32), -6.0, 6.0)
    return (query_rows, key_rows)


def forget_cumulative(key, head_count, salt):
    base = jax.random.fold_in(key, salt)
    sequence_lanes = jax.random.split(base, 5)
    rough = jnp.exp(jax.random.uniform(sequence_lanes[0], (SEQUENCE_LENGTH, head_count), jnp.float32, math.log(0.5), math.log(2.0)))
    block_rate = jnp.exp(jax.random.uniform(sequence_lanes[1], (SEQUENCE_LENGTH // TOK_DEV, head_count), jnp.float32, math.log(0.5), math.log(2.0)))
    block_rate = jnp.repeat(block_rate, TOK_DEV, axis=0)
    order = jax.random.permutation(sequence_lanes[2], head_count)
    quick = order < head_count // 2
    rate = jnp.where(quick, 1.0 / 40.0, 0.4 / SEQUENCE_LENGTH)
    gate_logarithm = -rate[None, :] * rough * block_rate
    segment_start = jax.random.randint(sequence_lanes[3], (2, head_count), 0, SEQUENCE_LENGTH)
    segment_length = jax.random.uniform(sequence_lanes[4], (2, head_count), jnp.float32, math.log(0.5), math.log(0.8))
    place_indices = jnp.arange(SEQUENCE_LENGTH, dtype=jnp.int32)[:, None]
    for round_index in range(2):
        gate_logarithm = gate_logarithm + jnp.where(place_indices == segment_start[round_index][None, :], segment_length[round_index][None, :], 0.0)
    return jnp.cumsum(gate_logarithm, axis=0)


def draw_query_narrow(key, part):
    return plant_pairs(key, NARROW_HEADS, NARROW_KV, NARROW_SIZE, 101)[0].astype(jnp.bfloat16)


def draw_key_narrow(key, part):
    return plant_pairs(key, NARROW_HEADS, NARROW_KV, NARROW_SIZE, 101)[1].astype(jnp.bfloat16)


def draw_query_broad(key, part):
    return plant_pairs(key, BROAD_HEADS, BROAD_KV, BROAD_SIZE, 202)[0].astype(jnp.bfloat16)


def draw_key_broad(key, part):
    return plant_pairs(key, BROAD_HEADS, BROAD_KV, BROAD_SIZE, 202)[1].astype(jnp.bfloat16)


def draw_gates_narrow(key, part):
    return forget_cumulative(key, NARROW_HEADS, 303)


def draw_gates_broad(key, part):
    return forget_cumulative(key, BROAD_HEADS, 404)


def block_scale(own_key, shape, shards, smallest, top_value):
    def one(dim, blocks):
        steps = jax.random.uniform(jax.random.fold_in(jax.random.fold_in(own_key, 6), dim), (blocks,), jnp.float32, smallest / len(shards), top_value / len(shards))
        return jnp.repeat(jnp.exp(steps), shape[dim] // blocks).reshape((-1,) + (1,) * (len(shape) - dim - 1))

    gain = one(*shards[0])
    for cut in shards[1:]:
        gain = gain * one(*cut)
    return gain


def shared_out(stream_key, own, number, rows, count, top, reach, slope):
    ranking = jax.random.permutation(stream_key, count)
    packed, usual = shares(count, rows * top, reach, slope, True), shares(count, rows * top, reach, slope, False)
    places = jnp.arange(count)

    def named(tallies, turn):
        used = int((tallies > 0).sum())
        fixed = max(1, used // 4)
        moved = fixed + (places - fixed + turn * (used - fixed)) % max(1, count - fixed)
        return jnp.zeros((count,), jnp.int32).at[ranking[jnp.where(places < fixed, places, moved)]].set(jnp.asarray(tallies, jnp.int32))

    tallies = jnp.where(number % 4 == 0, named(packed, number // 4), named(usual, number - number // 4 - 1))
    mixed = jax.random.permutation(jax.random.fold_in(own, 3), count)
    donor, sink = mixed[0:count // 2 * 2:2], mixed[1:count // 2 * 2:2]
    slack = jnp.minimum(tallies[donor] - 1, reach - tallies[sink]) // 2
    slack = jnp.where((donor == ranking[0]) | (sink == ranking[0]) | (tallies[sink] == 0), 0, jnp.maximum(slack, 0))
    moved = jax.random.randint(jax.random.fold_in(own, 4), (count // 2,), 0, 1 << 20) % (slack + 1)
    tallies = tallies.at[donor].add(-moved).at[sink].add(moved)
    items = jnp.searchsorted(jnp.cumsum(tallies), jnp.arange(rows * top), side="right").astype(jnp.int32)
    grid = items.reshape(top, rows).T
    grid = grid[jax.random.permutation(jax.random.fold_in(own, 1), rows)]
    turn = jax.random.randint(jax.random.fold_in(own, 2), (rows, 1), 0, top)
    return jnp.take_along_axis(grid, (jnp.arange(top)[None, :] + turn) % top, axis=1)


def shares(amount, total, bound, skew, full):
    portions = [(1 << 20) // math.isqrt(rank ** skew) + 1 for rank in range(1, amount + 1)]
    largest = bound if full else min(bound, max(-(-total // amount), total * portions[0] // sum(portions)))
    least = 1 if total - largest >= amount - 1 else 0
    holding, surplus = [largest] + [least] * (amount - 1), total - largest - least * (amount - 1)
    while surplus > 0:
        movable = [i for i in range(1, amount) if holding[i] < largest] or [i for i in range(1, amount) if holding[i] < bound]
        pool, left = sum([portions[i] for i in movable]), surplus
        for i in movable:
            more = min(bound - holding[i], max(1, left * portions[i] // pool), surplus)
            holding[i] = holding[i] + more
            surplus = surplus - more
    return np.array(holding)


def centred(stream_key, shape, deviation, most, shards=(), held_as=jnp.bfloat16):
    gain = block_scale(stream_key, shape, shards, -0.22, 0.18) if shards else 1.0
    values = jax.random.normal(stream_key, shape, jnp.float32) * deviation * gain
    return jnp.minimum(jnp.maximum(values, -most), most).astype(held_as)


def setup_inputs(seed: int = 0) -> dict:
    key_list = jax.random.split(jax.random.key(seed), 21)
    query_narrow = draw_query_narrow(jax.random.fold_in(key_list[20], 71), 0)
    key_narrow = draw_key_narrow(jax.random.fold_in(key_list[20], 71), 0)
    value_narrow = centred(key_list[2], (SEQUENCE_LENGTH, NARROW_KV * NARROW_SIZE), 1.0, 6.0, ((0, 32), (1, 4)))
    gates_narrow = draw_gates_narrow(jax.random.fold_in(key_list[20], 71), 0)
    query_broad = draw_query_broad(jax.random.fold_in(key_list[20], 71), 0)
    key_broad = draw_key_broad(jax.random.fold_in(key_list[20], 71), 0)
    value_broad = centred(key_list[6], (SEQUENCE_LENGTH, BROAD_KV * BROAD_SIZE), 1.0, 6.0, ((0, 32), (1, 4)))
    gates_broad = draw_gates_broad(jax.random.fold_in(key_list[20], 71), 0)
    project_narrow = centred(key_list[8], (NARROW_HEADS * NARROW_SIZE, D), (ATT_W // 4) ** -0.5, 0.1875, ((0, 4),))
    project_broad = centred(key_list[9], (BROAD_HEADS * BROAD_SIZE, D), (ATT_W // 4) ** -0.5, 0.1875, ((0, 4),))
    residual = centred(key_list[10], (SEQUENCE_LENGTH, D), 1.0, 6.0, ((0, 32),))
    norm_gain = jnp.clip(1.0 + 0.18 * jax.random.normal(key_list[11], (D,), jnp.float32), 0.1, 1.9)
    route_ids_keys = jax.random.split(jax.random.fold_in(key_list[12], 1), SEQUENCE_LENGTH // TOK_SUB)
    route_ids_turns = jax.random.permutation(jax.random.fold_in(key_list[12], 3), SEQUENCE_LENGTH // TOK_SUB)
    route_ids = jax.vmap(lambda own, number: shared_out(jax.random.fold_in(key_list[12], 2), own, number, TOK_SUB, EXPERTS, TOP, CAP, 1))(route_ids_keys, route_ids_turns).reshape((SEQUENCE_LENGTH, TOP))
    route_weight = jnp.clip(jnp.exp(math.log(1.2) - 1.7917595 * jax.random.uniform(key_list[13], (SEQUENCE_LENGTH, TOP), jnp.float32) ** block_scale(key_list[13], (SEQUENCE_LENGTH, TOP), ((0, 128),), -0.2, 0.2)), 0.2, 1.2)
    expert_gate = centred(key_list[14], (EXPERTS, D, EXPERT_WIDTH), D ** -0.5, 0.09375, ((0, 128),))
    expert_up = centred(key_list[15], (EXPERTS, D, EXPERT_WIDTH), D ** -0.5, 0.09375, ((0, 128),))
    expert_down = centred(key_list[16], (EXPERTS, EXPERT_WIDTH, D), EXPERT_WIDTH ** -0.5, 0.375, ((0, 128),))
    shared_gate = centred(key_list[17], (D, SHARED_WIDTH), D ** -0.5, 0.09375, ((1, 4),))
    shared_up = centred(key_list[18], (D, SHARED_WIDTH), D ** -0.5, 0.09375, ((1, 4),))
    shared_down = centred(key_list[19], (SHARED_WIDTH, D), SHARED_WIDTH ** -0.5, 0.1875, ((0, 4),))
    return {"query_narrow": query_narrow, "key_narrow": key_narrow, "value_narrow": value_narrow, "gates_narrow": gates_narrow, "query_broad": query_broad, "key_broad": key_broad, "value_broad": value_broad, "gates_broad": gates_broad, "project_narrow": project_narrow, "project_broad": project_broad, "residual": residual, "norm_gain": norm_gain, "route_ids": route_ids, "route_weight": route_weight, "expert_gate": expert_gate, "expert_up": expert_up, "expert_down": expert_down, "shared_gate": shared_gate, "shared_up": shared_up, "shared_down": shared_down}


norm_epsilon = 1e-06

def group_attention(queries, key_rows, value_rows, gate_totals, head_count, kv_heads, head_size):
    group_size = head_count // kv_heads
    query_block = 256
    scaling = head_size ** (-0.5)
    outputs = []
    for first_query in range(0, SEQUENCE_LENGTH, query_block):
        last_key = first_query + query_block
        query_heads = queries[first_query:last_key].astype(jnp.float32).reshape(query_block, kv_heads, group_size, head_size)
        key_heads = key_rows[:last_key].astype(jnp.float32).reshape(last_key, kv_heads, head_size)
        value_heads = value_rows[:last_key].astype(jnp.float32).reshape(last_key, kv_heads, head_size)
        scores = jnp.einsum('tkgd,skd->kgts', query_heads, key_heads) * scaling
        query_gates = gate_totals[first_query:last_key].reshape(query_block, kv_heads, group_size).transpose(1, 2, 0)
        key_gates = gate_totals[:last_key].T.reshape(kv_heads, group_size, 1, last_key)
        scores = scores + query_gates[..., None] - key_gates
        allowed = jnp.arange(last_key)[None, :] <= (first_query + jnp.arange(query_block))[:, None]
        scores = jnp.where(allowed, scores, -jnp.inf)
        highest = lax.optimization_barrier(jnp.max(scores, axis=-1, keepdims=True))
        weights = jnp.exp(scores - highest)
        totals = lax.optimization_barrier(jnp.sum(weights, axis=-1))
        rounded = lax.optimization_barrier(weights.astype(jnp.bfloat16)).astype(jnp.float32)
        blended = jnp.einsum('kgts,skd->tkgd', rounded, value_heads) / totals.transpose(2, 0, 1)[..., None]
        outputs.append(blended.reshape(query_block, head_count * head_size).astype(jnp.bfloat16))
    return jnp.concatenate(outputs, axis=0)

def routed_experts(normed, route_ids, route_weight, expert_gate, expert_up, expert_down):
    top_count = route_ids.shape[1]
    flat_ids = route_ids.reshape(-1)
    flat_weight = lax.optimization_barrier(route_weight.reshape(-1).astype(jnp.bfloat16)).astype(jnp.float32)
    most_rows = N_SP * N_TP * CAP

    def one_expert(carried, expert):
        chosen = flat_ids == expert
        picked = jnp.nonzero(chosen, size=most_rows, fill_value=0)[0].astype(jnp.int32)
        live = jnp.arange(most_rows) < jnp.sum(chosen.astype(jnp.int32))
        token_index = picked // top_count
        rows = normed[token_index]
        gate_out = jnp.dot(rows, expert_gate[expert], preferred_element_type=jnp.float32)
        up_out = jnp.dot(rows, expert_up[expert], preferred_element_type=jnp.float32)
        hidden = (jax.nn.silu(gate_out) * up_out).astype(jnp.bfloat16)
        output = jnp.dot(hidden, expert_down[expert], preferred_element_type=jnp.float32)
        output = lax.optimization_barrier(output.astype(jnp.bfloat16)).astype(jnp.float32)
        contribution = jnp.where(live[:, None], flat_weight[picked][:, None] * output, jnp.zeros((), jnp.float32))
        return (carried.at[token_index].add(contribution), None)
    routed, ignored = lax.scan(one_expert, jnp.zeros((SEQUENCE_LENGTH, D), jnp.float32), jnp.arange(EXPERTS, dtype=jnp.int32))
    return routed

def reference(query_narrow, key_narrow, value_narrow, gates_narrow, query_broad, key_broad, value_broad, gates_broad, project_narrow, project_broad, residual, norm_gain, route_ids, route_weight, expert_gate, expert_up, expert_down, shared_gate, shared_up, shared_down):
    narrow = group_attention(query_narrow, key_narrow, value_narrow, gates_narrow, NARROW_HEADS, NARROW_KV, NARROW_SIZE)
    broad = group_attention(query_broad, key_broad, value_broad, gates_broad, BROAD_HEADS, BROAD_KV, BROAD_SIZE)
    width_narrow = NARROW_HEADS * NARROW_SIZE // N_TP
    width_broad = BROAD_HEADS * BROAD_SIZE // N_TP
    mixture = jnp.zeros((SEQUENCE_LENGTH, D), jnp.float32)
    for member in range(N_TP):
        low_n, high_n = (member * width_narrow, (member + 1) * width_narrow)
        low_b, high_b = (member * width_broad, (member + 1) * width_broad)
        portion = jnp.dot(narrow[:, low_n:high_n], project_narrow[low_n:high_n], preferred_element_type=jnp.float32)
        portion = portion + jnp.dot(broad[:, low_b:high_b], project_broad[low_b:high_b], preferred_element_type=jnp.float32)
        mixture = mixture + lax.optimization_barrier(portion.astype(jnp.bfloat16)).astype(jnp.float32)
    stream = residual.astype(jnp.float32) + mixture
    normed = (stream * lax.rsqrt(lax.optimization_barrier(jnp.mean(stream * stream, axis=-1, keepdims=True)) + norm_epsilon) * norm_gain).astype(jnp.bfloat16)
    shared_hidden = (jax.nn.silu(jnp.dot(normed, shared_gate, preferred_element_type=jnp.float32)) * jnp.dot(normed, shared_up, preferred_element_type=jnp.float32)).astype(jnp.bfloat16)
    width_shared = SHARED_WIDTH // N_TP
    shared = jnp.zeros((SEQUENCE_LENGTH, D), jnp.float32)
    for member in range(N_TP):
        low_s, high_s = (member * width_shared, (member + 1) * width_shared)
        portion = jnp.dot(shared_hidden[:, low_s:high_s], shared_down[low_s:high_s], preferred_element_type=jnp.float32)
        shared = shared + lax.optimization_barrier(portion.astype(jnp.bfloat16)).astype(jnp.float32)
    routed = routed_experts(normed, route_ids, route_weight, expert_gate, expert_up, expert_down)
    return (stream + shared + routed).astype(jnp.bfloat16)
```

```python
import functools

import jax
import jax.numpy as jnp
from jax import lax
from jax.experimental import pallas as pl
from jax.experimental.pallas import tpu as pltpu
from jax.sharding import Mesh
from jax.sharding import PartitionSpec as P

SP = ("z", "y", "c")
NARROW_SIZE = 128
BROAD_SIZE = 256
LOG2E = 1.4426950408889634
MASKED = -1e30
EPSILON = 1e-06
ORDER = (0, 1, 3, 2)
BF = jnp.bfloat16
F32 = jnp.float32


def shift(x, axis, k):
    return lax.ppermute(x, axis, [(i, (i + k) % 4) for i in range(4)])


def swap_core(x):
    return lax.ppermute(x, "c", [(0, 1), (1, 0)])


def direct_ring(x, axis):
    return jnp.stack([x] + [shift(x, axis, k) for k in ORDER[1:]])


def halved_ring(g, axis):
    back = shift(g, axis, 1)
    ahead = shift(g, axis, 3)
    far_low = shift(back[:2], axis, 1)
    far_high = shift(ahead[2:], axis, 3)
    return back, ahead, far_low, far_high


def scatter_sum(partial):
    t = lax.axis_index("tp")
    rows, width = partial.shape[0] // 4, partial.shape[1] // 2

    def part(k, half):
        return lax.dynamic_slice(partial, (((t + k) % 4) * rows, half * width), (rows, width))

    far_a = shift(part(2, 0), "tp", 1)
    far_b = shift(part(2, 1), "tp", 3)
    near_b = shift(part(1, 1), "tp", 1)
    near_a = shift(part(3, 0), "tp", 3)
    sum_a = shift((part(1, 0).astype(F32) + far_a.astype(F32)).astype(BF), "tp", 1)
    sum_b = shift((part(3, 1).astype(F32) + far_b.astype(F32)).astype(BF), "tp", 3)
    low = part(0, 0).astype(F32) + sum_a.astype(F32) + near_a.astype(F32)
    high = part(0, 1).astype(F32) + sum_b.astype(F32) + near_b.astype(F32)
    return jnp.concatenate([low, high], axis=1)


def gather_rows(own):
    t = lax.axis_index("tp")
    rows, width = own.shape
    back = shift(own, "tp", 1)
    ahead = shift(own, "tp", 3)
    far_a = shift(back[:, : width // 2], "tp", 1)
    far_b = shift(ahead[:, width // 2 :], "tp", 3)
    far = jnp.concatenate([far_a, far_b], axis=1)
    out = jnp.zeros((4 * rows, width), own.dtype)
    for k, piece in ((0, own), (1, back), (2, far), (3, ahead)):
        out = lax.dynamic_update_slice(out, piece, (((t - k) % 4) * rows, 0))
    return out


def attend_kernel(counts, first, last, *refs):
    at = 0

    def take(n):
        nonlocal at
        at += n
        return refs[at - n : at]

    q_own, q_other, core = take(3)
    tiles = []
    for n, own_block in counts:
        tiles.append((take(n), take(1)[0], own_block))
    if not first:
        m_in, l_in, an_in, ab_in = take(4)
    if last:
        own_out, send_out = take(2)
    else:
        m_out, l_out, an_out, ab_out = take(4)

    def keys(ref, lo, hi):
        value = ref[..., lo:hi]
        return value.reshape(-1, hi - lo)

    results = {}
    for group, size, heads, lo in (("n", NARROW_SIZE, 4, 0), ("b", BROAD_SIZE, 2, 256)):
        scale = size**-0.5 * LOG2E
        base = 0 if group == "n" else 4
        row_base = 0 if group == "n" else 1024
        loaded = []
        for arrays, bias, own_block in tiles:
            k = jnp.concatenate([keys(r, lo, lo + size) for r in arrays], axis=0)
            v = jnp.concatenate([keys(r, lo + size, lo + 2 * size) for r in arrays], axis=0)
            loaded.append((k, v, bias, own_block))
        for side, q_ref in ((0, q_own), (1, q_other)):
            for h0 in range(0, heads, 2):
                col = (0 if group == "n" else 512) + h0 * size
                q = jnp.concatenate([q_ref[:, col + i * size : col + (i + 1) * size] for i in range(2)], axis=0)
                rows = row_base + side * heads * 128 + h0 * 128
                arow = rows - row_base
                scores = []
                for k, v, bias, own_block in loaded:
                    s = lax.dot_general(q, k, (((1,), (1,)), ((), ())), preferred_element_type=F32) * scale
                    n = k.shape[0]
                    b = bias[base + h0 : base + h0 + 2, :]
                    s = (s.reshape(2, 128, n) + b[:, None, :]).reshape(256, n)
                    if own_block:
                        qi = lax.broadcasted_iota(jnp.int32, (256, n), 0) % 128
                        ki = lax.broadcasted_iota(jnp.int32, (256, n), 1)
                        offset = 0 if side == 0 else 128 * (1 - 2 * core[0])
                        s = jnp.where(ki <= qi + offset, s, MASKED)
                    scores.append(s)
                m = functools.reduce(jnp.maximum, [jnp.max(s, axis=1, keepdims=True) for s in scores])
                if not first:
                    m_old = m_in[pl.ds(rows, 256), :][:, :1]
                    m = jnp.maximum(m, m_old)
                l = jnp.zeros((256, 1), F32)
                acc = jnp.zeros((256, size), F32)
                for s, (k, v, bias, own_block) in zip(scores, loaded):
                    p = jnp.exp2(s - m)
                    l = l + jnp.sum(p, axis=1, keepdims=True)
                    acc = acc + jnp.dot(p.astype(BF), v, preferred_element_type=F32)
                acc_in, acc_out = (None, None)
                if not first:
                    a_in = an_in if group == "n" else ab_in
                    factor = jnp.exp2(m_old - m)
                    l = l + l_in[pl.ds(rows, 256), :][:, :1] * factor
                    acc = acc + a_in[pl.ds(arow, 256), :] * factor
                if last:
                    out = own_out if side == 0 else send_out
                    o = acc / l
                    lse = m + jnp.log2(l)
                    for i in range(2):
                        out[:, col + i * size : col + (i + 1) * size] = o[i * 128 : (i + 1) * 128]
                        results[(side, base + h0 + i)] = lse[i * 128 : (i + 1) * 128]
                else:
                    a_out = an_out if group == "n" else ab_out
                    m_out[pl.ds(rows, 256), :] = jnp.broadcast_to(m, (256, 128))
                    l_out[pl.ds(rows, 256), :] = jnp.broadcast_to(l, (256, 128))
                    a_out[pl.ds(arow, 256), :] = acc
    if last:
        lane = lax.broadcasted_iota(jnp.int32, (128, 128), 1)
        for side, out in ((0, own_out), (1, send_out)):
            stats = jnp.zeros((128, 128), F32)
            for h in range(6):
                stats = jnp.where(lane == h, results[(side, h)], stats)
            out[:, 1024:1152] = stats


def attend(q_own, q_other, core, tiles, state, last):
    counts = tuple((len(arrays), own_block) for arrays, _, own_block in tiles)
    operands = [q_own, q_other, core]
    n_keys = 0
    for arrays, bias, _ in tiles:
        operands += list(arrays) + [bias]
        n_keys += bias.shape[1]
    vmem = pl.BlockSpec(memory_space=pltpu.VMEM)
    specs = [vmem] * len(operands)
    specs[2] = pl.BlockSpec(memory_space=pltpu.SMEM)
    if state is not None:
        operands += list(state)
        specs += [vmem] * 4
    if last:
        shapes = [jax.ShapeDtypeStruct((128, 1152), F32)] * 2
    else:
        shapes = [
            jax.ShapeDtypeStruct((1536, 128), F32),
            jax.ShapeDtypeStruct((1536, 128), F32),
            jax.ShapeDtypeStruct((1024, 128), F32),
            jax.ShapeDtypeStruct((512, 256), F32),
        ]
    return pl.pallas_call(
        functools.partial(attend_kernel, counts, state is None, last),
        out_shape=shapes,
        in_specs=specs,
        out_specs=[vmem] * len(shapes),
        compiler_params=pltpu.CompilerParams(vmem_limit_bytes=40 * 1024 * 1024),
        cost_estimate=pl.CostEstimate(
            flops=4 * n_keys * 256 * 1024, transcendentals=n_keys * 1536, bytes_accessed=4 * 1024 * 1024
        ),
    )(*operands)


def key_biases(gates_narrow, gates_broad, z, y, c):
    gates = jnp.concatenate([gates_narrow, gates_broad], axis=1) * (-LOG2E)
    gates = gates.reshape(4, 4, 2, 128, 6)
    gates = lax.dynamic_index_in_dim(gates, c, 2, keepdims=False).transpose(0, 1, 3, 2)
    planes = []
    for i in ORDER:
        zs = (z - i) % 4
        plane = lax.dynamic_index_in_dim(gates, zs, 0, keepdims=False)
        blocks = []
        for k in ORDER:
            ys = (y - k) % 4
            block = lax.dynamic_index_in_dim(plane, ys, 0, keepdims=False)
            blocks.append(jnp.where(zs * 4 + ys > z * 4 + y, MASKED, block))
        planes.append(jnp.stack(blocks))
    return jnp.stack(planes)


def flat_bias(*pieces):
    rows = [p.reshape(-1, 6, 64) for p in pieces]
    return jnp.concatenate(rows, axis=0).transpose(1, 0, 2).reshape(6, -1)


def local(
    query_narrow,
    key_narrow,
    value_narrow,
    gates_narrow,
    query_broad,
    key_broad,
    value_broad,
    gates_broad,
    project_narrow,
    project_broad,
    residual,
    norm_gain,
    route_ids,
    route_weight,
    expert_gate,
    expert_up,
    expert_down,
    shared_gate,
    shared_up,
    shared_down,
):
    z, y, c, t = (lax.axis_index(n) for n in ("z", "y", "c", "tp"))

    own_kv = jnp.concatenate([key_narrow, value_narrow, key_broad, value_broad], axis=1)
    plane_a = direct_ring(own_kv[:64], "y")
    plane_b = direct_ring(own_kv[64:], "z")
    q_own = jnp.concatenate([query_narrow, query_broad], axis=1)
    q_other = swap_core(q_own)
    a_back, a_ahead, a_far_low, a_far_high = halved_ring(plane_a, "z")
    b_back, b_ahead, b_far_low, b_far_high = halved_ring(plane_b, "y")

    bias = key_biases(gates_narrow, gates_broad, z, y, c)
    bias_a, bias_b = bias[..., :64], bias[..., 64:].swapaxes(0, 1)
    core = c.astype(jnp.int32).reshape(1)
    own_bias = bias[0, 0]

    state = attend(
        q_own,
        q_other,
        core,
        [
            ((own_kv,), own_bias, True),
            ((plane_a[1:], plane_b[1:]), flat_bias(bias_a[0, 1:], bias_b[0, 1:]), False),
        ],
        None,
        False,
    )
    state = attend(
        q_own,
        q_other,
        core,
        [
            ((a_back, a_ahead), flat_bias(bias_a[1], bias_a[2]), False),
            ((b_back, b_ahead), flat_bias(bias_b[1], bias_b[2]), False),
        ],
        state,
        False,
    )
    own_part, send_part = attend(
        q_own,
        q_other,
        core,
        [
            (
                (a_far_low, a_far_high, b_far_low, b_far_high),
                flat_bias(bias_a[3], bias_b[3]),
                False,
            ),
        ],
        state,
        True,
    )
    other_part = swap_core(send_part)
    lse_own, lse_other = own_part[:, 1024:1030], other_part[:, 1024:1030]
    top = jnp.maximum(lse_own, lse_other)
    w_own, w_other = jnp.exp2(lse_own - top), jnp.exp2(lse_other - top)
    total = w_own + w_other
    w_own, w_other = w_own / total, w_other / total

    def spread(w):
        n = jnp.broadcast_to(w[:, :4, None], (128, 4, 128)).reshape(128, 512)
        b = jnp.broadcast_to(w[:, 4:, None], (128, 2, 256)).reshape(128, 512)
        return jnp.concatenate([n, b], axis=1)

    attn = (own_part[:, :1024] * spread(w_own) + other_part[:, :1024] * spread(w_other)).astype(BF)
    head_part = jnp.dot(attn[:, :512], project_narrow, preferred_element_type=F32)
    head_part = head_part + jnp.dot(attn[:, 512:], project_broad, preferred_element_type=F32)
    mixture = scatter_sum(head_part.astype(BF))

    line_ids = lax.all_gather(route_ids, "tp", axis=0, tiled=True)
    line_weight = lax.all_gather(route_weight.astype(BF).astype(F32), "tp", axis=0, tiled=True)
    tokens = line_ids.shape[0]
    experts = jnp.arange(32, dtype=jnp.int32) * 4 + t
    hit = line_ids[:, :, None] == experts[None, None, :]
    named = jnp.any(hit, axis=1)
    weight_of = jnp.sum(jnp.where(hit, line_weight[:, :, None], 0.0), axis=1)
    before = jnp.tril(jnp.ones((tokens, tokens), BF), -1)
    slot_of = jnp.dot(before, named.astype(BF), preferred_element_type=F32).astype(jnp.int32)
    taken = named[:, :, None] & (slot_of[:, :, None] == jnp.arange(8, dtype=jnp.int32))
    taken = taken.reshape(tokens, 256)
    dispatch = taken.astype(BF).T
    combiner = jnp.where(taken, jnp.repeat(weight_of, 8, axis=1), 0.0).astype(BF)

    sub_rows = route_ids.shape[0]
    own_rows = lax.dynamic_slice_in_dim(residual, t * sub_rows, sub_rows, 0)
    stream = own_rows.astype(F32) + mixture
    normed = stream * lax.rsqrt(jnp.mean(stream * stream, axis=-1, keepdims=True) + EPSILON) * norm_gain
    line_normed = gather_rows(normed.astype(BF))

    outbound = jnp.dot(dispatch, line_normed, preferred_element_type=F32).astype(BF)
    inbound = lax.all_to_all(outbound.reshape(32, 8, -1), SP, 0, 0, tiled=True).reshape(256, -1)

    gate = jnp.dot(line_normed, shared_gate, preferred_element_type=F32)
    up = jnp.dot(line_normed, shared_up, preferred_element_type=F32)
    shared_hidden = (jax.nn.silu(gate) * up).astype(BF)
    shared = jnp.dot(shared_hidden, shared_down, preferred_element_type=F32)

    gate = jnp.dot(inbound, expert_gate[0], preferred_element_type=F32)
    up = jnp.dot(inbound, expert_up[0], preferred_element_type=F32)
    hidden = (jax.nn.silu(gate) * up).astype(BF)
    result = jnp.dot(hidden, expert_down[0], preferred_element_type=F32).astype(BF)
    returned = lax.all_to_all(result.reshape(32, 8, -1), SP, 0, 0, tiled=True).reshape(256, -1)
    routed = jnp.dot(combiner, returned, preferred_element_type=F32)
    return (stream + scatter_sum((routed + shared).astype(BF))).astype(BF)


def solution(mesh):
    mesh = Mesh(mesh.devices.reshape(4, 4, 2, 4), ("z", "y", "c", "tp"))
    every = SP + ("tp",)
    placed = (
        P(SP, "tp"),
        P(SP, "tp"),
        P(SP, "tp"),
        P(None, "tp"),
        P(SP, "tp"),
        P(SP, "tp"),
        P(SP, "tp"),
        P(None, "tp"),
        P("tp", None),
        P("tp", None),
        P(SP, None),
        P(),
        P(every, None),
        P(every, None),
        P(every, None, None),
        P(every, None, None),
        P(every, None, None),
        P(None, "tp"),
        P(None, "tp"),
        P("tp", None),
    )
    return jax.shard_map(local, mesh=mesh, in_specs=placed, out_specs=P(every, None), check_vma=False)
```

```python
import functools

import jax
import jax.numpy as jnp
from jax import lax
from jax.experimental import pallas as pl
from jax.experimental.pallas import tpu as pltpu
from jax.sharding import Mesh
from jax.sharding import PartitionSpec as P

SP = ("z", "y", "c")
NARROW_SIZE = 128
BROAD_SIZE = 256
LOG2E = 1.4426950408889634
MASKED = -1e30
EPSILON = 1e-06
ORDER = (0, 1, 3, 2)
VMEM = pl.BlockSpec(memory_space=pltpu.VMEM)
SMEM = pl.BlockSpec(memory_space=pltpu.SMEM)
BF = jnp.bfloat16
F32 = jnp.float32


def shift(x, axis, k):
    return lax.ppermute(x, axis, [(i, (i + k) % 4) for i in range(4)])


def swap_core(x):
    return lax.ppermute(x, "c", [(0, 1), (1, 0)])


def call(kernel, operands, shapes, smem=(), scratch=(), mib=32, flops=0):
    return pl.pallas_call(
        kernel,
        out_shape=shapes,
        in_specs=[SMEM if i in smem else VMEM for i in range(len(operands))],
        out_specs=[VMEM] * len(shapes),
        scratch_shapes=list(scratch),
        compiler_params=pltpu.CompilerParams(vmem_limit_bytes=mib * 1024 * 1024),
        cost_estimate=pl.CostEstimate(flops=flops, transcendentals=0, bytes_accessed=2 * 1024 * 1024),
    )(*operands)


def shaped(shape, dtype):
    return jax.ShapeDtypeStruct(shape, dtype)


def pack_kernel(kn, vn, kb, vb, qn, qb, a, b, q):
    for at, ref in ((0, kn), (128, vn), (256, kb), (512, vb)):
        a[:, at : at + ref.shape[1]] = ref[:64]
        b[:, at : at + ref.shape[1]] = ref[64:]
    q[:, :512] = qn[...]
    q[:, 512:] = qb[...]


def stack_kernel(a, b, c, d, out):
    for i, ref in enumerate((a, b, c, d)):
        out[i] = ref[...]


def bias_kernel(place, gates, own, first, second, third):
    z, y = place[0], place[1]
    here = z * 4 + y
    own[...] = gates[here]

    def put(out, at, back_z, back_y, half):
        chip = ((z + 4 - back_z) % 4) * 4 + (y + 4 - back_y) % 4
        piece = gates[chip][:, half * 64 : half * 64 + 64]
        out[:, at : at + 64] = jnp.where(chip > here, MASKED, piece)

    for i in range(1, 4):
        put(first, (i - 1) * 64, 0, ORDER[i], 0)
        put(first, 192 + (i - 1) * 64, ORDER[i], 0, 1)
    for i in range(4):
        put(second, i * 64, 1, ORDER[i], 0)
        put(second, 256 + i * 64, 3, ORDER[i], 0)
        put(second, 512 + i * 64, ORDER[i], 1, 1)
        put(second, 768 + i * 64, ORDER[i], 3, 1)
        put(third, i * 64, 2, ORDER[i], 0)
        put(third, 256 + i * 64, ORDER[i], 2, 1)


def project_kernel(place, own, other, narrow, broad, *refs):
    outs, total, attn = refs[:4], refs[4], refs[5]
    a, b = own[:, 1024:], other[:, 1024:]
    top = jnp.maximum(a, b)
    wa, wb = jnp.exp2(a - top), jnp.exp2(b - top)
    joined = wa + wb
    wa, wb = wa / joined, wb / joined
    for h in range(6):
        lo, size = (h * 128, 128) if h < 4 else (512 + (h - 4) * 256, 256)
        value = own[:, lo : lo + size] * wa[:, h : h + 1] + other[:, lo : lo + size] * wb[:, h : h + 1]
        attn[:, lo : lo + size] = value.astype(BF)
    for at in range(0, 4096, 1024):
        part = jnp.dot(attn[:, :512], narrow[:, at : at + 1024], preferred_element_type=F32)
        total[:, at : at + 1024] = part + jnp.dot(attn[:, 512:], broad[:, at : at + 1024], preferred_element_type=F32)
    for k in range(4):
        outs[k][...] = total[pl.ds(((place[0] + k) % 4) * 32, 32), :].astype(BF)


def dispatch_kernel(p0, p1, p2, p3, residual, gain, target, stream_out, normed_out, out):
    mixture = p0[...].astype(F32) + p1[...].astype(F32) + p2[...].astype(F32) + p3[...].astype(F32)
    stream = residual[...].astype(F32) + mixture
    stream_out[...] = stream
    scale = lax.rsqrt(jnp.mean(stream * stream, axis=1, keepdims=True) + EPSILON)
    normed = (stream * scale * gain[...]).astype(BF)
    normed_out[...] = normed
    cut = jnp.concatenate([normed[:, g * 1024 : (g + 1) * 1024] for g in range(4)], axis=0)
    row = lax.broadcasted_iota(jnp.int32, (256, 128), 0)
    for at in range(0, 1024, 256):
        pick = row + at == target[0:1, :]
        for k in range(1, 4):
            pick = pick | (row + at == target[k : k + 1, :])
        out[at : at + 256, :] = jnp.dot(pick.astype(F32).astype(BF), cut, preferred_element_type=F32).astype(BF)


def silu(v):
    return v / (1.0 + jnp.exp(-v))


def shared_kernel(n0, n1, n2, n3, gate, up, down, o0, o1, o2, o3):
    x = jnp.concatenate([n0[...], n1[...], n2[...], n3[...]], axis=0)
    g = jnp.dot(x, gate[...], preferred_element_type=F32)
    u = jnp.dot(x, up[...], preferred_element_type=F32)
    hidden = (silu(g) * u).astype(BF)
    for at in range(0, 4096, 1024):
        part = jnp.dot(hidden, down[:, at : at + 1024], preferred_element_type=F32).astype(BF)
        for k, out in enumerate((o0, o1, o2, o3)):
            out[:, at : at + 1024] = part[k * 32 : (k + 1) * 32]


def expert_kernel(inbound, gate, up, down, out, x):
    i = lax.broadcasted_iota(jnp.int32, (256, 256), 0)
    j = lax.broadcasted_iota(jnp.int32, (256, 256), 1)
    order = (j == ((i % 64) // 2) * 8 + (i % 2) * 4 + i // 64).astype(F32).astype(BF)
    back = (i == ((j % 64) // 2) * 8 + (j % 2) * 4 + j // 64).astype(F32).astype(BF)
    for b in range(4):
        rows = jnp.dot(order, inbound[b * 256 : (b + 1) * 256, :], preferred_element_type=F32).astype(BF)
        for g in range(4):
            x[b * 64 : (b + 1) * 64, g * 1024 : (g + 1) * 1024] = rows[g * 64 : (g + 1) * 64]
    gated = jnp.dot(x[...], gate[0], preferred_element_type=F32)
    upped = jnp.dot(x[...], up[0], preferred_element_type=F32)
    hidden = (silu(gated) * upped).astype(BF)
    for g in range(4):
        part = jnp.dot(hidden, down[0, :, g * 1024 : (g + 1) * 1024], preferred_element_type=F32)
        x[:, g * 1024 : (g + 1) * 1024] = part.astype(BF)
    for b in range(4):
        rows = jnp.concatenate([x[b * 64 : (b + 1) * 64, g * 1024 : (g + 1) * 1024] for g in range(4)], axis=0)
        out[b * 256 : (b + 1) * 256, :] = jnp.dot(back, rows, preferred_element_type=F32).astype(BF)


def combine_kernel(returned, target, weight, stream, s0, s1, s2, s3, out):
    column = lax.broadcasted_iota(jnp.int32, (128, 1024), 1)
    mix = jnp.zeros((128, 1024), F32)
    for k in range(4):
        mix = mix + jnp.where(column == target[:, k : k + 1], weight[:, k : k + 1], 0.0)
    routed = jnp.dot(mix.astype(BF), returned[...], preferred_element_type=F32)
    for g in range(4):
        lo, hi = g * 1024, (g + 1) * 1024
        total = stream[:, lo:hi] + routed[g * 32 : (g + 1) * 32]
        for s in (s0, s1, s2, s3):
            total = total + s[:, lo:hi].astype(F32)
        out[:, lo:hi] = total.astype(BF)


def attend_kernel(counts, first, last, *refs):
    at = 0

    def take(n):
        nonlocal at
        at += n
        return refs[at - n : at]

    q_own, q_other, core = take(3)
    tiles, planes = [], []
    for n, own_block in counts:
        tiles.append((take(n), take(1)[0], own_block))
        if first and not own_block:
            planes += tiles[-1][0]
    if not first:
        m_in, l_in, an_in, ab_in = take(4)
    if last:
        own_out, send_out = take(2)
    else:
        m_out, l_out, an_out, ab_out = take(4)

    def keys(ref, lo, hi):
        value = ref[1:, :, lo:hi] if any(ref is p for p in planes) else ref[..., lo:hi]
        return value.reshape(-1, hi - lo)

    results = {}
    for group, size, heads, lo in (("n", NARROW_SIZE, 4, 0), ("b", BROAD_SIZE, 2, 256)):
        scale = size**-0.5 * LOG2E
        base = 0 if group == "n" else 4
        row_base = 0 if group == "n" else 1024
        loaded = []
        for arrays, bias, own_block in tiles:
            k = jnp.concatenate([keys(r, lo, lo + size) for r in arrays], axis=0)
            v = jnp.concatenate([keys(r, lo + size, lo + 2 * size) for r in arrays], axis=0)
            loaded.append((k, v, bias, own_block))
        for side, q_ref in ((0, q_own), (1, q_other)):
            for h0 in range(0, heads, 2):
                col = (0 if group == "n" else 512) + h0 * size
                q = jnp.concatenate([q_ref[:, col + i * size : col + (i + 1) * size] for i in range(2)], axis=0)
                rows = row_base + side * heads * 128 + h0 * 128
                arow = rows - row_base
                scores = []
                for k, v, bias, own_block in loaded:
                    s = lax.dot_general(q, k, (((1,), (1,)), ((), ())), preferred_element_type=F32) * scale
                    n = k.shape[0]
                    b = bias[base + h0 : base + h0 + 2, :]
                    s = (s.reshape(2, 128, n) + b[:, None, :]).reshape(256, n)
                    if own_block:
                        qi = lax.broadcasted_iota(jnp.int32, (256, n), 0) % 128
                        ki = lax.broadcasted_iota(jnp.int32, (256, n), 1)
                        offset = 0 if side == 0 else 128 * (1 - 2 * core[0])
                        s = jnp.where(ki <= qi + offset, s, MASKED)
                    scores.append(s)
                m = functools.reduce(jnp.maximum, [jnp.max(s, axis=1, keepdims=True) for s in scores])
                if not first:
                    m_old = m_in[pl.ds(rows, 256), :][:, :1]
                    m = jnp.maximum(m, m_old)
                l = jnp.zeros((256, 1), F32)
                acc = jnp.zeros((256, size), F32)
                for s, (k, v, bias, own_block) in zip(scores, loaded):
                    p = jnp.exp2(s - m)
                    l = l + jnp.sum(p, axis=1, keepdims=True)
                    acc = acc + jnp.dot(p.astype(BF), v, preferred_element_type=F32)
                acc_in, acc_out = (None, None)
                if not first:
                    a_in = an_in if group == "n" else ab_in
                    factor = jnp.exp2(m_old - m)
                    l = l + l_in[pl.ds(rows, 256), :][:, :1] * factor
                    acc = acc + a_in[pl.ds(arow, 256), :] * factor
                if last:
                    out = own_out if side == 0 else send_out
                    o = acc / l
                    lse = m + jnp.log2(l)
                    for i in range(2):
                        out[:, col + i * size : col + (i + 1) * size] = o[i * 128 : (i + 1) * 128]
                        results[(side, base + h0 + i)] = lse[i * 128 : (i + 1) * 128]
                else:
                    a_out = an_out if group == "n" else ab_out
                    m_out[pl.ds(rows, 256), :] = jnp.broadcast_to(m, (256, 128))
                    l_out[pl.ds(rows, 256), :] = jnp.broadcast_to(l, (256, 128))
                    a_out[pl.ds(arow, 256), :] = acc
    if last:
        lane = lax.broadcasted_iota(jnp.int32, (128, 128), 1)
        for side, out in ((0, own_out), (1, send_out)):
            stats = jnp.zeros((128, 128), F32)
            for h in range(6):
                stats = jnp.where(lane == h, results[(side, h)], stats)
            out[:, 1024:1152] = stats


def attend(q_own, q_other, core, tiles, state, last):
    counts = tuple((len(arrays), own_block) for arrays, _, own_block in tiles)
    operands = [q_own, q_other, core]
    n_keys = 0
    for arrays, bias, _ in tiles:
        operands += list(arrays) + [bias]
        n_keys += bias.shape[1]
    specs = [VMEM] * len(operands)
    specs[2] = SMEM
    if state is not None:
        operands += list(state)
        specs += [VMEM] * 4
    if last:
        shapes = [jax.ShapeDtypeStruct((128, 1152), F32)] * 2
    else:
        shapes = [
            jax.ShapeDtypeStruct((1536, 128), F32),
            jax.ShapeDtypeStruct((1536, 128), F32),
            jax.ShapeDtypeStruct((1024, 128), F32),
            jax.ShapeDtypeStruct((512, 256), F32),
        ]
    return pl.pallas_call(
        functools.partial(attend_kernel, counts, state is None, last),
        out_shape=shapes,
        in_specs=specs,
        out_specs=[VMEM] * len(shapes),
        compiler_params=pltpu.CompilerParams(vmem_limit_bytes=24 * 1024 * 1024),
        cost_estimate=pl.CostEstimate(
            flops=4 * n_keys * 256 * 1024, transcendentals=n_keys * 1536, bytes_accessed=4 * 1024 * 1024
        ),
    )(*operands)


def local(
    query_narrow,
    key_narrow,
    value_narrow,
    gates_narrow,
    query_broad,
    key_broad,
    value_broad,
    gates_broad,
    project_narrow,
    project_broad,
    residual,
    norm_gain,
    route_ids,
    route_weight,
    expert_gate,
    expert_up,
    expert_down,
    shared_gate,
    shared_up,
    shared_down,
):
    z, y, c, t = (lax.axis_index(n).astype(jnp.int32) for n in ("z", "y", "c", "tp"))

    own_a, own_b, q_own = call(
        pack_kernel,
        (key_narrow, value_narrow, key_broad, value_broad, query_narrow, query_broad),
        [shaped((64, 768), BF)] * 2 + [shaped((128, 1024), BF)],
    )
    first_a = [shift(own_a, "y", k) for k in ORDER[1:]]
    first_b = [shift(own_b, "z", k) for k in ORDER[1:]]
    q_other = swap_core(q_own)
    (plane_a,) = call(stack_kernel, [own_a] + first_a, [shaped((4, 64, 768), BF)])
    (plane_b,) = call(stack_kernel, [own_b] + first_b, [shaped((4, 64, 768), BF)])
    a_back, b_back, a_ahead, b_ahead, a_far, b_far = (
        shift(plane, axis, k) for k in ORDER[1:] for plane, axis in ((plane_a, "z"), (plane_b, "y"))
    )

    gates = jnp.concatenate([gates_narrow, gates_broad], axis=1) * (-LOG2E)
    gates = lax.dynamic_index_in_dim(gates.reshape(16, 2, 128, 6), c, 1, keepdims=False)
    gates = jnp.pad(gates.transpose(0, 2, 1), ((0, 0), (0, 2), (0, 0)))
    own_bias, bias_1, bias_2, bias_3 = call(
        bias_kernel,
        (jnp.stack([z, y]), gates),
        [shaped((8, n), F32) for n in (128, 384, 1024, 512)],
        smem=(0,),
    )
    core = c.reshape(1)
    state = attend(
        q_own,
        q_other,
        core,
        [((own_a, own_b), own_bias, True), ((plane_a, plane_b), bias_1, False)],
        None,
        False,
    )
    state = attend(q_own, q_other, core, [((a_back, a_ahead, b_back, b_ahead), bias_2, False)], state, False)
    own_part, send_part = attend(q_own, q_other, core, [((a_far, b_far), bias_3, False)], state, True)
    other_part = swap_core(send_part)

    p0, p1, p2, p3 = call(
        project_kernel,
        (t.reshape(1), own_part, other_part, project_narrow, project_broad),
        [shaped((32, 4096), BF)] * 4,
        smem=(0,),
        scratch=[pltpu.VMEM((128, 4096), F32), pltpu.VMEM((128, 1024), BF)],
        flops=2 * 128 * 1024 * 4096,
    )
    p1, p2, p3 = shift(p1, "tp", 1), shift(p2, "tp", 2), shift(p3, "tp", 3)

    flat = route_ids.reshape(-1)
    earlier = jnp.arange(128)[:, None] // 4 > jnp.arange(128)[None, :] // 4
    slot = jnp.sum((earlier & (flat[:, None] == flat[None, :])).astype(jnp.int32), axis=1).reshape(32, 4)
    target = jnp.tile(route_ids * 8 + slot * 4, (4, 1)) + jnp.arange(128, dtype=jnp.int32)[:, None] // 32
    weight = jnp.tile(route_weight.astype(BF).astype(F32), (4, 1))

    own_rows = lax.dynamic_slice_in_dim(residual, t * 32, 32, 0)
    stream, normed, outbound = call(
        dispatch_kernel,
        (p0, p1, p2, p3, own_rows, norm_gain.reshape(1, -1), target.T),
        [shaped((32, 4096), F32), shaped((32, 4096), BF), shaped((1024, 1024), BF)],
        flops=2 * 1024 * 128 * 1024,
    )
    every = SP + ("tp",)
    inbound = lax.all_to_all(outbound.reshape(128, 8, 1024), every, 0, 0, tiled=True)

    n1, n2, n3 = (shift(normed, "tp", k) for k in (1, 2, 3))
    s0, s1, s2, s3 = call(
        shared_kernel,
        (normed, n1, n2, n3, shared_gate, shared_up, shared_down),
        [shaped((32, 4096), BF)] * 4,
        flops=2 * 128 * 4096 * 768,
    )
    s1, s2, s3 = shift(s1, "tp", 3), shift(s2, "tp", 2), shift(s3, "tp", 1)

    (result,) = call(
        expert_kernel,
        (inbound.reshape(1024, 1024), expert_gate, expert_up, expert_down),
        [shaped((1024, 1024), BF)],
        scratch=[pltpu.VMEM((256, 4096), BF)],
        flops=2 * 256 * 4096 * 768,
    )
    returned = lax.all_to_all(result.reshape(128, 8, 1024), every, 0, 0, tiled=True)
    (out,) = call(
        combine_kernel,
        (returned.reshape(1024, 1024), target, weight, stream, s0, s1, s2, s3),
        [shaped((32, 4096), BF)],
        flops=2 * 128 * 1024 * 1024,
    )
    return out


def solution(mesh):
    mesh = Mesh(mesh.devices.reshape(4, 4, 2, 4), ("z", "y", "c", "tp"))
    every = SP + ("tp",)
    placed = (
        P(SP, "tp"),
        P(SP, "tp"),
        P(SP, "tp"),
        P(None, "tp"),
        P(SP, "tp"),
        P(SP, "tp"),
        P(SP, "tp"),
        P(None, "tp"),
        P("tp", None),
        P("tp", None),
        P(SP, None),
        P(),
        P(every, None),
        P(every, None),
        P(every, None, None),
        P(every, None, None),
        P(every, None, None),
        P(None, "tp"),
        P(None, "tp"),
        P("tp", None),
    )
    return jax.shard_map(local, mesh=mesh, in_specs=placed, out_specs=P(every, None), check_vma=False)
```

```python
import functools

import jax
import jax.numpy as jnp
from jax import lax
from jax.experimental import pallas as pl
from jax.experimental.pallas import tpu as pltpu
from jax.sharding import Mesh
from jax.sharding import PartitionSpec as P


SP = ("z", "y", "c")
NARROW_SIZE = 128
BROAD_SIZE = 256
LOG2E = 1.4426950408889634
MASKED = -1e30
EPSILON = 1e-06
ORDER = (0, 1, 3, 2)
VMEM = pl.BlockSpec(memory_space=pltpu.VMEM)
SMEM = pl.BlockSpec(memory_space=pltpu.SMEM)
HBM = pl.BlockSpec(memory_space=pltpu.HBM)
BF = jnp.bfloat16
F32 = jnp.float32


def shift(x, axis, k):
    return lax.ppermute(x, axis, [(i, (i + k) % 4) for i in range(4)])


def swap_core(x):
    return lax.ppermute(x, "c", [(0, 1), (1, 0)])


def turn(x, k, phase):
    pairs = []
    for z in range(4):
        for y in range(4):
            for c in range(2):
                to_z, to_y = (z, (y + k) % 4) if c == phase else ((z + k) % 4, y)
                pairs.append(((z * 4 + y) * 2 + c, (to_z * 4 + to_y) * 2 + c))
    return lax.ppermute(x, SP, pairs)


def call(kernel, operands, shapes, smem=(), hbm=(), scratch=(), mib=16, flops=0):
    return pl.pallas_call(
        kernel,
        out_shape=shapes,
        in_specs=[SMEM if i in smem else HBM if i in hbm else VMEM for i in range(len(operands))],
        out_specs=[VMEM] * len(shapes),
        scratch_shapes=list(scratch),
        compiler_params=pltpu.CompilerParams(vmem_limit_bytes=mib * 1024 * 1024),
        cost_estimate=pl.CostEstimate(flops=flops, transcendentals=0, bytes_accessed=2 * 1024 * 1024),
    )(*operands)


def shaped(shape, dtype):
    return jax.ShapeDtypeStruct(shape, dtype)


def pack_kernel(kn, vn, kb, vb, qn, qb, kv, q, sems):
    copies = []
    for ref, out, at in ((kn, kv, 0), (vn, kv, 128), (kb, kv, 256), (vb, kv, 512), (qn, q, 0), (qb, q, 512)):
        target = out.at[:, at : at + ref.shape[1]]
        copies.append(pltpu.make_async_copy(ref, target, sems.at[len(copies)]))
    for copy in copies:
        copy.start()
    for copy in copies:
        copy.wait()


def stack_kernel(a, b, c, d, out):
    for i, ref in enumerate((a, b, c, d)):
        out[i] = ref[...]


def bias_kernel(place, narrow, broad, own, first, second, third):
    z, y, c = place[0], place[1], place[2]
    here = z * 4 + y

    def put(out, at, early, late):
        back_y = jnp.where(c == 0, early, late)
        back_z = jnp.where(c == 0, late, early)
        chip = ((z + 4 - back_z) % 4) * 4 + (y + 4 - back_y) % 4
        block = pl.multiple_of(chip * 256 + c * 128, 128)
        ahead = chip > here
        for row, gates in ((0, narrow), (4, broad)):
            piece = gates[:, pl.ds(block, 128)] * (-LOG2E)
            out[row : row + gates.shape[0], at : at + 128] = jnp.where(ahead, MASKED, piece)

    put(own, 0, 0, 0)
    for i in range(1, 4):
        put(first, (i - 1) * 128, ORDER[i], 0)
    for i in range(4):
        put(second, i * 128, ORDER[i], 1)
        put(second, 512 + i * 128, ORDER[i], 3)
        put(third, i * 128, ORDER[i], 2)


def project_kernel(place, own, other, narrow, broad, *refs):
    outs, total, attn = refs[:4], refs[4], refs[5]
    a, b = own[:, 1024:], other[:, 1024:]
    top = jnp.maximum(a, b)
    wa, wb = jnp.exp2(a - top), jnp.exp2(b - top)
    joined = wa + wb
    wa, wb = wa / joined, wb / joined
    for h in range(6):
        lo, size = (h * 128, 128) if h < 4 else (512 + (h - 4) * 256, 256)
        value = own[:, lo : lo + size] * wa[:, h : h + 1] + other[:, lo : lo + size] * wb[:, h : h + 1]
        attn[:, lo : lo + size] = value.astype(BF)
    for at in range(0, 4096, 1024):
        part = jnp.dot(attn[:, :512], narrow[:, at : at + 1024], preferred_element_type=F32)
        total[:, at : at + 1024] = part + jnp.dot(attn[:, 512:], broad[:, at : at + 1024], preferred_element_type=F32)
    for k in range(4):
        outs[k][...] = total[pl.ds(((place[0] + k) % 4) * 32, 32), :].astype(BF)


def dispatch_kernel(p0, p1, p2, p3, residual, gain, target, stream_out, normed_out, out):
    mixture = p0[...].astype(F32) + p1[...].astype(F32) + p2[...].astype(F32) + p3[...].astype(F32)
    stream = residual[...].astype(F32) + mixture
    stream_out[...] = stream
    scale = lax.rsqrt(jnp.mean(stream * stream, axis=1, keepdims=True) + EPSILON)
    normed = (stream * scale * gain[...]).astype(BF)
    normed_out[...] = normed
    cut = jnp.concatenate([normed[:, g * 1024 : (g + 1) * 1024] for g in range(4)], axis=0)
    row = lax.broadcasted_iota(jnp.int32, (256, 128), 0)
    for at in range(0, 1024, 256):
        pick = row + at == target[0:1, :]
        for k in range(1, 4):
            pick = pick | (row + at == target[k : k + 1, :])
        out[at : at + 256, :] = jnp.dot(pick.astype(F32).astype(BF), cut, preferred_element_type=F32).astype(BF)


def silu(v):
    return v / (1.0 + jnp.exp(-v))


def shared_kernel(n0, n1, n2, n3, gate, up, down, o0, o1, o2, o3):
    x = jnp.concatenate([n0[...], n1[...], n2[...], n3[...]], axis=0)
    g = jnp.dot(x, gate[...], preferred_element_type=F32)
    u = jnp.dot(x, up[...], preferred_element_type=F32)
    hidden = (silu(g) * u).astype(BF)
    for at in range(0, 4096, 1024):
        part = jnp.dot(hidden, down[:, at : at + 1024], preferred_element_type=F32).astype(BF)
        for k, out in enumerate((o0, o1, o2, o3)):
            out[:, at : at + 1024] = part[k * 32 : (k + 1) * 32]


def expert_kernel(inbound, gate, up, down, out, x):
    i = lax.broadcasted_iota(jnp.int32, (256, 256), 0)
    j = lax.broadcasted_iota(jnp.int32, (256, 256), 1)
    order = (j == ((i % 64) // 2) * 8 + (i % 2) * 4 + i // 64).astype(F32).astype(BF)
    back = (i == ((j % 64) // 2) * 8 + (j % 2) * 4 + j // 64).astype(F32).astype(BF)
    for b in range(4):
        rows = jnp.dot(order, inbound[b * 256 : (b + 1) * 256, :], preferred_element_type=F32).astype(BF)
        for g in range(4):
            x[b * 64 : (b + 1) * 64, g * 1024 : (g + 1) * 1024] = rows[g * 64 : (g + 1) * 64]
    gated = jnp.dot(x[...], gate[0], preferred_element_type=F32)
    upped = jnp.dot(x[...], up[0], preferred_element_type=F32)
    hidden = (silu(gated) * upped).astype(BF)
    for g in range(4):
        part = jnp.dot(hidden, down[0, :, g * 1024 : (g + 1) * 1024], preferred_element_type=F32)
        x[:, g * 1024 : (g + 1) * 1024] = part.astype(BF)
    for b in range(4):
        rows = jnp.concatenate([x[b * 64 : (b + 1) * 64, g * 1024 : (g + 1) * 1024] for g in range(4)], axis=0)
        out[b * 256 : (b + 1) * 256, :] = jnp.dot(back, rows, preferred_element_type=F32).astype(BF)


def combine_kernel(returned, target, weight, stream, s0, s1, s2, s3, out):
    column = lax.broadcasted_iota(jnp.int32, (128, 1024), 1)
    mix = jnp.zeros((128, 1024), F32)
    for k in range(4):
        mix = mix + jnp.where(column == target[:, k : k + 1], weight[:, k : k + 1], 0.0)
    routed = jnp.dot(mix.astype(BF), returned[...], preferred_element_type=F32)
    for g in range(4):
        lo, hi = g * 1024, (g + 1) * 1024
        total = stream[:, lo:hi] + routed[g * 32 : (g + 1) * 32]
        for s in (s0, s1, s2, s3):
            total = total + s[:, lo:hi].astype(F32)
        out[:, lo:hi] = total.astype(BF)


def attend_kernel(counts, first, last, *refs):
    at = 0

    def take(n):
        nonlocal at
        at += n
        return refs[at - n : at]

    q_own, q_other, core = take(3)
    tiles, planes = [], []
    for n, own_block in counts:
        tiles.append((take(n), take(1)[0], own_block))
        if first and not own_block:
            planes += tiles[-1][0]
    if not first:
        m_in, l_in, an_in, ab_in = take(4)
    if first:
        weights_in = take(2)
    if last:
        own_out, send_out = take(2)
    else:
        m_out, l_out, an_out, ab_out = take(4)
    if first:
        weights_out, sems = take(2), take(1)[0]
        copies = [pltpu.make_async_copy(weights_in[i], weights_out[i], sems.at[i]) for i in range(2)]
        for copy in copies:
            copy.start()

    def keys(ref, lo, hi):
        value = ref[1:, :, lo:hi] if any(ref is p for p in planes) else ref[..., lo:hi]
        return value.reshape(-1, hi - lo)

    results = {}
    for group, size, heads, lo in (("n", NARROW_SIZE, 4, 0), ("b", BROAD_SIZE, 2, 256)):
        scale = size**-0.5 * LOG2E
        base = 0 if group == "n" else 4
        row_base = 0 if group == "n" else 1024
        loaded = []
        for arrays, bias, own_block in tiles:
            k = jnp.concatenate([keys(r, lo, lo + size) for r in arrays], axis=0)
            v = jnp.concatenate([keys(r, lo + size, lo + 2 * size) for r in arrays], axis=0)
            loaded.append((k, v, bias, own_block))
        for side, q_ref in ((0, q_own), (1, q_other)):
            for h0 in range(0, heads, 2):
                col = (0 if group == "n" else 512) + h0 * size
                q = jnp.concatenate([q_ref[:, col + i * size : col + (i + 1) * size] for i in range(2)], axis=0)
                rows = row_base + side * heads * 128 + h0 * 128
                arow = rows - row_base
                scores = []
                for k, v, bias, own_block in loaded:
                    s = lax.dot_general(q, k, (((1,), (1,)), ((), ())), preferred_element_type=F32) * scale
                    n = k.shape[0]
                    b = bias[base + h0 : base + h0 + 2, :]
                    s = (s.reshape(2, 128, n) + b[:, None, :]).reshape(256, n)
                    if own_block:
                        qi = lax.broadcasted_iota(jnp.int32, (256, n), 0) % 128
                        ki = lax.broadcasted_iota(jnp.int32, (256, n), 1)
                        offset = 0 if side == 0 else 128 * (1 - 2 * core[0])
                        s = jnp.where(ki <= qi + offset, s, MASKED)
                    scores.append(s)
                m = functools.reduce(jnp.maximum, [jnp.max(s, axis=1, keepdims=True) for s in scores])
                if not first:
                    m_old = m_in[pl.ds(rows, 256), :][:, :1]
                    m = jnp.maximum(m, m_old)
                l = jnp.zeros((256, 1), F32)
                acc = jnp.zeros((256, size), F32)
                for s, (k, v, bias, own_block) in zip(scores, loaded):
                    p = jnp.exp2(s - m)
                    l = l + jnp.sum(p, axis=1, keepdims=True)
                    acc = acc + jnp.dot(p.astype(BF), v, preferred_element_type=F32)
                if not first:
                    a_in = an_in if group == "n" else ab_in
                    factor = jnp.exp2(m_old - m)
                    l = l + l_in[pl.ds(rows, 256), :][:, :1] * factor
                    acc = acc + a_in[pl.ds(arow, 256), :] * factor
                if last:
                    out = own_out if side == 0 else send_out
                    o = acc / l
                    lse = m + jnp.log2(l)
                    for i in range(2):
                        out[:, col + i * size : col + (i + 1) * size] = o[i * 128 : (i + 1) * 128]
                        results[(side, base + h0 + i)] = lse[i * 128 : (i + 1) * 128]
                else:
                    a_out = an_out if group == "n" else ab_out
                    m_out[pl.ds(rows, 256), :] = jnp.broadcast_to(m, (256, 128))
                    l_out[pl.ds(rows, 256), :] = jnp.broadcast_to(l, (256, 128))
                    a_out[pl.ds(arow, 256), :] = acc
    if last:
        lane = lax.broadcasted_iota(jnp.int32, (128, 128), 1)
        for side, out in ((0, own_out), (1, send_out)):
            stats = jnp.zeros((128, 128), F32)
            for h in range(6):
                stats = jnp.where(lane == h, results[(side, h)], stats)
            out[:, 1024:1152] = stats
    if first:
        for copy in copies:
            copy.wait()


def attend(q_own, q_other, core, tiles, state, last, weights=None):
    counts = tuple((len(arrays), own_block) for arrays, _, own_block in tiles)
    operands = [q_own, q_other, core]
    n_keys = 0
    for arrays, bias, _ in tiles:
        operands += list(arrays) + [bias]
        n_keys += bias.shape[1]
    specs = [VMEM] * len(operands)
    specs[2] = SMEM
    if state is not None:
        operands += list(state)
        specs += [VMEM] * 4
    else:
        operands += list(weights)
        specs += [HBM] * 2
    if last:
        shapes = [jax.ShapeDtypeStruct((128, 1152), F32)] * 2
    else:
        shapes = [
            jax.ShapeDtypeStruct((1536, 128), F32),
            jax.ShapeDtypeStruct((1536, 128), F32),
            jax.ShapeDtypeStruct((1024, 128), F32),
            jax.ShapeDtypeStruct((512, 256), F32),
        ]
    if state is None:
        shapes += [jax.ShapeDtypeStruct(w.shape, w.dtype) for w in weights]
    return pl.pallas_call(
        functools.partial(attend_kernel, counts, state is None, last),
        out_shape=shapes,
        in_specs=specs,
        out_specs=[VMEM] * len(shapes),
        scratch_shapes=[pltpu.SemaphoreType.DMA((2,))] if state is None else [],
        compiler_params=pltpu.CompilerParams(vmem_limit_bytes=24 * 1024 * 1024),
        cost_estimate=pl.CostEstimate(
            flops=4 * n_keys * 256 * 1024, transcendentals=n_keys * 1536, bytes_accessed=4 * 1024 * 1024
        ),
    )(*operands)


def local(
    query_narrow,
    key_narrow,
    value_narrow,
    gates_narrow,
    query_broad,
    key_broad,
    value_broad,
    gates_broad,
    project_narrow,
    project_broad,
    residual,
    norm_gain,
    route_ids,
    route_weight,
    expert_gate,
    expert_up,
    expert_down,
    shared_gate,
    shared_up,
    shared_down,
):
    z, y, c, t = (lax.axis_index(n).astype(jnp.int32) for n in ("z", "y", "c", "tp"))

    own_kv, q_own = call(
        pack_kernel,
        (key_narrow, value_narrow, key_broad, value_broad, query_narrow, query_broad),
        [shaped((128, 768), BF), shaped((128, 1024), BF)],
        hbm=range(6),
        scratch=[pltpu.SemaphoreType.DMA((6,))],
    )
    line = [turn(own_kv, k, 0) for k in ORDER[1:]]
    q_other = swap_core(q_own)
    (plane,) = call(stack_kernel, [own_kv] + line, [shaped((4, 128, 768), BF)])
    back, ahead, far = (turn(plane, k, 1) for k in ORDER[1:])

    own_bias, bias_1, bias_2, bias_3 = call(
        bias_kernel,
        (jnp.stack([z, y, c]), gates_narrow.T, gates_broad.T),
        [shaped((8, n), F32) for n in (128, 384, 1024, 512)],
        smem=(0,),
    )
    core = c.reshape(1)
    first_tiles = [((own_kv,), own_bias, True), ((plane,), bias_1, False)]
    *state, narrow, broad = attend(
        q_own, q_other, core, first_tiles, None, False, (project_narrow, project_broad)
    )
    state = attend(q_own, q_other, core, [((back, ahead), bias_2, False)], state, False)
    own_part, send_part = attend(q_own, q_other, core, [((far,), bias_3, False)], state, True)
    other_part = swap_core(send_part)

    p0, p1, p2, p3 = call(
        project_kernel,
        (t.reshape(1), own_part, other_part, narrow, broad),
        [shaped((32, 4096), BF)] * 4,
        smem=(0,),
        scratch=[pltpu.VMEM((128, 4096), F32), pltpu.VMEM((128, 1024), BF)],
        flops=2 * 128 * 1024 * 4096,
    )
    p1, p2, p3 = shift(p1, "tp", 1), shift(p2, "tp", 2), shift(p3, "tp", 3)

    flat = route_ids.reshape(-1)
    earlier = jnp.arange(128)[:, None] // 4 > jnp.arange(128)[None, :] // 4
    slot = jnp.sum((earlier & (flat[:, None] == flat[None, :])).astype(jnp.int32), axis=1).reshape(32, 4)
    target = jnp.tile(route_ids * 8 + slot * 4, (4, 1)) + jnp.arange(128, dtype=jnp.int32)[:, None] // 32
    weight = jnp.tile(route_weight.astype(BF).astype(F32), (4, 1))

    own_rows = lax.dynamic_slice_in_dim(residual, t * 32, 32, 0)
    stream, normed, outbound = call(
        dispatch_kernel,
        (p0, p1, p2, p3, own_rows, norm_gain.reshape(1, -1), target.T),
        [shaped((32, 4096), F32), shaped((32, 4096), BF), shaped((1024, 1024), BF)],
        flops=2 * 1024 * 128 * 1024,
    )
    every = SP + ("tp",)
    inbound = lax.all_to_all(outbound.reshape(128, 8, 1024), every, 0, 0, tiled=True)

    n1 = shift(normed, "tp", 1)
    n2 = shift(normed, "tp", 2)
    n3 = shift(normed, "tp", 3)
    s0, s1, s2, s3 = call(
        shared_kernel,
        (normed, n1, n2, n3, shared_gate, shared_up, shared_down),
        [shaped((32, 4096), BF)] * 4,
        flops=2 * 128 * 4096 * 768,
    )
    s1 = shift(s1, "tp", 3)
    s2 = shift(s2, "tp", 2)
    s3 = shift(s3, "tp", 1)

    (result,) = call(
        expert_kernel,
        (inbound.reshape(1024, 1024), expert_gate, expert_up, expert_down),
        [shaped((1024, 1024), BF)],
        scratch=[pltpu.VMEM((256, 4096), BF)],
        flops=2 * 256 * 4096 * 768,
    )
    returned = lax.all_to_all(result.reshape(128, 8, 1024), every, 0, 0, tiled=True)
    (out,) = call(
        combine_kernel,
        (returned.reshape(1024, 1024), target, weight, stream, s0, s1, s2, s3),
        [shaped((32, 4096), BF)],
        flops=2 * 128 * 1024 * 1024,
    )
    return out


def solution(mesh):
    mesh = Mesh(mesh.devices.reshape(4, 4, 2, 4), ("z", "y", "c", "tp"))
    every = SP + ("tp",)
    placed = (
        P(SP, "tp"),
        P(SP, "tp"),
        P(SP, "tp"),
        P(None, "tp"),
        P(SP, "tp"),
        P(SP, "tp"),
        P(SP, "tp"),
        P(None, "tp"),
        P("tp", None),
        P("tp", None),
        P(SP, None),
        P(),
        P(every, None),
        P(every, None),
        P(every, None, None),
        P(every, None, None),
        P(every, None, None),
        P(None, "tp"),
        P(None, "tp"),
        P("tp", None),
    )

    return jax.shard_map(local, mesh=mesh, in_specs=placed, out_specs=P(every, None), check_vma=False)
```

```python
import functools

import jax
import jax.numpy as jnp
from jax import lax
from jax.experimental import pallas as pl
from jax.experimental.pallas import tpu as pltpu
from jax.sharding import Mesh
from jax.sharding import PartitionSpec as P


SP = ("z", "y", "c")
NARROW_SIZE = 128
BROAD_SIZE = 256
LOG2E = 1.4426950408889634
MASKED = -1e30
EPSILON = 1e-06
ORDER = (0, 1, 3, 2)
VMEM = pl.BlockSpec(memory_space=pltpu.VMEM)
SMEM = pl.BlockSpec(memory_space=pltpu.SMEM)
HBM = pl.BlockSpec(memory_space=pltpu.HBM)
BF = jnp.bfloat16
F32 = jnp.float32


def shift(x, axis, k):
    return lax.ppermute(x, axis, [(i, (i + k) % 4) for i in range(4)])


def swap_core(x):
    return lax.ppermute(x, "c", [(0, 1), (1, 0)])


def turn(x, k, phase):
    pairs = []
    for z in range(4):
        for y in range(4):
            for c in range(2):
                to_z, to_y = (z, (y + k) % 4) if c == phase else ((z + k) % 4, y)
                pairs.append(((z * 4 + y) * 2 + c, (to_z * 4 + to_y) * 2 + c))
    return lax.ppermute(x, SP, pairs)


def call(kernel, operands, shapes, smem=(), hbm=(), scratch=(), mib=16, flops=0, moved=2**21):
    return pl.pallas_call(
        kernel,
        out_shape=shapes,
        in_specs=[SMEM if i in smem else HBM if i in hbm else VMEM for i in range(len(operands))],
        out_specs=[VMEM] * len(shapes),
        scratch_shapes=list(scratch),
        compiler_params=pltpu.CompilerParams(vmem_limit_bytes=mib * 1024 * 1024),
        cost_estimate=pl.CostEstimate(flops=flops, transcendentals=0, bytes_accessed=moved),
    )(*operands)


def shaped(shape, dtype):
    return jax.ShapeDtypeStruct(shape, dtype)


def pack_kernel(kn, vn, kb, vb, qn, qb, kv, q, sems):
    copies = []
    for ref, out, at in ((kn, kv, 0), (vn, kv, 128), (kb, kv, 256), (vb, kv, 512), (qn, q, 0), (qb, q, 512)):
        target = out.at[:, at : at + ref.shape[1]]
        copies.append(pltpu.make_async_copy(ref, target, sems.at[len(copies)]))
    for copy in copies:
        copy.start()
    for copy in copies:
        copy.wait()


def stack_kernel(a, b, c, d, ready, low, high):
    for out, i, ref in ((low, 0, a), (low, 1, b), (high, 0, c), (high, 1, d)):
        out[i] = ref[...]


def route_kernel(ids_in, weight_in, target, mix):
    ids = jnp.concatenate([ids_in[...]] * 4, axis=1)
    weight = jnp.concatenate([weight_in[...].astype(BF).astype(F32)] * 4, axis=1)
    expert = lax.broadcasted_iota(jnp.int32, (128, 128), 0)
    column = lax.broadcasted_iota(jnp.int32, (128, 128), 1)
    named = jnp.zeros((128, 128), F32)
    for k in range(4):
        named = named + jnp.where(expert == ids[k : k + 1, :], 1.0, 0.0)
    earlier = jnp.where((expert < 32) & (expert < column % 32), 1.0, 0.0).astype(BF)
    before = jnp.dot(named.astype(BF), earlier, preferred_element_type=F32)
    row = lax.broadcasted_iota(jnp.int32, (1024, 128), 0)
    total = jnp.zeros((1024, 128), F32)
    for k in range(4):
        slot = jnp.sum(jnp.where(expert == ids[k : k + 1, :], before, 0.0), axis=0, keepdims=True)
        start = ids[k : k + 1, :] * 8 + slot.astype(jnp.int32) * 4 + column[:1] // 32
        target[k : k + 1, :] = start
        total = total + jnp.where(row == start, weight[k : k + 1, :], 0.0)
    mix[...] = total.T.astype(BF)


def bias_kernel(place, narrow, broad, own, first, second, third):
    z, y, c = place[0], place[1], place[2]
    here = z * 4 + y

    def put(out, at, early, late):
        back_y = jnp.where(c == 0, early, late)
        back_z = jnp.where(c == 0, late, early)
        chip = ((z + 4 - back_z) % 4) * 4 + (y + 4 - back_y) % 4
        block = pl.multiple_of(chip * 256 + c * 128, 128)
        ahead = chip > here
        for row, gates in ((0, narrow), (4, broad)):
            piece = gates[:, pl.ds(block, 128)] * (-LOG2E)
            out[row : row + gates.shape[0], at : at + 128] = jnp.where(ahead, MASKED, piece)

    put(own, 0, 0, 0)
    for i in range(1, 4):
        put(first, (i - 1) * 128, ORDER[i], 0)
    for i in range(4):
        put(second, i * 128, ORDER[i % 2], 1 if i < 2 else 3)
        put(second, 512 + i * 128, ORDER[2 + i % 2], 1 if i < 2 else 3)
        put(third, i * 128, ORDER[i], 2)


def project_kernel(place, own, other, narrow, broad, *refs):
    outs, total, attn, weights, sems = refs[:4], *refs[4:]
    copies = []
    for at in range(0, 4096, 1024):
        for i, ref in enumerate((narrow, broad)):
            source, target = ref.at[:, at : at + 1024], weights.at[i, :, at : at + 1024]
            copies.append(pltpu.make_async_copy(source, target, sems.at[len(copies)]))
    for copy in copies:
        copy.start()
    a, b = own[:, 1024:], other[:, 1024:]
    top = jnp.maximum(a, b)
    wa, wb = jnp.exp2(a - top), jnp.exp2(b - top)
    joined = wa + wb
    wa, wb = wa / joined, wb / joined
    for h in range(6):
        lo, size = (h * 128, 128) if h < 4 else (512 + (h - 4) * 256, 256)
        value = own[:, lo : lo + size] * wa[:, h : h + 1] + other[:, lo : lo + size] * wb[:, h : h + 1]
        attn[:, lo : lo + size] = value.astype(BF)
    for at in range(0, 4096, 1024):
        copies[at // 512].wait()
        copies[at // 512 + 1].wait()
        part = jnp.dot(attn[:, :512], weights[0, :, at : at + 1024], preferred_element_type=F32)
        part = part + jnp.dot(attn[:, 512:], weights[1, :, at : at + 1024], preferred_element_type=F32)
        total[:, at : at + 1024] = part
    for k in range(4):
        outs[k][...] = total[pl.ds(((place[3] + k) % 4) * 32, 32), :].astype(BF)


def dispatch_kernel(place, p0, p1, p2, p3, residual, gain, target, stream_out, normed_out, out):
    mixture = p0[...].astype(F32) + p1[...].astype(F32) + p2[...].astype(F32) + p3[...].astype(F32)
    stream = residual[pl.ds(place[3] * 32, 32), :].astype(F32) + mixture
    stream_out[...] = stream
    scale = lax.rsqrt(jnp.mean(stream * stream, axis=1, keepdims=True) + EPSILON)
    normed = (stream * scale * gain[...]).astype(BF)
    normed_out[...] = normed
    cut = jnp.concatenate([normed[:, g * 1024 : (g + 1) * 1024] for g in range(4)], axis=0)
    row = lax.broadcasted_iota(jnp.int32, (256, 128), 0)
    for at in range(0, 1024, 256):
        pick = row + at == target[0:1, :]
        for k in range(1, 4):
            pick = pick | (row + at == target[k : k + 1, :])
        out[at : at + 256, :] = jnp.dot(pick.astype(F32).astype(BF), cut, preferred_element_type=F32).astype(BF)


def silu(v):
    return v / (1.0 + jnp.exp(-v))


def shared_kernel(n0, n1, n2, n3, gate, up, down, o0, o1, o2, o3):
    x = jnp.concatenate([n0[...], n1[...], n2[...], n3[...]], axis=0)
    g = jnp.dot(x, gate[...], preferred_element_type=F32)
    u = jnp.dot(x, up[...], preferred_element_type=F32)
    hidden = (silu(g) * u).astype(BF)
    for at in range(0, 4096, 1024):
        part = jnp.dot(hidden, down[:, at : at + 1024], preferred_element_type=F32).astype(BF)
        for k, out in enumerate((o0, o1, o2, o3)):
            out[:, at : at + 1024] = part[k * 32 : (k + 1) * 32]


def expert_kernel(inbound, gate, up, down, out, x, gate_up, down_copy, sems):
    copies = []
    for g in range(4):
        for i, ref in enumerate((gate, up)):
            part = pl.ds(g * 1024, 1024)
            copies.append(pltpu.make_async_copy(ref.at[0, part], gate_up.at[i, part], sems.at[len(copies)]))
    copies.append(pltpu.make_async_copy(down.at[0], down_copy, sems.at[len(copies)]))
    for copy in copies:
        copy.start()
    i = lax.broadcasted_iota(jnp.int32, (256, 256), 0)
    j = lax.broadcasted_iota(jnp.int32, (256, 256), 1)
    order = (j == ((i % 64) // 2) * 8 + (i % 2) * 4 + i // 64).astype(F32).astype(BF)
    back = (i == ((j % 64) // 2) * 8 + (j % 2) * 4 + j // 64).astype(F32).astype(BF)
    for b in range(4):
        rows = jnp.dot(order, inbound[b * 256 : (b + 1) * 256, :], preferred_element_type=F32).astype(BF)
        for g in range(4):
            x[b * 64 : (b + 1) * 64, g * 1024 : (g + 1) * 1024] = rows[g * 64 : (g + 1) * 64]
    gated, upped = jnp.zeros((256, 256), F32), jnp.zeros((256, 256), F32)
    for g in range(4):
        lo, hi = g * 1024, (g + 1) * 1024
        copies[2 * g].wait()
        gated = gated + jnp.dot(x[:, lo:hi], gate_up[0, lo:hi], preferred_element_type=F32)
        copies[2 * g + 1].wait()
        upped = upped + jnp.dot(x[:, lo:hi], gate_up[1, lo:hi], preferred_element_type=F32)
    copies[-1].wait()
    hidden = (silu(gated) * upped).astype(BF)
    for g in range(4):
        part = jnp.dot(hidden, down_copy[:, g * 1024 : (g + 1) * 1024], preferred_element_type=F32)
        x[:, g * 1024 : (g + 1) * 1024] = part.astype(BF)
    for b in range(4):
        rows = jnp.concatenate([x[b * 64 : (b + 1) * 64, g * 1024 : (g + 1) * 1024] for g in range(4)], axis=0)
        out[b * 256 : (b + 1) * 256, :] = jnp.dot(back, rows, preferred_element_type=F32).astype(BF)


def combine_kernel(returned, mix, stream, s0, s1, s2, s3, out):
    routed = jnp.dot(mix[...], returned[...], preferred_element_type=F32)
    for g in range(4):
        lo, hi = g * 1024, (g + 1) * 1024
        total = stream[:, lo:hi] + routed[g * 32 : (g + 1) * 32]
        for s in (s0, s1, s2, s3):
            total = total + s[:, lo:hi].astype(F32)
        out[:, lo:hi] = total.astype(BF)


def attend_kernel(counts, first, last, *refs):
    at = 0

    def take(n):
        nonlocal at
        at += n
        return refs[at - n : at]

    q_own, q_other, core = take(3)
    tiles, planes = [], []
    for n, own_block in counts:
        tiles.append((take(n), take(1)[0], own_block))
        if first and not own_block:
            planes.append(tiles[-1][0][0])
    if not first:
        m_in, l_in, an_in, ab_in = take(4)
    if last:
        own_out, send_out = take(2)
    else:
        m_out, l_out, an_out, ab_out = take(4)

    def keys(ref, lo, hi):
        value = ref[1, :, lo:hi] if any(ref is p for p in planes) else ref[..., lo:hi]
        return value.reshape(-1, hi - lo)

    results = {}
    for group, size, heads, lo in (("n", NARROW_SIZE, 4, 0), ("b", BROAD_SIZE, 2, 256)):
        scale = size**-0.5 * LOG2E
        base = 0 if group == "n" else 4
        row_base = 0 if group == "n" else 1024
        loaded = []
        for arrays, bias, own_block in tiles:
            k = jnp.concatenate([keys(r, lo, lo + size) for r in arrays], axis=0)
            v = jnp.concatenate([keys(r, lo + size, lo + 2 * size) for r in arrays], axis=0)
            loaded.append((k, v, bias, own_block))
        for side, q_ref in ((0, q_own), (1, q_other)):
            for h0 in range(0, heads, 2):
                col = (0 if group == "n" else 512) + h0 * size
                q = jnp.concatenate([q_ref[:, col + i * size : col + (i + 1) * size] for i in range(2)], axis=0)
                rows = row_base + side * heads * 128 + h0 * 128
                arow = rows - row_base
                scores = []
                for k, v, bias, own_block in loaded:
                    s = lax.dot_general(q, k, (((1,), (1,)), ((), ())), preferred_element_type=F32) * scale
                    n = k.shape[0]
                    b = bias[base + h0 : base + h0 + 2, :]
                    s = (s.reshape(2, 128, n) + b[:, None, :]).reshape(256, n)
                    if own_block:
                        qi = lax.broadcasted_iota(jnp.int32, (256, n), 0) % 128
                        ki = lax.broadcasted_iota(jnp.int32, (256, n), 1)
                        offset = 0 if side == 0 else 128 * (1 - 2 * core[0])
                        s = jnp.where(ki <= qi + offset, s, MASKED)
                    scores.append(s)
                m = functools.reduce(jnp.maximum, [jnp.max(s, axis=1, keepdims=True) for s in scores])
                if not first:
                    m_old = m_in[pl.ds(rows, 256), :][:, :1]
                    m = jnp.maximum(m, m_old)
                l = jnp.zeros((256, 1), F32)
                acc = jnp.zeros((256, size), F32)
                for s, (k, v, bias, own_block) in zip(scores, loaded):
                    p = jnp.exp2(s - m)
                    l = l + jnp.sum(p, axis=1, keepdims=True)
                    acc = acc + jnp.dot(p.astype(BF), v, preferred_element_type=F32)
                if not first:
                    a_in = an_in if group == "n" else ab_in
                    factor = jnp.exp2(m_old - m)
                    l = l + l_in[pl.ds(rows, 256), :][:, :1] * factor
                    acc = acc + a_in[pl.ds(arow, 256), :] * factor
                if last:
                    out = own_out if side == 0 else send_out
                    o = acc / l
                    lse = m + jnp.log2(l)
                    for i in range(2):
                        out[:, col + i * size : col + (i + 1) * size] = o[i * 128 : (i + 1) * 128]
                        results[(side, base + h0 + i)] = lse[i * 128 : (i + 1) * 128]
                else:
                    a_out = an_out if group == "n" else ab_out
                    m_out[pl.ds(rows, 256), :] = jnp.broadcast_to(m, (256, 128))
                    l_out[pl.ds(rows, 256), :] = jnp.broadcast_to(l, (256, 128))
                    a_out[pl.ds(arow, 256), :] = acc
    if last:
        lane = lax.broadcasted_iota(jnp.int32, (128, 128), 1)
        for side, out in ((0, own_out), (1, send_out)):
            stats = jnp.zeros((128, 128), F32)
            for h in range(6):
                stats = jnp.where(lane == h, results[(side, h)], stats)
            out[:, 1024:1152] = stats


def attend(q_own, q_other, core, tiles, state, last):
    counts = tuple((len(arrays), own_block) for arrays, _, own_block in tiles)
    operands = [q_own, q_other, core]
    n_keys = 0
    for arrays, bias, _ in tiles:
        operands += list(arrays) + [bias]
        n_keys += bias.shape[1]
    specs = [VMEM] * len(operands)
    specs[2] = SMEM
    if state is not None:
        operands += list(state)
        specs += [VMEM] * 4
    if last:
        shapes = [jax.ShapeDtypeStruct((128, 1152), F32)] * 2
    else:
        shapes = [
            jax.ShapeDtypeStruct((1536, 128), F32),
            jax.ShapeDtypeStruct((1536, 128), F32),
            jax.ShapeDtypeStruct((1024, 128), F32),
            jax.ShapeDtypeStruct((512, 256), F32),
        ]
    return pl.pallas_call(
        functools.partial(attend_kernel, counts, state is None, last),
        out_shape=shapes,
        in_specs=specs,
        out_specs=[VMEM] * len(shapes),
        compiler_params=pltpu.CompilerParams(vmem_limit_bytes=24 * 1024 * 1024),
        cost_estimate=pl.CostEstimate(
            flops=4 * n_keys * 256 * 1024, transcendentals=n_keys * 1536, bytes_accessed=4 * 1024 * 1024
        ),
    )(*operands)


def local(
    query_narrow,
    key_narrow,
    value_narrow,
    gates_narrow,
    query_broad,
    key_broad,
    value_broad,
    gates_broad,
    project_narrow,
    project_broad,
    residual,
    norm_gain,
    route_ids,
    route_weight,
    expert_gate,
    expert_up,
    expert_down,
    shared_gate,
    shared_up,
    shared_down,
):
    z, y, c, t = (lax.axis_index(n).astype(jnp.int32) for n in ("z", "y", "c", "tp"))

    own_kv, q_own = call(
        pack_kernel,
        (key_narrow, value_narrow, key_broad, value_broad, query_narrow, query_broad),
        [shaped((128, 768), BF), shaped((128, 1024), BF)],
        hbm=range(6),
        scratch=[pltpu.SemaphoreType.DMA((6,))],
        moved=0,
    )
    target, mix = call(
        route_kernel,
        (route_ids.T, route_weight.T),
        [shaped((4, 128), jnp.int32), shaped((128, 1024), BF)],
    )
    place = jnp.stack([z, y, c, t])
    line = [turn(own_kv, k, 0) for k in ORDER[1:]]
    q_other = swap_core(q_own)
    low, high = call(stack_kernel, [own_kv] + line + [target], [shaped((2, 128, 768), BF)] * 2)
    low_back, high_ahead = turn(low, 1, 1), turn(high, 3, 1)
    low_ahead, high_back = turn(low, 3, 1), turn(high, 1, 1)
    low_far, high_far = turn(low_back, 1, 1), turn(high_ahead, 3, 1)

    own_bias, bias_1, bias_2, bias_3 = call(
        bias_kernel,
        (place, gates_narrow.T, gates_broad.T),
        [shaped((8, n), F32) for n in (128, 384, 1024, 512)],
        smem=(0,),
    )
    core = c.reshape(1)
    first_tiles = [((own_kv,), own_bias, True), ((low, high), bias_1, False)]
    state = attend(q_own, q_other, core, first_tiles, None, False)
    second_tiles = [((low_back, low_ahead, high_back, high_ahead), bias_2, False)]
    state = attend(q_own, q_other, core, second_tiles, state, False)
    own_part, send_part = attend(q_own, q_other, core, [((low_far, high_far), bias_3, False)], state, True)
    other_part = swap_core(send_part)

    p0, p1, p2, p3 = call(
        project_kernel,
        (place, own_part, other_part, project_narrow, project_broad),
        [shaped((32, 4096), BF)] * 4,
        smem=(0,),
        hbm=(3, 4),
        scratch=[
            pltpu.VMEM((128, 4096), F32),
            pltpu.VMEM((128, 1024), BF),
            pltpu.VMEM((2, 512, 4096), BF),
            pltpu.SemaphoreType.DMA((8,)),
        ],
        mib=20,
        moved=0,
        flops=2 * 128 * 1024 * 4096,
    )
    p1, p2, p3 = shift(p1, "tp", 1), shift(p2, "tp", 2), shift(p3, "tp", 3)

    stream, normed, outbound = call(
        dispatch_kernel,
        (place, p0, p1, p2, p3, residual, norm_gain.reshape(1, -1), target),
        [shaped((32, 4096), F32), shaped((32, 4096), BF), shaped((1024, 1024), BF)],
        smem=(0,),
        flops=2 * 1024 * 128 * 1024,
    )
    every = SP + ("tp",)
    inbound = lax.all_to_all(outbound.reshape(128, 8, 1024), every, 0, 0, tiled=True)

    n1 = shift(normed, "tp", 1)
    n2 = shift(normed, "tp", 2)
    n3 = shift(normed, "tp", 3)
    s0, s1, s2, s3 = call(
        shared_kernel,
        (normed, n1, n2, n3, shared_gate, shared_up, shared_down),
        [shaped((32, 4096), BF)] * 4,
        flops=2 * 128 * 4096 * 768,
    )
    s1 = shift(s1, "tp", 3)
    s2 = shift(s2, "tp", 2)
    s3 = shift(s3, "tp", 1)

    (result,) = call(
        expert_kernel,
        (inbound.reshape(1024, 1024), expert_gate, expert_up, expert_down),
        [shaped((1024, 1024), BF)],
        hbm=(1, 2, 3),
        scratch=[
            pltpu.VMEM((256, 4096), BF),
            pltpu.VMEM((2, 4096, 256), BF),
            pltpu.VMEM((256, 4096), BF),
            pltpu.SemaphoreType.DMA((9,)),
        ],
        mib=20,
        moved=0,
        flops=2 * 256 * 4096 * 768,
    )
    returned = lax.all_to_all(result.reshape(128, 8, 1024), every, 0, 0, tiled=True)
    (out,) = call(
        combine_kernel,
        (returned.reshape(1024, 1024), mix, stream, s0, s1, s2, s3),
        [shaped((32, 4096), BF)],
        flops=2 * 128 * 1024 * 1024,
    )
    return out


def solution(mesh):
    mesh = Mesh(mesh.devices.reshape(4, 4, 2, 4), ("z", "y", "c", "tp"))
    every = SP + ("tp",)
    placed = (
        P(SP, "tp"),
        P(SP, "tp"),
        P(SP, "tp"),
        P(None, "tp"),
        P(SP, "tp"),
        P(SP, "tp"),
        P(SP, "tp"),
        P(None, "tp"),
        P("tp", None),
        P("tp", None),
        P(SP, None),
        P(),
        P(every, None),
        P(every, None),
        P(every, None, None),
        P(every, None, None),
        P(every, None, None),
        P(None, "tp"),
        P(None, "tp"),
        P("tp", None),
    )

    return jax.shard_map(local, mesh=mesh, in_specs=placed, out_specs=P(every, None), check_vma=False)
```

```python
import functools

import jax
import jax.numpy as jnp
from jax import lax
from jax.experimental import pallas as pl
from jax.experimental.pallas import tpu as pltpu
from jax.sharding import Mesh
from jax.sharding import PartitionSpec as P


SP = ("z", "y", "c")
NARROW_SIZE = 128
BROAD_SIZE = 256
LOG2E = 1.4426950408889634
MASKED = -1e30
EPSILON = 1e-06
ORDER = (0, 1, 3, 2)
VMEM = pl.BlockSpec(memory_space=pltpu.VMEM)
SMEM = pl.BlockSpec(memory_space=pltpu.SMEM)
HBM = pl.BlockSpec(memory_space=pltpu.HBM)
BF = jnp.bfloat16
F32 = jnp.float32


def shift(x, axis, k):
    return lax.ppermute(x, axis, [(i, (i + k) % 4) for i in range(4)])


def swap_core(x):
    return lax.ppermute(x, "c", [(0, 1), (1, 0)])


def turn(x, k, phase):
    pairs = []
    for z in range(4):
        for y in range(4):
            for c in range(2):
                to_z, to_y = (z, (y + k) % 4) if c == phase else ((z + k) % 4, y)
                pairs.append(((z * 4 + y) * 2 + c, (to_z * 4 + to_y) * 2 + c))
    return lax.ppermute(x, SP, pairs)


def call(kernel, operands, shapes, smem=(), hbm=(), hbm_out=(), scratch=(), mib=16, flops=0, moved=2**21):
    operands = [
        pltpu.with_memory_space_constraint(x, pltpu.HBM) if i in hbm else x for i, x in enumerate(operands)
    ]
    return pl.pallas_call(
        kernel,
        out_shape=shapes,
        in_specs=[SMEM if i in smem else HBM if i in hbm else VMEM for i in range(len(operands))],
        out_specs=[HBM if i in hbm_out else VMEM for i in range(len(shapes))],
        scratch_shapes=list(scratch),
        compiler_params=pltpu.CompilerParams(vmem_limit_bytes=mib * 1024 * 1024),
        cost_estimate=pl.CostEstimate(flops=flops, transcendentals=0, bytes_accessed=moved),
    )(*operands)


def shaped(shape, dtype):
    return jax.ShapeDtypeStruct(shape, dtype)


def pack_kernel(kn, vn, kb, vb, qn, qb, kv, q, sems):
    copies = []
    for ref, out, at in ((kn, kv, 0), (vn, kv, 128), (kb, kv, 256), (vb, kv, 512), (qn, q, 0), (qb, q, 512)):
        target = out.at[:, at : at + ref.shape[1]]
        copies.append(pltpu.make_async_copy(ref, target, sems.at[len(copies)]))
    for copy in copies:
        copy.start()
    for copy in copies:
        copy.wait()


def stack_kernel(a, b, c, d, routed, biased, low, high):
    for out, i, ref in ((low, 0, a), (low, 1, b), (high, 0, c), (high, 1, d)):
        out[i] = ref[...]


def route_kernel(ids_in, weight_in, target, mix):
    ids = jnp.concatenate([ids_in[...]] * 4, axis=1)
    weight = jnp.concatenate([weight_in[...].astype(BF).astype(F32)] * 4, axis=1)
    expert = lax.broadcasted_iota(jnp.int32, (128, 128), 0)
    column = lax.broadcasted_iota(jnp.int32, (128, 128), 1)
    named = jnp.zeros((128, 128), F32)
    for k in range(4):
        named = named + jnp.where(expert == ids[k : k + 1, :], 1.0, 0.0)
    earlier = jnp.where((expert < 32) & (expert < column % 32), 1.0, 0.0).astype(BF)
    before = jnp.dot(named.astype(BF), earlier, preferred_element_type=F32)
    row = lax.broadcasted_iota(jnp.int32, (1024, 128), 0)
    total = jnp.zeros((1024, 128), F32)
    for k in range(4):
        slot = jnp.sum(jnp.where(expert == ids[k : k + 1, :], before, 0.0), axis=0, keepdims=True)
        start = ids[k : k + 1, :] * 8 + slot.astype(jnp.int32) * 4 + column[:1] // 32
        target[k : k + 1, :] = start
        total = total + jnp.where(row == start, weight[k : k + 1, :], 0.0)
    mix[...] = total.T.astype(BF)


def bias_kernel(place, narrow, broad, own, first, second, third):
    z, y, c = place[0], place[1], place[2]
    here = z * 4 + y

    def put(out, at, early, late):
        back_y = jnp.where(c == 0, early, late)
        back_z = jnp.where(c == 0, late, early)
        chip = ((z + 4 - back_z) % 4) * 4 + (y + 4 - back_y) % 4
        block = pl.multiple_of(chip * 256 + c * 128, 128)
        ahead = chip > here
        for row, gates in ((0, narrow), (4, broad)):
            piece = gates[:, pl.ds(block, 128)] * (-LOG2E)
            out[row : row + gates.shape[0], at : at + 128] = jnp.where(ahead, MASKED, piece)

    put(own, 0, 0, 0)
    for i in range(1, 4):
        put(first, (i - 1) * 128, ORDER[i], 0)
    for i in range(4):
        put(second, i * 128, ORDER[i % 2], 1 if i < 2 else 3)
        put(second, 512 + i * 128, ORDER[2 + i % 2], 1 if i < 2 else 3)
        put(third, i * 128, ORDER[i], 2)


def project_kernel(place, own, other, narrow, broad, *refs):
    outs, total, attn = refs[:4], *refs[4:]
    a, b = own[:, 1024:], other[:, 1024:]
    top = jnp.maximum(a, b)
    wa, wb = jnp.exp2(a - top), jnp.exp2(b - top)
    joined = wa + wb
    wa, wb = wa / joined, wb / joined
    for h in range(6):
        lo, size = (h * 128, 128) if h < 4 else (512 + (h - 4) * 256, 256)
        value = own[:, lo : lo + size] * wa[:, h : h + 1] + other[:, lo : lo + size] * wb[:, h : h + 1]
        attn[:, lo : lo + size] = value.astype(BF)
    for at in range(0, 4096, 1024):
        part = jnp.dot(attn[:, :512], narrow[:, at : at + 1024], preferred_element_type=F32)
        part = part + jnp.dot(attn[:, 512:], broad[:, at : at + 1024], preferred_element_type=F32)
        total[:, at : at + 1024] = part
    for k in range(4):
        outs[k][...] = total[pl.ds(((place[3] + k) % 4) * 32, 32), :].astype(BF)


def dispatch_kernel(place, p0, p1, p2, p3, residual, gain, target, stream_out, normed_out, out, rows, sems):
    mixture = p0[...].astype(F32) + p1[...].astype(F32) + p2[...].astype(F32) + p3[...].astype(F32)
    stream = residual[pl.ds(place[3] * 32, 32), :].astype(F32) + mixture
    stream_out[...] = stream
    scale = lax.rsqrt(jnp.mean(stream * stream, axis=1, keepdims=True) + EPSILON)
    normed = (stream * scale * gain[...]).astype(BF)
    normed_out[...] = normed
    cut = jnp.concatenate([normed[:, g * 1024 : (g + 1) * 1024] for g in range(4)], axis=0)
    row = lax.broadcasted_iota(jnp.int32, (256, 128), 0)
    copies = []
    for at in range(0, 1024, 256):
        pick = row + at == target[0:1, :]
        for k in range(1, 4):
            pick = pick | (row + at == target[k : k + 1, :])
        rows[at : at + 256, :] = jnp.dot(pick.astype(F32).astype(BF), cut, preferred_element_type=F32).astype(BF)
        part = pl.ds(at, 256)
        copies.append(pltpu.make_async_copy(rows.at[part], out.at[part], sems.at[at // 256]))
        copies[-1].start()
    for copy in copies:
        copy.wait()


def silu(v):
    return v / (1.0 + jnp.exp(-v))


def shared_kernel(n0, n1, n2, n3, gate, up, down, o0, o1, o2, o3):
    x = jnp.concatenate([n0[...], n1[...], n2[...], n3[...]], axis=0)
    g = jnp.dot(x, gate[...], preferred_element_type=F32)
    u = jnp.dot(x, up[...], preferred_element_type=F32)
    hidden = (silu(g) * u).astype(BF)
    for at in range(0, 4096, 1024):
        part = jnp.dot(hidden, down[:, at : at + 1024], preferred_element_type=F32).astype(BF)
        for k, out in enumerate((o0, o1, o2, o3)):
            out[:, at : at + 1024] = part[k * 32 : (k + 1) * 32]


def expert_kernel(inbound, gate, up, down, stream, s0, s1, s2, s3, out, base, x, gate_up, down_copy, sems):
    copies = []
    for g in range(4):
        for i, ref in enumerate((gate, up)):
            part = pl.ds(g * 1024, 1024)
            copies.append(pltpu.make_async_copy(ref.at[0, part], gate_up.at[i, part], sems.at[len(copies)]))
    copies.append(pltpu.make_async_copy(down.at[0], down_copy, sems.at[len(copies)]))
    for copy in copies:
        copy.start()
    total = stream[...]
    for s in (s0, s1, s2, s3):
        total = total + s[...].astype(F32)
    base[...] = total
    i = lax.broadcasted_iota(jnp.int32, (256, 256), 0)
    j = lax.broadcasted_iota(jnp.int32, (256, 256), 1)
    order = (j == ((i % 64) // 2) * 8 + (i % 2) * 4 + i // 64).astype(F32).astype(BF)
    back = (i == ((j % 64) // 2) * 8 + (j % 2) * 4 + j // 64).astype(F32).astype(BF)
    for b in range(4):
        rows = jnp.dot(order, inbound[b * 256 : (b + 1) * 256, :], preferred_element_type=F32).astype(BF)
        for g in range(4):
            x[b * 64 : (b + 1) * 64, g * 1024 : (g + 1) * 1024] = rows[g * 64 : (g + 1) * 64]
    gated, upped = jnp.zeros((256, 256), F32), jnp.zeros((256, 256), F32)
    for g in range(4):
        lo, hi = g * 1024, (g + 1) * 1024
        copies[2 * g].wait()
        gated = gated + jnp.dot(x[:, lo:hi], gate_up[0, lo:hi], preferred_element_type=F32)
        copies[2 * g + 1].wait()
        upped = upped + jnp.dot(x[:, lo:hi], gate_up[1, lo:hi], preferred_element_type=F32)
    copies[-1].wait()
    hidden = (silu(gated) * upped).astype(BF)
    for g in range(4):
        part = jnp.dot(hidden, down_copy[:, g * 1024 : (g + 1) * 1024], preferred_element_type=F32)
        x[:, g * 1024 : (g + 1) * 1024] = part.astype(BF)
    for b in range(4):
        rows = jnp.concatenate([x[b * 64 : (b + 1) * 64, g * 1024 : (g + 1) * 1024] for g in range(4)], axis=0)
        out[b * 256 : (b + 1) * 256, :] = jnp.dot(back, rows, preferred_element_type=F32).astype(BF)


def combine_kernel(returned, mix, base, out):
    for g in range(4):
        lo, hi = g * 1024, (g + 1) * 1024
        rows = mix[g * 32 : (g + 1) * 32, :]
        routed = jnp.dot(rows, returned[...], preferred_element_type=F32)
        out[:, lo:hi] = (base[:, lo:hi] + routed).astype(BF)


def attend_kernel(counts, first, last, *refs):
    at = 0

    def take(n):
        nonlocal at
        at += n
        return refs[at - n : at]

    q_own, q_other, core = take(3)
    tiles, planes = [], []
    for n, own_block in counts:
        tiles.append((take(n), take(1)[0], own_block))
        if first and not own_block:
            planes.append(tiles[-1][0][0])
    if not first:
        m_in, l_in, an_in, ab_in = take(4)
    if last:
        own_out, send_out = take(2)
    else:
        m_out, l_out, an_out, ab_out = take(4)

    def keys(ref, lo, hi):
        value = ref[1, :, lo:hi] if any(ref is p for p in planes) else ref[..., lo:hi]
        return value.reshape(-1, hi - lo)

    results = {}
    for group, size, heads, lo in (("n", NARROW_SIZE, 4, 0), ("b", BROAD_SIZE, 2, 256)):
        scale = size**-0.5 * LOG2E
        base = 0 if group == "n" else 4
        row_base = 0 if group == "n" else 1024
        loaded = []
        for arrays, bias, own_block in tiles:
            k = jnp.concatenate([keys(r, lo, lo + size) for r in arrays], axis=0)
            v = jnp.concatenate([keys(r, lo + size, lo + 2 * size) for r in arrays], axis=0)
            loaded.append((k, v, bias, own_block))
        for side, q_ref in ((0, q_own), (1, q_other)):
            for h0 in range(0, heads, 2):
                col = (0 if group == "n" else 512) + h0 * size
                q = jnp.concatenate([q_ref[:, col + i * size : col + (i + 1) * size] for i in range(2)], axis=0)
                rows = row_base + side * heads * 128 + h0 * 128
                arow = rows - row_base
                scores = []
                for k, v, bias, own_block in loaded:
                    s = lax.dot_general(q, k, (((1,), (1,)), ((), ())), preferred_element_type=F32) * scale
                    n = k.shape[0]
                    b = bias[base + h0 : base + h0 + 2, :]
                    s = (s.reshape(2, 128, n) + b[:, None, :]).reshape(256, n)
                    if own_block:
                        qi = lax.broadcasted_iota(jnp.int32, (256, n), 0) % 128
                        ki = lax.broadcasted_iota(jnp.int32, (256, n), 1)
                        offset = 0 if side == 0 else 128 * (1 - 2 * core[0])
                        s = jnp.where(ki <= qi + offset, s, MASKED)
                    scores.append(s)
                m = functools.reduce(jnp.maximum, [jnp.max(s, axis=1, keepdims=True) for s in scores])
                if not first:
                    m_old = m_in[pl.ds(rows, 256), :][:, :1]
                    m = jnp.maximum(m, m_old)
                l = jnp.zeros((256, 1), F32)
                acc = jnp.zeros((256, size), F32)
                for s, (k, v, bias, own_block) in zip(scores, loaded):
                    p = jnp.exp2(s - m)
                    l = l + jnp.sum(p, axis=1, keepdims=True)
                    acc = acc + jnp.dot(p.astype(BF), v, preferred_element_type=F32)
                if not first:
                    a_in = an_in if group == "n" else ab_in
                    factor = jnp.exp2(m_old - m)
                    l = l + l_in[pl.ds(rows, 256), :][:, :1] * factor
                    acc = acc + a_in[pl.ds(arow, 256), :] * factor
                if last:
                    out = own_out if side == 0 else send_out
                    o = acc / l
                    lse = m + jnp.log2(l)
                    for i in range(2):
                        out[:, col + i * size : col + (i + 1) * size] = o[i * 128 : (i + 1) * 128]
                        results[(side, base + h0 + i)] = lse[i * 128 : (i + 1) * 128]
                else:
                    a_out = an_out if group == "n" else ab_out
                    m_out[pl.ds(rows, 256), :] = jnp.broadcast_to(m, (256, 128))
                    l_out[pl.ds(rows, 256), :] = jnp.broadcast_to(l, (256, 128))
                    a_out[pl.ds(arow, 256), :] = acc
    if last:
        lane = lax.broadcasted_iota(jnp.int32, (128, 128), 1)
        for side, out in ((0, own_out), (1, send_out)):
            stats = jnp.zeros((128, 128), F32)
            for h in range(6):
                stats = jnp.where(lane == h, results[(side, h)], stats)
            out[:, 1024:1152] = stats


def attend(q_own, q_other, core, tiles, state, last):
    counts = tuple((len(arrays), own_block) for arrays, _, own_block in tiles)
    operands = [q_own, q_other, core]
    n_keys = 0
    for arrays, bias, _ in tiles:
        operands += list(arrays) + [bias]
        n_keys += bias.shape[1]
    specs = [VMEM] * len(operands)
    specs[2] = SMEM
    if state is not None:
        operands += list(state)
        specs += [VMEM] * 4
    if last:
        shapes = [jax.ShapeDtypeStruct((128, 1152), F32)] * 2
    else:
        shapes = [
            jax.ShapeDtypeStruct((1536, 128), F32),
            jax.ShapeDtypeStruct((1536, 128), F32),
            jax.ShapeDtypeStruct((1024, 128), F32),
            jax.ShapeDtypeStruct((512, 256), F32),
        ]
    return pl.pallas_call(
        functools.partial(attend_kernel, counts, state is None, last),
        out_shape=shapes,
        in_specs=specs,
        out_specs=[VMEM] * len(shapes),
        compiler_params=pltpu.CompilerParams(vmem_limit_bytes=24 * 1024 * 1024),
        cost_estimate=pl.CostEstimate(
            flops=4 * n_keys * 256 * 1024, transcendentals=n_keys * 1536, bytes_accessed=4 * 1024 * 1024
        ),
    )(*operands)


def local(
    query_narrow,
    key_narrow,
    value_narrow,
    gates_narrow,
    query_broad,
    key_broad,
    value_broad,
    gates_broad,
    project_narrow,
    project_broad,
    residual,
    norm_gain,
    route_ids,
    route_weight,
    expert_gate,
    expert_up,
    expert_down,
    shared_gate,
    shared_up,
    shared_down,
):
    z, y, c, t = (lax.axis_index(n).astype(jnp.int32) for n in ("z", "y", "c", "tp"))

    own_kv, q_own = call(
        pack_kernel,
        (key_narrow, value_narrow, key_broad, value_broad, query_narrow, query_broad),
        [shaped((128, 768), BF), shaped((128, 1024), BF)],
        hbm=range(6),
        scratch=[pltpu.SemaphoreType.DMA((6,))],
        moved=0,
    )
    target, mix = call(
        route_kernel,
        (route_ids.T, route_weight.T),
        [shaped((4, 128), jnp.int32), shaped((128, 1024), BF)],
    )
    place = jnp.stack([z, y, c, t])
    q_other = swap_core(q_own)
    line = {}
    for k in (2, 1, 3):
        line[k] = turn(own_kv, k, 0)
    own_bias, bias_1, bias_2, bias_3 = call(
        bias_kernel,
        (place, gates_narrow.T, gates_broad.T),
        [shaped((8, n), F32) for n in (128, 384, 1024, 512)],
        smem=(0,),
    )
    low, high = call(
        stack_kernel,
        [own_kv] + [line[k] for k in ORDER[1:]] + [target, own_bias],
        [shaped((2, 128, 768), BF)] * 2,
    )
    low_back = turn(low, 1, 1)
    high_ahead = turn(high, 3, 1)
    low_ahead = turn(low, 3, 1)
    high_back = turn(high, 1, 1)
    low_far = turn(low_back, 1, 1)
    high_far = turn(high_ahead, 3, 1)

    core = c.reshape(1)
    first_tiles = [((own_kv,), own_bias, True), ((low, high), bias_1, False)]
    state = attend(q_own, q_other, core, first_tiles, None, False)
    second_tiles = [((low_back, low_ahead, high_back, high_ahead), bias_2, False)]
    state = attend(q_own, q_other, core, second_tiles, state, False)
    own_part, send_part = attend(q_own, q_other, core, [((low_far, high_far), bias_3, False)], state, True)
    other_part = swap_core(send_part)

    p0, p1, p2, p3 = call(
        project_kernel,
        (place, own_part, other_part, project_narrow, project_broad),
        [shaped((32, 4096), BF)] * 4,
        smem=(0,),
        scratch=[pltpu.VMEM((128, 4096), F32), pltpu.VMEM((128, 1024), BF)],
        flops=2 * 128 * 1024 * 4096,
    )
    p2 = shift(p2, "tp", 2)
    p1 = shift(p1, "tp", 1)
    p3 = shift(p3, "tp", 3)

    stream, normed, outbound = call(
        dispatch_kernel,
        (place, p0, p1, p2, p3, residual, norm_gain.reshape(1, -1), target),
        [shaped((32, 4096), F32), shaped((32, 4096), BF), pltpu.HBM((1024, 1024), BF)],
        smem=(0,),
        hbm_out=(2,),
        scratch=[pltpu.VMEM((1024, 1024), BF), pltpu.SemaphoreType.DMA((4,))],
        flops=2 * 1024 * 128 * 1024,
    )
    every = SP + ("tp",)
    inbound = lax.all_to_all(outbound.reshape(128, 8, 1024), every, 0, 0, tiled=True)

    n1 = shift(normed, "tp", 1)
    n2 = shift(normed, "tp", 2)
    n3 = shift(normed, "tp", 3)
    s0, s1, s2, s3 = call(
        shared_kernel,
        (normed, n1, n2, n3, shared_gate, shared_up, shared_down),
        [shaped((32, 4096), BF)] * 4,
        flops=2 * 128 * 4096 * 768,
    )
    s1 = shift(s1, "tp", 3)
    s2 = shift(s2, "tp", 2)
    s3 = shift(s3, "tp", 1)

    result, base = call(
        expert_kernel,
        (inbound.reshape(1024, 1024), expert_gate, expert_up, expert_down, stream, s0, s1, s2, s3),
        [shaped((1024, 1024), BF), shaped((32, 4096), F32)],
        hbm=(1, 2, 3),
        scratch=[
            pltpu.VMEM((256, 4096), BF),
            pltpu.VMEM((2, 4096, 256), BF),
            pltpu.VMEM((256, 4096), BF),
            pltpu.SemaphoreType.DMA((9,)),
        ],
        mib=20,
        moved=0,
        flops=2 * 256 * 4096 * 768,
    )
    returned = lax.all_to_all(result.reshape(128, 8, 1024), every, 0, 0, tiled=True)
    (out,) = call(
        combine_kernel,
        (returned.reshape(1024, 1024), mix, base),
        [shaped((32, 4096), BF)],
        flops=2 * 128 * 1024 * 1024,
    )
    return out


def solution(mesh):
    mesh = Mesh(mesh.devices.reshape(4, 4, 2, 4), ("z", "y", "c", "tp"))
    every = SP + ("tp",)
    placed = (
        P(SP, "tp"),
        P(SP, "tp"),
        P(SP, "tp"),
        P(None, "tp"),
        P(SP, "tp"),
        P(SP, "tp"),
        P(SP, "tp"),
        P(None, "tp"),
        P("tp", None),
        P("tp", None),
        P(SP, None),
        P(),
        P(every, None),
        P(every, None),
        P(every, None, None),
        P(every, None, None),
        P(every, None, None),
        P(None, "tp"),
        P(None, "tp"),
        P("tp", None),
    )

    return jax.shard_map(local, mesh=mesh, in_specs=placed, out_specs=P(every, None), check_vma=False)
```

```python
import functools

import jax
import jax.numpy as jnp
from jax import lax
from jax.experimental import pallas as pl
from jax.experimental.pallas import tpu as pltpu
from jax.sharding import Mesh
from jax.sharding import PartitionSpec as P


SP = ("z", "y", "c")
NARROW_SIZE = 128
BROAD_SIZE = 256
LOG2E = 1.4426950408889634
MASKED = -1e30
EPSILON = 1e-06
ORDER = (0, 1, 3, 2)
VMEM = pl.BlockSpec(memory_space=pltpu.VMEM)
SMEM = pl.BlockSpec(memory_space=pltpu.SMEM)
HBM = pl.BlockSpec(memory_space=pltpu.HBM)
BF = jnp.bfloat16
F32 = jnp.float32


def shift(x, axis, k):
    return lax.ppermute(x, axis, [(i, (i + k) % 4) for i in range(4)])


def swap_core(x):
    return lax.ppermute(x, "c", [(0, 1), (1, 0)])


def turn(x, k, phase):
    pairs = []
    for z in range(4):
        for y in range(4):
            for c in range(2):
                to_z, to_y = (z, (y + k) % 4) if c == phase else ((z + k) % 4, y)
                pairs.append(((z * 4 + y) * 2 + c, (to_z * 4 + to_y) * 2 + c))
    return lax.ppermute(x, SP, pairs)


def call(kernel, operands, shapes, smem=(), hbm=(), hbm_out=(), scratch=(), mib=16, flops=0, moved=2**21):
    operands = [
        pltpu.with_memory_space_constraint(x, pltpu.HBM) if i in hbm else x for i, x in enumerate(operands)
    ]
    return pl.pallas_call(
        kernel,
        out_shape=shapes,
        in_specs=[SMEM if i in smem else HBM if i in hbm else VMEM for i in range(len(operands))],
        out_specs=[HBM if i in hbm_out else VMEM for i in range(len(shapes))],
        scratch_shapes=list(scratch),
        compiler_params=pltpu.CompilerParams(vmem_limit_bytes=mib * 1024 * 1024),
        cost_estimate=pl.CostEstimate(flops=flops, transcendentals=0, bytes_accessed=moved),
    )(*operands)


def shaped(shape, dtype):
    return jax.ShapeDtypeStruct(shape, dtype)


def pack_kernel(kn, vn, kb, vb, qn, qb, kv, q, sems):
    copies = []
    for ref, out, at in ((kn, kv, 0), (vn, kv, 128), (kb, kv, 256), (vb, kv, 512), (qn, q, 0), (qb, q, 512)):
        target = out.at[:, at : at + ref.shape[1]]
        copies.append(pltpu.make_async_copy(ref, target, sems.at[len(copies)]))
    for copy in copies:
        copy.start()
    for copy in copies:
        copy.wait()


def stack_kernel(a, b, c, d, routed, biased, low, high):
    for out, i, ref in ((low, 0, a), (low, 1, b), (high, 0, c), (high, 1, d)):
        out[i] = ref[...]


def tables_kernel(place, ids_hbm, weight_hbm, narrow_hbm, broad_hbm, target, mix, own, first, second, third, *scratch):
    ids_in, weight_in, narrow, broad, sems = scratch
    copies = []
    for ref, held in ((narrow_hbm, narrow), (broad_hbm, broad), (ids_hbm, ids_in), (weight_hbm, weight_in)):
        copies.append(pltpu.make_async_copy(ref, held, sems.at[len(copies)]))
    for copy in copies:
        copy.start()
    for copy in copies:
        copy.wait()
    ids = jnp.concatenate([ids_in[...]] * 4, axis=1)
    weight = jnp.concatenate([weight_in[...].astype(BF).astype(F32)] * 4, axis=1)
    expert = lax.broadcasted_iota(jnp.int32, (128, 128), 0)
    column = lax.broadcasted_iota(jnp.int32, (128, 128), 1)
    named = jnp.zeros((128, 128), F32)
    for k in range(4):
        named = named + jnp.where(expert == ids[k : k + 1, :], 1.0, 0.0)
    earlier = jnp.where((expert < 32) & (expert < column % 32), 1.0, 0.0).astype(BF)
    before = jnp.dot(named.astype(BF), earlier, preferred_element_type=F32)
    row = lax.broadcasted_iota(jnp.int32, (1024, 128), 0)
    total = jnp.zeros((1024, 128), F32)
    for k in range(4):
        slot = jnp.sum(jnp.where(expert == ids[k : k + 1, :], before, 0.0), axis=0, keepdims=True)
        start = ids[k : k + 1, :] * 8 + slot.astype(jnp.int32) * 4 + column[:1] // 32
        target[k : k + 1, :] = start
        total = total + jnp.where(row == start, weight[k : k + 1, :], 0.0)
    mix[...] = total.T.astype(BF)


    z, y, c = place[0], place[1], place[2]
    here = z * 4 + y

    def put(out, at, early, late):
        back_y = jnp.where(c == 0, early, late)
        back_z = jnp.where(c == 0, late, early)
        chip = ((z + 4 - back_z) % 4) * 4 + (y + 4 - back_y) % 4
        block = pl.multiple_of(chip * 256 + c * 128, 128)
        ahead = chip > here
        for row, gates in ((0, narrow), (4, broad)):
            piece = gates[:, pl.ds(block, 128)] * (-LOG2E)
            out[row : row + gates.shape[0], at : at + 128] = jnp.where(ahead, MASKED, piece)

    put(own, 0, 0, 0)
    for i in range(1, 4):
        put(first, (i - 1) * 128, ORDER[i], 0)
    for i in range(4):
        put(second, i * 128, ORDER[i % 2], 1 if i < 2 else 3)
        put(second, 512 + i * 128, ORDER[2 + i % 2], 1 if i < 2 else 3)
        put(third, i * 128, ORDER[i], 2)


def project_kernel(place, own, other, narrow, broad, *refs):
    outs, total, attn = refs[:4], *refs[4:]
    a, b = own[:, 1024:], other[:, 1024:]
    top = jnp.maximum(a, b)
    wa, wb = jnp.exp2(a - top), jnp.exp2(b - top)
    joined = wa + wb
    wa, wb = wa / joined, wb / joined
    for h in range(6):
        lo, size = (h * 128, 128) if h < 4 else (512 + (h - 4) * 256, 256)
        value = own[:, lo : lo + size] * wa[:, h : h + 1] + other[:, lo : lo + size] * wb[:, h : h + 1]
        attn[:, lo : lo + size] = value.astype(BF)
    for at in range(0, 4096, 1024):
        part = jnp.dot(attn[:, :512], narrow[:, at : at + 1024], preferred_element_type=F32)
        part = part + jnp.dot(attn[:, 512:], broad[:, at : at + 1024], preferred_element_type=F32)
        total[:, at : at + 1024] = part
    for k in range(4):
        outs[k][...] = total[pl.ds(((place[3] + k) % 4) * 32, 32), :].astype(BF)


def dispatch_kernel(place, p0, p1, p2, p3, residual, gain, target, stream_out, normed_out, out, rows, sems):
    mixture = p0[...].astype(F32) + p1[...].astype(F32) + p2[...].astype(F32) + p3[...].astype(F32)
    stream = residual[pl.ds(place[3] * 32, 32), :].astype(F32) + mixture
    stream_out[...] = stream
    scale = lax.rsqrt(jnp.mean(stream * stream, axis=1, keepdims=True) + EPSILON)
    normed = (stream * scale * gain[...]).astype(BF)
    normed_out[...] = normed
    cut = jnp.concatenate([normed[:, g * 1024 : (g + 1) * 1024] for g in range(4)], axis=0)
    row = lax.broadcasted_iota(jnp.int32, (256, 128), 0)
    copies = []
    for at in range(0, 1024, 256):
        pick = row + at == target[0:1, :]
        for k in range(1, 4):
            pick = pick | (row + at == target[k : k + 1, :])
        rows[at : at + 256, :] = jnp.dot(pick.astype(F32).astype(BF), cut, preferred_element_type=F32).astype(BF)
        part = pl.ds(at, 256)
        copies.append(pltpu.make_async_copy(rows.at[part], out.at[part], sems.at[at // 256]))
        copies[-1].start()
    for copy in copies:
        copy.wait()


def fetch(pairs, sems):
    copies = [pltpu.make_async_copy(ref, held, sems.at[i]) for i, (ref, held) in enumerate(pairs)]
    for copy in copies:
        copy.start()
    return copies


def silu(v):
    return v / (1.0 + jnp.exp(-v))


def shared_kernel(n0, n1, n2, n3, gate_hbm, up_hbm, down_hbm, o0, o1, o2, o3, gate, up, down, sems):
    fetched = fetch(((gate_hbm, gate), (up_hbm, up), (down_hbm, down)), sems)
    x = jnp.concatenate([n0[...], n1[...], n2[...], n3[...]], axis=0)
    fetched[0].wait()
    g = jnp.dot(x, gate[...], preferred_element_type=F32)
    fetched[1].wait()
    u = jnp.dot(x, up[...], preferred_element_type=F32)
    fetched[2].wait()
    hidden = (silu(g) * u).astype(BF)
    for at in range(0, 4096, 1024):
        part = jnp.dot(hidden, down[:, at : at + 1024], preferred_element_type=F32).astype(BF)
        for k, out in enumerate((o0, o1, o2, o3)):
            out[:, at : at + 1024] = part[k * 32 : (k + 1) * 32]


def expert_kernel(inbound, gate_hbm, up_hbm, down_hbm, out, x, rows_out, gate, up, down, weight_sems, sems):
    pairs = [(ref.at[0], held) for ref, held in ((gate_hbm, gate), (up_hbm, up), (down_hbm, down))]
    fetched = fetch(pairs, weight_sems)
    i = lax.broadcasted_iota(jnp.int32, (256, 256), 0)
    j = lax.broadcasted_iota(jnp.int32, (256, 256), 1)
    order = (j == ((i % 64) // 2) * 8 + (i % 2) * 4 + i // 64).astype(F32).astype(BF)
    back = (i == ((j % 64) // 2) * 8 + (j % 2) * 4 + j // 64).astype(F32).astype(BF)
    for b in range(4):
        rows = jnp.dot(order, inbound[b * 256 : (b + 1) * 256, :], preferred_element_type=F32).astype(BF)
        for g in range(4):
            x[b * 64 : (b + 1) * 64, g * 1024 : (g + 1) * 1024] = rows[g * 64 : (g + 1) * 64]
    fetched[0].wait()
    gated = jnp.dot(x[...], gate[...], preferred_element_type=F32)
    fetched[1].wait()
    upped = jnp.dot(x[...], up[...], preferred_element_type=F32)
    fetched[2].wait()
    hidden = (silu(gated) * upped).astype(BF)
    for g in range(4):
        part = jnp.dot(hidden, down[:, g * 1024 : (g + 1) * 1024], preferred_element_type=F32)
        x[:, g * 1024 : (g + 1) * 1024] = part.astype(BF)
    copies = []
    for b in range(4):
        rows = jnp.concatenate([x[b * 64 : (b + 1) * 64, g * 1024 : (g + 1) * 1024] for g in range(4)], axis=0)
        part = pl.ds(b * 256, 256)
        rows_out[part, :] = jnp.dot(back, rows, preferred_element_type=F32).astype(BF)
        copies.append(pltpu.make_async_copy(rows_out.at[part], out.at[part], sems.at[b]))
        copies[-1].start()
    for copy in copies:
        copy.wait()


def combine_kernel(returned, mix, stream, s0, s1, s2, s3, out):
    routed = jnp.dot(mix[...], returned[...], preferred_element_type=F32)
    for g in range(4):
        lo, hi = g * 1024, (g + 1) * 1024
        total = stream[:, lo:hi] + routed[g * 32 : (g + 1) * 32]
        for s in (s0, s1, s2, s3):
            total = total + s[:, lo:hi].astype(F32)
        out[:, lo:hi] = total.astype(BF)


def attend_kernel(counts, first, last, *refs):
    at = 0

    def take(n):
        nonlocal at
        at += n
        return refs[at - n : at]

    q_own, q_other, core = take(3)
    tiles, planes = [], []
    for n, own_block in counts:
        tiles.append((take(n), take(1)[0], own_block))
        if first and not own_block:
            planes.append(tiles[-1][0][0])
    if not first:
        m_in, l_in, an_in, ab_in = take(4)
    if last:
        own_out, send_out = take(2)
    else:
        m_out, l_out, an_out, ab_out = take(4)

    def keys(ref, lo, hi):
        value = ref[1, :, lo:hi] if any(ref is p for p in planes) else ref[..., lo:hi]
        return value.reshape(-1, hi - lo)

    results = {}
    for group, size, heads, lo in (("n", NARROW_SIZE, 4, 0), ("b", BROAD_SIZE, 2, 256)):
        scale = size**-0.5 * LOG2E
        base = 0 if group == "n" else 4
        row_base = 0 if group == "n" else 1024
        loaded = []
        for arrays, bias, own_block in tiles:
            k = jnp.concatenate([keys(r, lo, lo + size) for r in arrays], axis=0)
            v = jnp.concatenate([keys(r, lo + size, lo + 2 * size) for r in arrays], axis=0)
            loaded.append((k, v, bias, own_block))
        for side, q_ref in ((0, q_own), (1, q_other)):
            for h0 in range(0, heads, 2):
                col = (0 if group == "n" else 512) + h0 * size
                q = jnp.concatenate([q_ref[:, col + i * size : col + (i + 1) * size] for i in range(2)], axis=0)
                rows = row_base + side * heads * 128 + h0 * 128
                arow = rows - row_base
                scores = []
                for k, v, bias, own_block in loaded:
                    s = lax.dot_general(q, k, (((1,), (1,)), ((), ())), preferred_element_type=F32) * scale
                    n = k.shape[0]
                    b = bias[base + h0 : base + h0 + 2, :]
                    s = (s.reshape(2, 128, n) + b[:, None, :]).reshape(256, n)
                    if own_block:
                        qi = lax.broadcasted_iota(jnp.int32, (256, n), 0) % 128
                        ki = lax.broadcasted_iota(jnp.int32, (256, n), 1)
                        offset = 0 if side == 0 else 128 * (1 - 2 * core[0])
                        s = jnp.where(ki <= qi + offset, s, MASKED)
                    scores.append(s)
                m = functools.reduce(jnp.maximum, [jnp.max(s, axis=1, keepdims=True) for s in scores])
                if not first:
                    m_old = m_in[pl.ds(rows, 256), :][:, :1]
                    m = jnp.maximum(m, m_old)
                l = jnp.zeros((256, 1), F32)
                acc = jnp.zeros((256, size), F32)
                for s, (k, v, bias, own_block) in zip(scores, loaded):
                    p = jnp.exp2(s - m)
                    l = l + jnp.sum(p, axis=1, keepdims=True)
                    acc = acc + jnp.dot(p.astype(BF), v, preferred_element_type=F32)
                if not first:
                    a_in = an_in if group == "n" else ab_in
                    factor = jnp.exp2(m_old - m)
                    l = l + l_in[pl.ds(rows, 256), :][:, :1] * factor
                    acc = acc + a_in[pl.ds(arow, 256), :] * factor
                if last:
                    out = own_out if side == 0 else send_out
                    o = acc / l
                    lse = m + jnp.log2(l)
                    for i in range(2):
                        out[:, col + i * size : col + (i + 1) * size] = o[i * 128 : (i + 1) * 128]
                        results[(side, base + h0 + i)] = lse[i * 128 : (i + 1) * 128]
                else:
                    a_out = an_out if group == "n" else ab_out
                    m_out[pl.ds(rows, 256), :] = jnp.broadcast_to(m, (256, 128))
                    l_out[pl.ds(rows, 256), :] = jnp.broadcast_to(l, (256, 128))
                    a_out[pl.ds(arow, 256), :] = acc
    if last:
        lane = lax.broadcasted_iota(jnp.int32, (128, 128), 1)
        for side, out in ((0, own_out), (1, send_out)):
            stats = jnp.zeros((128, 128), F32)
            for h in range(6):
                stats = jnp.where(lane == h, results[(side, h)], stats)
            out[:, 1024:1152] = stats


def attend(q_own, q_other, core, tiles, state, last):
    counts = tuple((len(arrays), own_block) for arrays, _, own_block in tiles)
    operands = [q_own, q_other, core]
    n_keys = 0
    for arrays, bias, _ in tiles:
        operands += list(arrays) + [bias]
        n_keys += bias.shape[1]
    specs = [VMEM] * len(operands)
    specs[2] = SMEM
    if state is not None:
        operands += list(state)
        specs += [VMEM] * 4
    if last:
        shapes = [jax.ShapeDtypeStruct((128, 1152), F32)] * 2
    else:
        shapes = [
            jax.ShapeDtypeStruct((1536, 128), F32),
            jax.ShapeDtypeStruct((1536, 128), F32),
            jax.ShapeDtypeStruct((1024, 128), F32),
            jax.ShapeDtypeStruct((512, 256), F32),
        ]
    return pl.pallas_call(
        functools.partial(attend_kernel, counts, state is None, last),
        out_shape=shapes,
        in_specs=specs,
        out_specs=[VMEM] * len(shapes),
        compiler_params=pltpu.CompilerParams(vmem_limit_bytes=24 * 1024 * 1024),
        cost_estimate=pl.CostEstimate(
            flops=4 * n_keys * 256 * 1024, transcendentals=n_keys * 1536, bytes_accessed=4 * 1024 * 1024
        ),
    )(*operands)


def local(
    query_narrow,
    key_narrow,
    value_narrow,
    gates_narrow,
    query_broad,
    key_broad,
    value_broad,
    gates_broad,
    project_narrow,
    project_broad,
    residual,
    norm_gain,
    route_ids,
    route_weight,
    expert_gate,
    expert_up,
    expert_down,
    shared_gate,
    shared_up,
    shared_down,
):
    z, y, c, t = (lax.axis_index(n).astype(jnp.int32) for n in ("z", "y", "c", "tp"))

    own_kv, q_own = call(
        pack_kernel,
        (key_narrow, value_narrow, key_broad, value_broad, query_narrow, query_broad),
        [shaped((128, 768), BF), shaped((128, 1024), BF)],
        hbm=range(6),
        scratch=[pltpu.SemaphoreType.DMA((6,))],
        moved=0,
    )
    place = jnp.stack([z, y, c, t])
    q_other = swap_core(q_own)
    line = {}
    for k in (2, 1, 3):
        line[k] = turn(own_kv, k, 0)
    target, mix, own_bias, bias_1, bias_2, bias_3 = call(
        tables_kernel,
        (place, route_ids.T, route_weight.T, gates_narrow.T, gates_broad.T),
        [shaped((4, 128), jnp.int32), shaped((128, 1024), BF)] + [shaped((8, n), F32) for n in (128, 384, 1024, 512)],
        smem=(0,),
        hbm=(1, 2, 3, 4),
        scratch=[
            pltpu.VMEM((4, 32), jnp.int32),
            pltpu.VMEM((4, 32), F32),
            pltpu.VMEM((4, 4096), F32),
            pltpu.VMEM((2, 4096), F32),
            pltpu.SemaphoreType.DMA((4,)),
        ],
    )
    low, high = call(
        stack_kernel,
        [own_kv] + [line[k] for k in ORDER[1:]] + [target, own_bias],
        [shaped((2, 128, 768), BF)] * 2,
    )
    low_back = turn(low, 1, 1)
    high_ahead = turn(high, 3, 1)
    low_ahead = turn(low, 3, 1)
    high_back = turn(high, 1, 1)
    low_far = turn(low_back, 1, 1)
    high_far = turn(high_ahead, 3, 1)

    core = c.reshape(1)
    first_tiles = [((own_kv,), own_bias, True), ((low, high), bias_1, False)]
    state = attend(q_own, q_other, core, first_tiles, None, False)
    second_tiles = [((low_back, low_ahead, high_back, high_ahead), bias_2, False)]
    state = attend(q_own, q_other, core, second_tiles, state, False)
    own_part, send_part = attend(q_own, q_other, core, [((low_far, high_far), bias_3, False)], state, True)
    other_part = swap_core(send_part)

    p0, p1, p2, p3 = call(
        project_kernel,
        (place, own_part, other_part, project_narrow, project_broad),
        [shaped((32, 4096), BF)] * 4,
        smem=(0,),
        scratch=[pltpu.VMEM((128, 4096), F32), pltpu.VMEM((128, 1024), BF)],
        flops=2 * 128 * 1024 * 4096,
    )
    p2 = shift(p2, "tp", 2)
    p1 = shift(p1, "tp", 1)
    p3 = shift(p3, "tp", 3)

    stream, normed, outbound = call(
        dispatch_kernel,
        (place, p0, p1, p2, p3, residual, norm_gain.reshape(1, -1), target),
        [shaped((32, 4096), F32), shaped((32, 4096), BF), pltpu.HBM((1024, 1024), BF)],
        smem=(0,),
        hbm_out=(2,),
        scratch=[pltpu.VMEM((1024, 1024), BF), pltpu.SemaphoreType.DMA((4,))],
        flops=2 * 1024 * 128 * 1024,
    )
    every = SP + ("tp",)
    inbound = lax.all_to_all(outbound.reshape(128, 8, 1024), every, 0, 0, tiled=True)

    n1 = shift(normed, "tp", 1)
    n2 = shift(normed, "tp", 2)
    n3 = shift(normed, "tp", 3)
    s0, s1, s2, s3 = call(
        shared_kernel,
        (normed, n1, n2, n3, shared_gate, shared_up, shared_down),
        [shaped((32, 4096), BF)] * 4,
        hbm=(4, 5, 6),
        scratch=[
            pltpu.VMEM((4096, 256), BF),
            pltpu.VMEM((4096, 256), BF),
            pltpu.VMEM((256, 4096), BF),
            pltpu.SemaphoreType.DMA((3,)),
        ],
        mib=20,
        flops=2 * 128 * 4096 * 768,
    )
    s1 = shift(s1, "tp", 3)
    s2 = shift(s2, "tp", 2)
    s3 = shift(s3, "tp", 1)

    (result,) = call(
        expert_kernel,
        (inbound.reshape(1024, 1024), expert_gate, expert_up, expert_down),
        [pltpu.HBM((1024, 1024), BF)],
        hbm=(1, 2, 3),
        hbm_out=(0,),
        scratch=[
            pltpu.VMEM((256, 4096), BF),
            pltpu.VMEM((1024, 1024), BF),
            pltpu.VMEM((4096, 256), BF),
            pltpu.VMEM((4096, 256), BF),
            pltpu.VMEM((256, 4096), BF),
            pltpu.SemaphoreType.DMA((3,)),
            pltpu.SemaphoreType.DMA((4,)),
        ],
        mib=20,
        flops=2 * 256 * 4096 * 768,
    )
    returned = lax.all_to_all(result.reshape(128, 8, 1024), every, 0, 0, tiled=True)
    (out,) = call(
        combine_kernel,
        (returned.reshape(1024, 1024), mix, stream, s0, s1, s2, s3),
        [shaped((32, 4096), BF)],
        flops=2 * 128 * 1024 * 1024,
    )
    return out


def solution(mesh):
    mesh = Mesh(mesh.devices.reshape(4, 4, 2, 4), ("z", "y", "c", "tp"))
    every = SP + ("tp",)
    placed = (
        P(SP, "tp"),
        P(SP, "tp"),
        P(SP, "tp"),
        P(None, "tp"),
        P(SP, "tp"),
        P(SP, "tp"),
        P(SP, "tp"),
        P(None, "tp"),
        P("tp", None),
        P("tp", None),
        P(SP, None),
        P(),
        P(every, None),
        P(every, None),
        P(every, None, None),
        P(every, None, None),
        P(every, None, None),
        P(None, "tp"),
        P(None, "tp"),
        P("tp", None),
    )

    return jax.shard_map(local, mesh=mesh, in_specs=placed, out_specs=P(every, None), check_vma=False)
```

```python
import functools

import jax
import jax.numpy as jnp
from jax import lax
from jax.experimental import pallas as pl
from jax.experimental.pallas import tpu as pltpu
from jax.sharding import Mesh
from jax.sharding import PartitionSpec as P


SP = ("z", "y", "c")
NARROW_SIZE = 128
BROAD_SIZE = 256
LOG2E = 1.4426950408889634
MASKED = -1e30
EPSILON = 1e-06
ORDER = (0, 1, 3, 2)
VMEM = pl.BlockSpec(memory_space=pltpu.VMEM)
SMEM = pl.BlockSpec(memory_space=pltpu.SMEM)
HBM = pl.BlockSpec(memory_space=pltpu.HBM)
BF = jnp.bfloat16
F32 = jnp.float32


def shift(x, axis, k):
    return lax.ppermute(x, axis, [(i, (i + k) % 4) for i in range(4)])


def swap_core(x):
    return lax.ppermute(x, "c", [(0, 1), (1, 0)])


def turn(x, k, phase):
    pairs = []
    for z in range(4):
        for y in range(4):
            for c in range(2):
                to_z, to_y = (z, (y + k) % 4) if c == phase else ((z + k) % 4, y)
                pairs.append(((z * 4 + y) * 2 + c, (to_z * 4 + to_y) * 2 + c))
    return lax.ppermute(x, SP, pairs)


def call(kernel, operands, shapes, smem=(), hbm=(), hbm_out=(), scratch=(), mib=16, flops=0, moved=2**21):
    operands = [
        pltpu.with_memory_space_constraint(x, pltpu.HBM) if i in hbm else x for i, x in enumerate(operands)
    ]
    return pl.pallas_call(
        kernel,
        out_shape=shapes,
        in_specs=[SMEM if i in smem else HBM if i in hbm else VMEM for i in range(len(operands))],
        out_specs=[HBM if i in hbm_out else VMEM for i in range(len(shapes))],
        scratch_shapes=list(scratch),
        compiler_params=pltpu.CompilerParams(vmem_limit_bytes=mib * 1024 * 1024),
        cost_estimate=pl.CostEstimate(flops=flops, transcendentals=0, bytes_accessed=moved),
    )(*operands)


def shaped(shape, dtype):
    return jax.ShapeDtypeStruct(shape, dtype)


def pack_kernel(kn, vn, kb, vb, qn, qb, kv, q, sems):
    copies = []
    for ref, out, at in ((kn, kv, 0), (vn, kv, 128), (kb, kv, 256), (vb, kv, 512), (qn, q, 0), (qb, q, 512)):
        target = out.at[:, at : at + ref.shape[1]]
        copies.append(pltpu.make_async_copy(ref, target, sems.at[len(copies)]))
    for copy in copies:
        copy.start()
    for copy in copies:
        copy.wait()


def stack_kernel(a, b, c, d, routed, biased, low, high):
    for out, i, ref in ((low, 0, a), (low, 1, b), (high, 0, c), (high, 1, d)):
        out[i] = ref[...]


def tables_kernel(place, ids_hbm, weight_hbm, narrow_hbm, broad_hbm, target, mix, own, first, second, third, *scratch):
    ids_in, weight_in, narrow, broad, sems = scratch
    copies = []
    for ref, held in ((narrow_hbm, narrow), (broad_hbm, broad), (ids_hbm, ids_in), (weight_hbm, weight_in)):
        copies.append(pltpu.make_async_copy(ref, held, sems.at[len(copies)]))
    for copy in copies:
        copy.start()
    for copy in copies:
        copy.wait()
    ids = jnp.concatenate([ids_in[...]] * 4, axis=1)
    weight = jnp.concatenate([weight_in[...].astype(BF).astype(F32)] * 4, axis=1)
    expert = lax.broadcasted_iota(jnp.int32, (128, 128), 0)
    column = lax.broadcasted_iota(jnp.int32, (128, 128), 1)
    named = jnp.zeros((128, 128), F32)
    for k in range(4):
        named = named + jnp.where(expert == ids[k : k + 1, :], 1.0, 0.0)
    earlier = jnp.where((expert < 32) & (expert < column % 32), 1.0, 0.0).astype(BF)
    before = jnp.dot(named.astype(BF), earlier, preferred_element_type=F32)
    row = lax.broadcasted_iota(jnp.int32, (1024, 128), 0)
    total = jnp.zeros((1024, 128), F32)
    for k in range(4):
        slot = jnp.sum(jnp.where(expert == ids[k : k + 1, :], before, 0.0), axis=0, keepdims=True)
        start = ids[k : k + 1, :] * 8 + slot.astype(jnp.int32) * 4 + column[:1] // 32
        target[k : k + 1, :] = start
        total = total + jnp.where(row == start, weight[k : k + 1, :], 0.0)
    mix[...] = total.T.astype(BF)


    z, y, c = place[0], place[1], place[2]
    here = z * 4 + y

    def put(out, at, early, late):
        back_y = jnp.where(c == 0, early, late)
        back_z = jnp.where(c == 0, late, early)
        chip = ((z + 4 - back_z) % 4) * 4 + (y + 4 - back_y) % 4
        block = pl.multiple_of(chip * 256 + c * 128, 128)
        ahead = chip > here
        for row, gates in ((0, narrow), (4, broad)):
            piece = gates[:, pl.ds(block, 128)] * (-LOG2E)
            out[row : row + gates.shape[0], at : at + 128] = jnp.where(ahead, MASKED, piece)

    put(own, 0, 0, 0)
    for i in range(1, 4):
        put(first, (i - 1) * 128, ORDER[i], 0)
    for i in range(4):
        put(second, i * 128, ORDER[i % 2], 1 if i < 2 else 3)
        put(second, 512 + i * 128, ORDER[2 + i % 2], 1 if i < 2 else 3)
        put(third, i * 128, ORDER[i], 2)


def project_kernel(place, own, other, narrow, broad, *refs):
    outs, total, attn = refs[:4], *refs[4:]
    a, b = own[:, 1024:], other[:, 1024:]
    top = jnp.maximum(a, b)
    wa, wb = jnp.exp2(a - top), jnp.exp2(b - top)
    joined = wa + wb
    wa, wb = wa / joined, wb / joined
    for h in range(6):
        lo, size = (h * 128, 128) if h < 4 else (512 + (h - 4) * 256, 256)
        value = own[:, lo : lo + size] * wa[:, h : h + 1] + other[:, lo : lo + size] * wb[:, h : h + 1]
        attn[:, lo : lo + size] = value.astype(BF)
    for at in range(0, 4096, 1024):
        part = jnp.dot(attn[:, :512], narrow[:, at : at + 1024], preferred_element_type=F32)
        part = part + jnp.dot(attn[:, 512:], broad[:, at : at + 1024], preferred_element_type=F32)
        total[:, at : at + 1024] = part
    for k in range(4):
        outs[k][...] = total[pl.ds(((place[3] + k) % 4) * 32, 32), :].astype(BF)


def dispatch_kernel(place, p0, p1, p2, p3, residual, gain, target, stream_out, normed_out, out, rows, sems):
    mixture = p0[...].astype(F32) + p1[...].astype(F32) + p2[...].astype(F32) + p3[...].astype(F32)
    stream = residual[pl.ds(place[3] * 32, 32), :].astype(F32) + mixture
    stream_out[...] = stream
    scale = lax.rsqrt(jnp.mean(stream * stream, axis=1, keepdims=True) + EPSILON)
    normed = (stream * scale * gain[...]).astype(BF)
    normed_out[...] = normed
    cut = jnp.concatenate([normed[:, g * 1024 : (g + 1) * 1024] for g in range(4)], axis=0)
    row = lax.broadcasted_iota(jnp.int32, (256, 128), 0)
    copies = []
    for at in range(0, 1024, 256):
        pick = row + at == target[0:1, :]
        for k in range(1, 4):
            pick = pick | (row + at == target[k : k + 1, :])
        rows[at : at + 256, :] = jnp.dot(pick.astype(F32).astype(BF), cut, preferred_element_type=F32).astype(BF)
        part = pl.ds(at, 256)
        copies.append(pltpu.make_async_copy(rows.at[part], out.at[part], sems.at[at // 256]))
        copies[-1].start()
    for copy in copies:
        copy.wait()


def fetch(pairs, sems):
    copies = [pltpu.make_async_copy(ref, held, sems.at[i]) for i, (ref, held) in enumerate(pairs)]
    for copy in copies:
        copy.start()
    return copies


def silu(v):
    return v / (1.0 + jnp.exp(-v))


def shared_kernel(n0, n1, n2, n3, gate_hbm, up_hbm, down_hbm, o0, o1, o2, o3, gate, up, down, sems):
    fetched = fetch(((gate_hbm, gate), (up_hbm, up), (down_hbm, down)), sems)
    x = jnp.concatenate([n0[...], n1[...], n2[...], n3[...]], axis=0)
    fetched[0].wait()
    g = jnp.dot(x, gate[...], preferred_element_type=F32)
    fetched[1].wait()
    u = jnp.dot(x, up[...], preferred_element_type=F32)
    fetched[2].wait()
    hidden = (silu(g) * u).astype(BF)
    for at in range(0, 4096, 1024):
        part = jnp.dot(hidden, down[:, at : at + 1024], preferred_element_type=F32).astype(BF)
        for k, out in enumerate((o0, o1, o2, o3)):
            out[:, at : at + 1024] = part[k * 32 : (k + 1) * 32]


def expert_kernel(inbound, gate_hbm, up_hbm, down_hbm, out, x, rows_out, gate, up, down, weight_sems, sems):
    pairs = []
    for g in range(4):
        part = pl.ds(g * 1024, 1024)
        pairs += [(ref.at[0, part], held.at[part]) for ref, held in ((gate_hbm, gate), (up_hbm, up))]
    fetched = fetch(pairs + [(down_hbm.at[0], down)], weight_sems)
    i = lax.broadcasted_iota(jnp.int32, (256, 256), 0)
    j = lax.broadcasted_iota(jnp.int32, (256, 256), 1)
    order = (j == ((i % 64) // 2) * 8 + (i % 2) * 4 + i // 64).astype(F32).astype(BF)
    back = (i == ((j % 64) // 2) * 8 + (j % 2) * 4 + j // 64).astype(F32).astype(BF)
    for b in range(4):
        rows = jnp.dot(order, inbound[b * 256 : (b + 1) * 256, :], preferred_element_type=F32).astype(BF)
        for g in range(4):
            x[b * 64 : (b + 1) * 64, g * 1024 : (g + 1) * 1024] = rows[g * 64 : (g + 1) * 64]
    gated, upped = jnp.zeros((256, 256), F32), jnp.zeros((256, 256), F32)
    for g in range(4):
        lo, hi = g * 1024, (g + 1) * 1024
        fetched[2 * g].wait()
        fetched[2 * g + 1].wait()
        gated = gated + jnp.dot(x[:, lo:hi], gate[lo:hi], preferred_element_type=F32)
        upped = upped + jnp.dot(x[:, lo:hi], up[lo:hi], preferred_element_type=F32)
    fetched[8].wait()
    hidden = (silu(gated) * upped).astype(BF)
    for g in range(4):
        part = jnp.dot(hidden, down[:, g * 1024 : (g + 1) * 1024], preferred_element_type=F32)
        x[:, g * 1024 : (g + 1) * 1024] = part.astype(BF)
    copies = []
    for b in range(4):
        rows = jnp.concatenate([x[b * 64 : (b + 1) * 64, g * 1024 : (g + 1) * 1024] for g in range(4)], axis=0)
        part = pl.ds(b * 256, 256)
        rows_out[part, :] = jnp.dot(back, rows, preferred_element_type=F32).astype(BF)
        copies.append(pltpu.make_async_copy(rows_out.at[part], out.at[part], sems.at[b]))
        copies[-1].start()
    for copy in copies:
        copy.wait()


def combine_kernel(returned, mix, stream, s0, s1, s2, s3, out):
    routed = jnp.dot(mix[...], returned[...], preferred_element_type=F32)
    for g in range(4):
        lo, hi = g * 1024, (g + 1) * 1024
        total = stream[:, lo:hi] + routed[g * 32 : (g + 1) * 32]
        for s in (s0, s1, s2, s3):
            total = total + s[:, lo:hi].astype(F32)
        out[:, lo:hi] = total.astype(BF)


def attend_kernel(counts, first, last, *refs):
    at = 0

    def take(n):
        nonlocal at
        at += n
        return refs[at - n : at]

    q_own, q_other, core = take(3)
    tiles, planes = [], []
    for n, own_block in counts:
        tiles.append((take(n), take(1)[0], own_block))
        if first and not own_block:
            planes.append(tiles[-1][0][0])
    if not first:
        m_in, l_in, an_in, ab_in = take(4)
    if last:
        own_out, send_out = take(2)
    else:
        m_out, l_out, an_out, ab_out = take(4)

    def keys(ref, lo, hi):
        value = ref[1, :, lo:hi] if any(ref is p for p in planes) else ref[..., lo:hi]
        return value.reshape(-1, hi - lo)

    results = {}
    for group, size, heads, lo, per in (("n", NARROW_SIZE, 4, 0, 2 if last else 4), ("b", BROAD_SIZE, 2, 256, 2)):
        count = per * 128
        scale = size**-0.5 * LOG2E
        base = 0 if group == "n" else 4
        row_base = 0 if group == "n" else 1024
        loaded = []
        for arrays, bias, own_block in tiles:
            k = jnp.concatenate([keys(r, lo, lo + size) for r in arrays], axis=0)
            v = jnp.concatenate([keys(r, lo + size, lo + 2 * size) for r in arrays], axis=0)
            loaded.append((k, v, bias, own_block))
        for side, q_ref in ((0, q_own), (1, q_other)):
            for h0 in range(0, heads, per):
                col = (0 if group == "n" else 512) + h0 * size
                q = jnp.concatenate([q_ref[:, col + i * size : col + (i + 1) * size] for i in range(per)], axis=0)
                rows = row_base + side * heads * 128 + h0 * 128
                arow = rows - row_base
                scores = []
                for k, v, bias, own_block in loaded:
                    s = lax.dot_general(q, k, (((1,), (1,)), ((), ())), preferred_element_type=F32) * scale
                    n = k.shape[0]
                    b = bias[base + h0 : base + h0 + per, :]
                    s = (s.reshape(per, 128, n) + b[:, None, :]).reshape(count, n)
                    if own_block:
                        qi = lax.broadcasted_iota(jnp.int32, (count, n), 0) % 128
                        ki = lax.broadcasted_iota(jnp.int32, (count, n), 1)
                        offset = 0 if side == 0 else 128 * (1 - 2 * core[0])
                        s = jnp.where(ki <= qi + offset, s, MASKED)
                    scores.append(s)
                m = functools.reduce(jnp.maximum, [jnp.max(s, axis=1, keepdims=True) for s in scores])
                if not first:
                    m_old = m_in[pl.ds(rows, count), :][:, :1]
                    m = jnp.maximum(m, m_old)
                l = jnp.zeros((count, 1), F32)
                acc = jnp.zeros((count, size), F32)
                for s, (k, v, bias, own_block) in zip(scores, loaded):
                    p = jnp.exp2(s - m)
                    l = l + jnp.sum(p, axis=1, keepdims=True)
                    acc = acc + jnp.dot(p.astype(BF), v, preferred_element_type=F32)
                if not first:
                    a_in = an_in if group == "n" else ab_in
                    factor = jnp.exp2(m_old - m)
                    l = l + l_in[pl.ds(rows, count), :][:, :1] * factor
                    acc = acc + a_in[pl.ds(arow, count), :] * factor
                if last:
                    out = own_out if side == 0 else send_out
                    o = acc / l
                    lse = m + jnp.log2(l)
                    for i in range(per):
                        out[:, col + i * size : col + (i + 1) * size] = o[i * 128 : (i + 1) * 128]
                        results[(side, base + h0 + i)] = lse[i * 128 : (i + 1) * 128]
                else:
                    a_out = an_out if group == "n" else ab_out
                    m_out[pl.ds(rows, count), :] = jnp.broadcast_to(m, (count, 128))
                    l_out[pl.ds(rows, count), :] = jnp.broadcast_to(l, (count, 128))
                    a_out[pl.ds(arow, count), :] = acc
    if last:
        lane = lax.broadcasted_iota(jnp.int32, (128, 128), 1)
        for side, out in ((0, own_out), (1, send_out)):
            stats = jnp.zeros((128, 128), F32)
            for h in range(6):
                stats = jnp.where(lane == h, results[(side, h)], stats)
            out[:, 1024:1152] = stats


def attend(q_own, q_other, core, tiles, state, last):
    counts = tuple((len(arrays), own_block) for arrays, _, own_block in tiles)
    operands = [q_own, q_other, core]
    n_keys = 0
    for arrays, bias, _ in tiles:
        operands += list(arrays) + [bias]
        n_keys += bias.shape[1]
    specs = [VMEM] * len(operands)
    specs[2] = SMEM
    if state is not None:
        operands += list(state)
        specs += [VMEM] * 4
    if last:
        shapes = [jax.ShapeDtypeStruct((128, 1152), F32)] * 2
    else:
        shapes = [
            jax.ShapeDtypeStruct((1536, 128), F32),
            jax.ShapeDtypeStruct((1536, 128), F32),
            jax.ShapeDtypeStruct((1024, 128), F32),
            jax.ShapeDtypeStruct((512, 256), F32),
        ]
    return pl.pallas_call(
        functools.partial(attend_kernel, counts, state is None, last),
        out_shape=shapes,
        in_specs=specs,
        out_specs=[VMEM] * len(shapes),
        compiler_params=pltpu.CompilerParams(vmem_limit_bytes=24 * 1024 * 1024),
        cost_estimate=pl.CostEstimate(
            flops=4 * n_keys * 256 * 1024, transcendentals=n_keys * 1536, bytes_accessed=4 * 1024 * 1024
        ),
    )(*operands)


def local(
    query_narrow,
    key_narrow,
    value_narrow,
    gates_narrow,
    query_broad,
    key_broad,
    value_broad,
    gates_broad,
    project_narrow,
    project_broad,
    residual,
    norm_gain,
    route_ids,
    route_weight,
    expert_gate,
    expert_up,
    expert_down,
    shared_gate,
    shared_up,
    shared_down,
):
    z, y, c, t = (lax.axis_index(n).astype(jnp.int32) for n in ("z", "y", "c", "tp"))

    own_kv, q_own = call(
        pack_kernel,
        (key_narrow, value_narrow, key_broad, value_broad, query_narrow, query_broad),
        [shaped((128, 768), BF), shaped((128, 1024), BF)],
        hbm=range(6),
        scratch=[pltpu.SemaphoreType.DMA((6,))],
        moved=0,
    )
    place = jnp.stack([z, y, c, t])
    q_other = swap_core(q_own)
    line = {}
    for k in (2, 1, 3):
        line[k] = turn(own_kv, k, 0)
    target, mix, own_bias, bias_1, bias_2, bias_3 = call(
        tables_kernel,
        (place, route_ids.T, route_weight.T, gates_narrow.T, gates_broad.T),
        [shaped((4, 128), jnp.int32), shaped((128, 1024), BF)] + [shaped((8, n), F32) for n in (128, 384, 1024, 512)],
        smem=(0,),
        hbm=(1, 2, 3, 4),
        scratch=[
            pltpu.VMEM((4, 32), jnp.int32),
            pltpu.VMEM((4, 32), F32),
            pltpu.VMEM((4, 4096), F32),
            pltpu.VMEM((2, 4096), F32),
            pltpu.SemaphoreType.DMA((4,)),
        ],
    )
    low, high = call(
        stack_kernel,
        [own_kv] + [line[k] for k in ORDER[1:]] + [target, own_bias],
        [shaped((2, 128, 768), BF)] * 2,
    )
    low_back = turn(low, 1, 1)
    high_ahead = turn(high, 3, 1)
    low_ahead = turn(low, 3, 1)
    high_back = turn(high, 1, 1)
    low_far = turn(low_back, 1, 1)
    high_far = turn(high_ahead, 3, 1)

    core = c.reshape(1)
    first_tiles = [((own_kv,), own_bias, True), ((low, high), bias_1, False)]
    state = attend(q_own, q_other, core, first_tiles, None, False)
    second_tiles = [((low_back, low_ahead, high_back, high_ahead), bias_2, False)]
    state = attend(q_own, q_other, core, second_tiles, state, False)
    own_part, send_part = attend(q_own, q_other, core, [((low_far, high_far), bias_3, False)], state, True)
    other_part = swap_core(send_part)

    p0, p1, p2, p3 = call(
        project_kernel,
        (place, own_part, other_part, project_narrow, project_broad),
        [shaped((32, 4096), BF)] * 4,
        smem=(0,),
        scratch=[pltpu.VMEM((128, 4096), F32), pltpu.VMEM((128, 1024), BF)],
        flops=2 * 128 * 1024 * 4096,
    )
    p2 = shift(p2, "tp", 2)
    p1 = shift(p1, "tp", 1)
    p3 = shift(p3, "tp", 3)

    stream, normed, outbound = call(
        dispatch_kernel,
        (place, p0, p1, p2, p3, residual, norm_gain.reshape(1, -1), target),
        [shaped((32, 4096), F32), shaped((32, 4096), BF), pltpu.HBM((1024, 1024), BF)],
        smem=(0,),
        hbm_out=(2,),
        scratch=[pltpu.VMEM((1024, 1024), BF), pltpu.SemaphoreType.DMA((4,))],
        flops=2 * 1024 * 128 * 1024,
    )
    every = SP + ("tp",)
    inbound = lax.all_to_all(outbound.reshape(128, 8, 1024), every, 0, 0, tiled=True)

    n1 = shift(normed, "tp", 1)
    n2 = shift(normed, "tp", 2)
    n3 = shift(normed, "tp", 3)
    s0, s1, s2, s3 = call(
        shared_kernel,
        (normed, n1, n2, n3, shared_gate, shared_up, shared_down),
        [shaped((32, 4096), BF)] * 4,
        hbm=(4, 5, 6),
        scratch=[
            pltpu.VMEM((4096, 256), BF),
            pltpu.VMEM((4096, 256), BF),
            pltpu.VMEM((256, 4096), BF),
            pltpu.SemaphoreType.DMA((3,)),
        ],
        mib=20,
        flops=2 * 128 * 4096 * 768,
    )
    s1 = shift(s1, "tp", 3)
    s2 = shift(s2, "tp", 2)
    s3 = shift(s3, "tp", 1)

    (result,) = call(
        expert_kernel,
        (inbound.reshape(1024, 1024), expert_gate, expert_up, expert_down),
        [pltpu.HBM((1024, 1024), BF)],
        hbm=(1, 2, 3),
        hbm_out=(0,),
        scratch=[
            pltpu.VMEM((256, 4096), BF),
            pltpu.VMEM((1024, 1024), BF),
            pltpu.VMEM((4096, 256), BF),
            pltpu.VMEM((4096, 256), BF),
            pltpu.VMEM((256, 4096), BF),
            pltpu.SemaphoreType.DMA((9,)),
            pltpu.SemaphoreType.DMA((4,)),
        ],
        mib=20,
        flops=2 * 256 * 4096 * 768,
    )
    returned = lax.all_to_all(result.reshape(128, 8, 1024), every, 0, 0, tiled=True)
    (out,) = call(
        combine_kernel,
        (returned.reshape(1024, 1024), mix, stream, s0, s1, s2, s3),
        [shaped((32, 4096), BF)],
        flops=2 * 128 * 1024 * 1024,
    )
    return out


def solution(mesh):
    mesh = Mesh(mesh.devices.reshape(4, 4, 2, 4), ("z", "y", "c", "tp"))
    every = SP + ("tp",)
    placed = (
        P(SP, "tp"),
        P(SP, "tp"),
        P(SP, "tp"),
        P(None, "tp"),
        P(SP, "tp"),
        P(SP, "tp"),
        P(SP, "tp"),
        P(None, "tp"),
        P("tp", None),
        P("tp", None),
        P(SP, None),
        P(),
        P(every, None),
        P(every, None),
        P(every, None, None),
        P(every, None, None),
        P(every, None, None),
        P(None, "tp"),
        P(None, "tp"),
        P("tp", None),
    )

    return jax.shard_map(local, mesh=mesh, in_specs=placed, out_specs=P(every, None), check_vma=False)
```

```python
import functools

import jax
import jax.numpy as jnp
from jax import lax
from jax.experimental import pallas as pl
from jax.experimental.pallas import tpu as pltpu
from jax.sharding import Mesh
from jax.sharding import PartitionSpec as P


SP = ("z", "y", "c")
NARROW_SIZE = 128
BROAD_SIZE = 256
LOG2E = 1.4426950408889634
MASKED = -1e30
EPSILON = 1e-06
ORDER = (0, 1, 3, 2)
VMEM = pl.BlockSpec(memory_space=pltpu.VMEM)
SMEM = pl.BlockSpec(memory_space=pltpu.SMEM)
HBM = pl.BlockSpec(memory_space=pltpu.HBM)
BF = jnp.bfloat16
F32 = jnp.float32


def shift(x, axis, k):
    return lax.ppermute(x, axis, [(i, (i + k) % 4) for i in range(4)])


def swap_core(x):
    return lax.ppermute(x, "c", [(0, 1), (1, 0)])


def turn(x, k, phase):
    pairs = []
    for z in range(4):
        for y in range(4):
            for c in range(2):
                to_z, to_y = (z, (y + k) % 4) if c == phase else ((z + k) % 4, y)
                pairs.append(((z * 4 + y) * 2 + c, (to_z * 4 + to_y) * 2 + c))
    return lax.ppermute(x, SP, pairs)


def call(kernel, operands, shapes, smem=(), hbm=(), hbm_out=(), scratch=(), mib=16, flops=0, moved=2**21):
    operands = [
        pltpu.with_memory_space_constraint(x, pltpu.HBM) if i in hbm else x for i, x in enumerate(operands)
    ]
    return pl.pallas_call(
        kernel,
        out_shape=shapes,
        in_specs=[SMEM if i in smem else HBM if i in hbm else VMEM for i in range(len(operands))],
        out_specs=[HBM if i in hbm_out else VMEM for i in range(len(shapes))],
        scratch_shapes=list(scratch),
        compiler_params=pltpu.CompilerParams(vmem_limit_bytes=mib * 1024 * 1024),
        cost_estimate=pl.CostEstimate(flops=flops, transcendentals=0, bytes_accessed=moved),
    )(*operands)


def shaped(shape, dtype):
    return jax.ShapeDtypeStruct(shape, dtype)


def pack_kernel(kn, vn, kb, vb, qn, qb, kv, q, sems):
    copies = []
    for ref, out, at in ((kn, kv, 0), (vn, kv, 128), (kb, kv, 256), (vb, kv, 512), (qn, q, 0), (qb, q, 512)):
        target = out.at[:, at : at + ref.shape[1]]
        copies.append(pltpu.make_async_copy(ref, target, sems.at[len(copies)]))
    for copy in copies:
        copy.start()
    for copy in copies:
        copy.wait()


def stack_kernel(a, b, c, d, routed, biased, low, high):
    for out, i, ref in ((low, 0, a), (low, 1, b), (high, 0, c), (high, 1, d)):
        out[i] = ref[...]


def tables_kernel(place, ids_hbm, weight_hbm, narrow_hbm, broad_hbm, target, mix, own, first, second, third, *scratch):
    ids_in, weight_in, narrow, broad, sems = scratch
    copies = []
    for ref, held in ((narrow_hbm, narrow), (broad_hbm, broad), (ids_hbm, ids_in), (weight_hbm, weight_in)):
        copies.append(pltpu.make_async_copy(ref, held, sems.at[len(copies)]))
    for copy in copies:
        copy.start()
    for copy in copies:
        copy.wait()
    ids = jnp.concatenate([ids_in[...]] * 4, axis=1)
    weight = jnp.concatenate([weight_in[...].astype(BF).astype(F32)] * 4, axis=1)
    expert = lax.broadcasted_iota(jnp.int32, (128, 128), 0)
    column = lax.broadcasted_iota(jnp.int32, (128, 128), 1)
    named = jnp.zeros((128, 128), F32)
    for k in range(4):
        named = named + jnp.where(expert == ids[k : k + 1, :], 1.0, 0.0)
    earlier = jnp.where((expert < 32) & (expert < column % 32), 1.0, 0.0).astype(BF)
    before = jnp.dot(named.astype(BF), earlier, preferred_element_type=F32)
    row = lax.broadcasted_iota(jnp.int32, (1024, 128), 0)
    total = jnp.zeros((1024, 128), F32)
    for k in range(4):
        slot = jnp.sum(jnp.where(expert == ids[k : k + 1, :], before, 0.0), axis=0, keepdims=True)
        start = ids[k : k + 1, :] * 8 + slot.astype(jnp.int32) * 4 + column[:1] // 32
        target[k : k + 1, :] = start
        total = total + jnp.where(row == start, weight[k : k + 1, :], 0.0)
    mix[...] = total.T.astype(BF)


    z, y, c = place[0], place[1], place[2]
    here = z * 4 + y

    def put(out, at, early, late):
        back_y = jnp.where(c == 0, early, late)
        back_z = jnp.where(c == 0, late, early)
        chip = ((z + 4 - back_z) % 4) * 4 + (y + 4 - back_y) % 4
        block = pl.multiple_of(chip * 256 + c * 128, 128)
        ahead = chip > here
        for row, gates in ((0, narrow), (4, broad)):
            piece = gates[:, pl.ds(block, 128)] * (-LOG2E)
            out[row : row + gates.shape[0], at : at + 128] = jnp.where(ahead, MASKED, piece)

    put(own, 0, 0, 0)
    for i in range(1, 4):
        put(first, (i - 1) * 128, ORDER[i], 0)
    for i in range(4):
        put(second, i * 128, ORDER[i % 2], 1 if i < 2 else 3)
        put(second, 512 + i * 128, ORDER[2 + i % 2], 1 if i < 2 else 3)
        put(third, i * 128, ORDER[i], 2)


def project_kernel(place, own, other, narrow, broad, *refs):
    outs, total, attn = refs[:4], *refs[4:]
    a, b = own[:, 1024:], other[:, 1024:]
    top = jnp.maximum(a, b)
    wa, wb = jnp.exp2(a - top), jnp.exp2(b - top)
    joined = wa + wb
    wa, wb = wa / joined, wb / joined
    for h in range(6):
        lo, size = (h * 128, 128) if h < 4 else (512 + (h - 4) * 256, 256)
        value = own[:, lo : lo + size] * wa[:, h : h + 1] + other[:, lo : lo + size] * wb[:, h : h + 1]
        attn[:, lo : lo + size] = value.astype(BF)
    for at in range(0, 4096, 1024):
        part = jnp.dot(attn[:, :512], narrow[:, at : at + 1024], preferred_element_type=F32)
        part = part + jnp.dot(attn[:, 512:], broad[:, at : at + 1024], preferred_element_type=F32)
        total[:, at : at + 1024] = part
    for k in range(4):
        outs[k][...] = total[pl.ds(((place[3] + k) % 4) * 32, 32), :].astype(BF)


def dispatch_kernel(place, p0, p1, p2, p3, residual, gain, target, stream_out, normed_out, out, rows, sems):
    mixture = p0[...].astype(F32) + p1[...].astype(F32) + p2[...].astype(F32) + p3[...].astype(F32)
    stream = residual[pl.ds(place[3] * 32, 32), :].astype(F32) + mixture
    stream_out[...] = stream
    scale = lax.rsqrt(jnp.mean(stream * stream, axis=1, keepdims=True) + EPSILON)
    normed = (stream * scale * gain[...]).astype(BF)
    normed_out[...] = normed
    cut = jnp.concatenate([normed[:, g * 1024 : (g + 1) * 1024] for g in range(4)], axis=0)
    row = lax.broadcasted_iota(jnp.int32, (256, 128), 0)
    copies = []
    for at in range(0, 1024, 256):
        pick = row + at == target[0:1, :]
        for k in range(1, 4):
            pick = pick | (row + at == target[k : k + 1, :])
        rows[at : at + 256, :] = jnp.dot(pick.astype(F32).astype(BF), cut, preferred_element_type=F32).astype(BF)
        part = pl.ds(at, 256)
        copies.append(pltpu.make_async_copy(rows.at[part], out.at[part], sems.at[at // 256]))
        copies[-1].start()
    for copy in copies:
        copy.wait()


def fetch(pairs, sems):
    copies = [pltpu.make_async_copy(ref, held, sems.at[i]) for i, (ref, held) in enumerate(pairs)]
    for copy in copies:
        copy.start()
    return copies


def silu(v):
    return v / (1.0 + jnp.exp(-v))


def shared_kernel(n0, n1, n2, n3, gate_hbm, up_hbm, down_hbm, o0, o1, o2, o3, x, gate, up, down, sems):
    pairs = [(n, x.at[pl.ds(k * 32, 32)]) for k, n in enumerate((n0, n1, n2, n3))]
    fetched = fetch(pairs + [(gate_hbm, gate), (up_hbm, up), (down_hbm, down)], sems)
    for copy in fetched[:5]:
        copy.wait()
    x = x[...]
    g = jnp.dot(x, gate[...], preferred_element_type=F32)
    fetched[5].wait()
    u = jnp.dot(x, up[...], preferred_element_type=F32)
    fetched[6].wait()
    hidden = (silu(g) * u).astype(BF)
    for at in range(0, 4096, 1024):
        part = jnp.dot(hidden, down[:, at : at + 1024], preferred_element_type=F32).astype(BF)
        for k, out in enumerate((o0, o1, o2, o3)):
            out[:, at : at + 1024] = part[k * 32 : (k + 1) * 32]


def mark_kernel(value, out):
    out[...] = value[...]


def expert_kernel(mark, inbound, gate_hbm, up_hbm, down_hbm, out, x, rows_out, gate, up, down, weight_sems, sems):
    pairs = []
    for g in range(4):
        part = pl.ds(g * 1024, 1024)
        pairs += [(ref.at[0, part], held.at[part]) for ref, held in ((gate_hbm, gate), (up_hbm, up))]
    fetched = fetch(pairs + [(down_hbm.at[0], down)], weight_sems)
    i = lax.broadcasted_iota(jnp.int32, (256, 256), 0)
    j = lax.broadcasted_iota(jnp.int32, (256, 256), 1)
    order = (j == ((i % 64) // 2) * 8 + (i % 2) * 4 + i // 64).astype(F32).astype(BF)
    back = (i == ((j % 64) // 2) * 8 + (j % 2) * 4 + j // 64).astype(F32).astype(BF)
    for b in range(4):
        rows = jnp.dot(order, inbound[b * 256 : (b + 1) * 256, :], preferred_element_type=F32).astype(BF)
        for g in range(4):
            x[b * 64 : (b + 1) * 64, g * 1024 : (g + 1) * 1024] = rows[g * 64 : (g + 1) * 64]
    gated, upped = jnp.zeros((256, 256), F32), jnp.zeros((256, 256), F32)
    for g in range(4):
        lo, hi = g * 1024, (g + 1) * 1024
        fetched[2 * g].wait()
        fetched[2 * g + 1].wait()
        gated = gated + jnp.dot(x[:, lo:hi], gate[lo:hi], preferred_element_type=F32)
        upped = upped + jnp.dot(x[:, lo:hi], up[lo:hi], preferred_element_type=F32)
    fetched[8].wait()
    hidden = (silu(gated) * upped).astype(BF)
    for g in range(4):
        part = jnp.dot(hidden, down[:, g * 1024 : (g + 1) * 1024], preferred_element_type=F32)
        x[:, g * 1024 : (g + 1) * 1024] = part.astype(BF)
    copies = []
    for b in range(4):
        rows = jnp.concatenate([x[b * 64 : (b + 1) * 64, g * 1024 : (g + 1) * 1024] for g in range(4)], axis=0)
        part = pl.ds(b * 256, 256)
        rows_out[part, :] = jnp.dot(back, rows, preferred_element_type=F32).astype(BF)
        copies.append(pltpu.make_async_copy(rows_out.at[part], out.at[part], sems.at[b]))
        copies[-1].start()
    for copy in copies:
        copy.wait()


def combine_kernel(returned, mix, stream_hbm, s0, s1, s2, s3, out, stream, shared, sems):
    pairs = [(s, shared.at[k]) for k, s in enumerate((s0, s1, s2, s3))]
    fetched = fetch(pairs + [(stream_hbm, stream)], sems)
    routed = jnp.dot(mix[...], returned[...], preferred_element_type=F32)
    for copy in fetched:
        copy.wait()
    for g in range(4):
        lo, hi = g * 1024, (g + 1) * 1024
        total = stream[:, lo:hi] + routed[g * 32 : (g + 1) * 32]
        for k in range(4):
            total = total + shared[k, :, lo:hi].astype(F32)
        out[:, lo:hi] = total.astype(BF)


def attend_kernel(counts, first, last, *refs):
    at = 0

    def take(n):
        nonlocal at
        at += n
        return refs[at - n : at]

    q_own, q_other, core = take(3)
    tiles, planes = [], []
    for n, own_block in counts:
        tiles.append((take(n), take(1)[0], own_block))
        if first and not own_block:
            planes.append(tiles[-1][0][0])
    if not first:
        m_in, l_in, an_in, ab_in = take(4)
    if last:
        own_out, send_out = take(2)
    else:
        m_out, l_out, an_out, ab_out = take(4)

    def keys(ref, lo, hi):
        value = ref[1, :, lo:hi] if any(ref is p for p in planes) else ref[..., lo:hi]
        return value.reshape(-1, hi - lo)

    results = {}
    for group, size, heads, lo, per in (("n", NARROW_SIZE, 4, 0, 2 if last else 4), ("b", BROAD_SIZE, 2, 256, 2)):
        count = per * 128
        scale = size**-0.5 * LOG2E
        base = 0 if group == "n" else 4
        row_base = 0 if group == "n" else 1024
        loaded = []
        for arrays, bias, own_block in tiles:
            k = jnp.concatenate([keys(r, lo, lo + size) for r in arrays], axis=0)
            v = jnp.concatenate([keys(r, lo + size, lo + 2 * size) for r in arrays], axis=0)
            loaded.append((k, v, bias, own_block))
        for side, q_ref in ((0, q_own), (1, q_other)):
            for h0 in range(0, heads, per):
                col = (0 if group == "n" else 512) + h0 * size
                q = jnp.concatenate([q_ref[:, col + i * size : col + (i + 1) * size] for i in range(per)], axis=0)
                rows = row_base + side * heads * 128 + h0 * 128
                arow = rows - row_base
                scores = []
                for k, v, bias, own_block in loaded:
                    s = lax.dot_general(q, k, (((1,), (1,)), ((), ())), preferred_element_type=F32) * scale
                    n = k.shape[0]
                    b = bias[base + h0 : base + h0 + per, :]
                    s = (s.reshape(per, 128, n) + b[:, None, :]).reshape(count, n)
                    if own_block:
                        qi = lax.broadcasted_iota(jnp.int32, (count, n), 0) % 128
                        ki = lax.broadcasted_iota(jnp.int32, (count, n), 1)
                        offset = 0 if side == 0 else 128 * (1 - 2 * core[0])
                        s = jnp.where(ki <= qi + offset, s, MASKED)
                    scores.append(s)
                m = functools.reduce(jnp.maximum, [jnp.max(s, axis=1, keepdims=True) for s in scores])
                if not first:
                    m_old = m_in[pl.ds(rows, count), :][:, :1]
                    m = jnp.maximum(m, m_old)
                l = jnp.zeros((count, 1), F32)
                acc = jnp.zeros((count, size), F32)
                for s, (k, v, bias, own_block) in zip(scores, loaded):
                    p = jnp.exp2(s - m)
                    l = l + jnp.sum(p, axis=1, keepdims=True)
                    acc = acc + jnp.dot(p.astype(BF), v, preferred_element_type=F32)
                if not first:
                    a_in = an_in if group == "n" else ab_in
                    factor = jnp.exp2(m_old - m)
                    l = l + l_in[pl.ds(rows, count), :][:, :1] * factor
                    acc = acc + a_in[pl.ds(arow, count), :] * factor
                if last:
                    out = own_out if side == 0 else send_out
                    o = acc / l
                    lse = m + jnp.log2(l)
                    for i in range(per):
                        out[:, col + i * size : col + (i + 1) * size] = o[i * 128 : (i + 1) * 128]
                        results[(side, base + h0 + i)] = lse[i * 128 : (i + 1) * 128]
                else:
                    a_out = an_out if group == "n" else ab_out
                    m_out[pl.ds(rows, count), :] = jnp.broadcast_to(m, (count, 128))
                    l_out[pl.ds(rows, count), :] = jnp.broadcast_to(l, (count, 128))
                    a_out[pl.ds(arow, count), :] = acc
    if last:
        lane = lax.broadcasted_iota(jnp.int32, (128, 128), 1)
        for side, out in ((0, own_out), (1, send_out)):
            stats = jnp.zeros((128, 128), F32)
            for h in range(6):
                stats = jnp.where(lane == h, results[(side, h)], stats)
            out[:, 1024:1152] = stats


def attend(q_own, q_other, core, tiles, state, last):
    counts = tuple((len(arrays), own_block) for arrays, _, own_block in tiles)
    operands = [q_own, q_other, core]
    n_keys = 0
    for arrays, bias, _ in tiles:
        operands += list(arrays) + [bias]
        n_keys += bias.shape[1]
    specs = [VMEM] * len(operands)
    specs[2] = SMEM
    if state is not None:
        operands += list(state)
        specs += [VMEM] * 4
    if last:
        shapes = [jax.ShapeDtypeStruct((128, 1152), F32)] * 2
    else:
        shapes = [
            jax.ShapeDtypeStruct((1536, 128), F32),
            jax.ShapeDtypeStruct((1536, 128), F32),
            jax.ShapeDtypeStruct((1024, 128), F32),
            jax.ShapeDtypeStruct((512, 256), F32),
        ]
    return pl.pallas_call(
        functools.partial(attend_kernel, counts, state is None, last),
        out_shape=shapes,
        in_specs=specs,
        out_specs=[VMEM] * len(shapes),
        compiler_params=pltpu.CompilerParams(vmem_limit_bytes=24 * 1024 * 1024),
        cost_estimate=pl.CostEstimate(
            flops=4 * n_keys * 256 * 1024, transcendentals=n_keys * 1536, bytes_accessed=4 * 1024 * 1024
        ),
    )(*operands)


def local(
    query_narrow,
    key_narrow,
    value_narrow,
    gates_narrow,
    query_broad,
    key_broad,
    value_broad,
    gates_broad,
    project_narrow,
    project_broad,
    residual,
    norm_gain,
    route_ids,
    route_weight,
    expert_gate,
    expert_up,
    expert_down,
    shared_gate,
    shared_up,
    shared_down,
):
    z, y, c, t = (lax.axis_index(n).astype(jnp.int32) for n in ("z", "y", "c", "tp"))

    own_kv, q_own = call(
        pack_kernel,
        (key_narrow, value_narrow, key_broad, value_broad, query_narrow, query_broad),
        [shaped((128, 768), BF), shaped((128, 1024), BF)],
        hbm=range(6),
        scratch=[pltpu.SemaphoreType.DMA((6,))],
        moved=0,
    )
    place = jnp.stack([z, y, c, t])
    q_other = swap_core(q_own)
    line = {}
    for k in (2, 1, 3):
        line[k] = turn(own_kv, k, 0)
    target, mix, own_bias, bias_1, bias_2, bias_3 = call(
        tables_kernel,
        (place, route_ids.T, route_weight.T, gates_narrow.T, gates_broad.T),
        [shaped((4, 128), jnp.int32), shaped((128, 1024), BF)] + [shaped((8, n), F32) for n in (128, 384, 1024, 512)],
        smem=(0,),
        hbm=(1, 2, 3, 4),
        scratch=[
            pltpu.VMEM((4, 32), jnp.int32),
            pltpu.VMEM((4, 32), F32),
            pltpu.VMEM((4, 4096), F32),
            pltpu.VMEM((2, 4096), F32),
            pltpu.SemaphoreType.DMA((4,)),
        ],
    )
    low, high = call(
        stack_kernel,
        [own_kv] + [line[k] for k in ORDER[1:]] + [target, own_bias],
        [shaped((2, 128, 768), BF)] * 2,
    )
    low_back = turn(low, 1, 1)
    high_ahead = turn(high, 3, 1)
    low_ahead = turn(low, 3, 1)
    high_back = turn(high, 1, 1)
    low_far = turn(low_back, 1, 1)
    high_far = turn(high_ahead, 3, 1)

    core = c.reshape(1)
    first_tiles = [((own_kv,), own_bias, True), ((low, high), bias_1, False)]
    state = attend(q_own, q_other, core, first_tiles, None, False)
    second_tiles = [((low_back, low_ahead, high_back, high_ahead), bias_2, False)]
    state = attend(q_own, q_other, core, second_tiles, state, False)
    own_part, send_part = attend(q_own, q_other, core, [((low_far, high_far), bias_3, False)], state, True)
    other_part = swap_core(send_part)

    p0, p1, p2, p3 = call(
        project_kernel,
        (place, own_part, other_part, project_narrow, project_broad),
        [shaped((32, 4096), BF)] * 4,
        smem=(0,),
        scratch=[pltpu.VMEM((128, 4096), F32), pltpu.VMEM((128, 1024), BF)],
        flops=2 * 128 * 1024 * 4096,
    )
    p2 = shift(p2, "tp", 2)
    p1 = shift(p1, "tp", 1)
    p3 = shift(p3, "tp", 3)

    stream, normed, outbound = call(
        dispatch_kernel,
        (place, p0, p1, p2, p3, residual, norm_gain.reshape(1, -1), target),
        [shaped((32, 4096), F32), shaped((32, 4096), BF), pltpu.HBM((1024, 1024), BF)],
        smem=(0,),
        hbm_out=(2,),
        scratch=[pltpu.VMEM((1024, 1024), BF), pltpu.SemaphoreType.DMA((4,))],
        flops=2 * 1024 * 128 * 1024,
    )
    every = SP + ("tp",)
    inbound = lax.all_to_all(outbound.reshape(128, 8, 1024), every, 0, 0, tiled=True)

    n1 = shift(normed, "tp", 1)
    n2 = shift(normed, "tp", 2)
    n3 = shift(normed, "tp", 3)
    s0, s1, s2, s3 = call(
        shared_kernel,
        (normed, n1, n2, n3, shared_gate, shared_up, shared_down),
        [shaped((32, 4096), BF)] * 4,
        hbm=range(7),
        scratch=[
            pltpu.VMEM((128, 4096), BF),
            pltpu.VMEM((4096, 256), BF),
            pltpu.VMEM((4096, 256), BF),
            pltpu.VMEM((256, 4096), BF),
            pltpu.SemaphoreType.DMA((7,)),
        ],
        mib=20,
        flops=2 * 128 * 4096 * 768,
    )
    s1 = shift(s1, "tp", 3)
    s2 = shift(s2, "tp", 2)
    s3 = shift(s3, "tp", 1)

    (mark,) = call(mark_kernel, (target,), [shaped((4, 128), jnp.int32)])
    (result,) = call(
        expert_kernel,
        (mark, inbound.reshape(1024, 1024), expert_gate, expert_up, expert_down),
        [pltpu.HBM((1024, 1024), BF)],
        hbm=(2, 3, 4),
        hbm_out=(0,),
        scratch=[
            pltpu.VMEM((256, 4096), BF),
            pltpu.VMEM((1024, 1024), BF),
            pltpu.VMEM((4096, 256), BF),
            pltpu.VMEM((4096, 256), BF),
            pltpu.VMEM((256, 4096), BF),
            pltpu.SemaphoreType.DMA((9,)),
            pltpu.SemaphoreType.DMA((4,)),
        ],
        mib=20,
        flops=2 * 256 * 4096 * 768,
    )
    returned = lax.all_to_all(result.reshape(128, 8, 1024), every, 0, 0, tiled=True)
    (out,) = call(
        combine_kernel,
        (returned.reshape(1024, 1024), mix, stream, s0, s1, s2, s3),
        [shaped((32, 4096), BF)],
        hbm=(2, 3, 4, 5, 6),
        scratch=[pltpu.VMEM((32, 4096), F32), pltpu.VMEM((4, 32, 4096), BF), pltpu.SemaphoreType.DMA((5,))],
        flops=2 * 128 * 1024 * 1024,
    )
    return out


def solution(mesh):
    mesh = Mesh(mesh.devices.reshape(4, 4, 2, 4), ("z", "y", "c", "tp"))
    every = SP + ("tp",)
    placed = (
        P(SP, "tp"),
        P(SP, "tp"),
        P(SP, "tp"),
        P(None, "tp"),
        P(SP, "tp"),
        P(SP, "tp"),
        P(SP, "tp"),
        P(None, "tp"),
        P("tp", None),
        P("tp", None),
        P(SP, None),
        P(),
        P(every, None),
        P(every, None),
        P(every, None, None),
        P(every, None, None),
        P(every, None, None),
        P(None, "tp"),
        P(None, "tp"),
        P("tp", None),
    )

    return jax.shard_map(local, mesh=mesh, in_specs=placed, out_specs=P(every, None), check_vma=False)
```

```python
import functools

import jax
import jax.numpy as jnp
from jax import lax
from jax.experimental import pallas as pl
from jax.experimental.pallas import tpu as pltpu
from jax.sharding import Mesh
from jax.sharding import PartitionSpec as P


SP = ("z", "y", "c")
NARROW_SIZE = 128
BROAD_SIZE = 256
LOG2E = 1.4426950408889634
MASKED = -1e30
EPSILON = 1e-06
ORDER = (0, 1, 3, 2)
VMEM = pl.BlockSpec(memory_space=pltpu.VMEM)
SMEM = pl.BlockSpec(memory_space=pltpu.SMEM)
HBM = pl.BlockSpec(memory_space=pltpu.HBM)
BF = jnp.bfloat16
F32 = jnp.float32


def shift(x, axis, k):
    return lax.ppermute(x, axis, [(i, (i + k) % 4) for i in range(4)])


def swap_core(x):
    return lax.ppermute(x, "c", [(0, 1), (1, 0)])


def turn(x, k, phase):
    pairs = []
    for z in range(4):
        for y in range(4):
            for c in range(2):
                to_z, to_y = (z, (y + k) % 4) if c == phase else ((z + k) % 4, y)
                pairs.append(((z * 4 + y) * 2 + c, (to_z * 4 + to_y) * 2 + c))
    return lax.ppermute(x, SP, pairs)


def call(kernel, operands, shapes, smem=(), hbm=(), hbm_out=(), scratch=(), mib=16, flops=0, moved=2**21):
    operands = [
        pltpu.with_memory_space_constraint(x, pltpu.HBM) if i in hbm else x for i, x in enumerate(operands)
    ]
    return pl.pallas_call(
        kernel,
        out_shape=shapes,
        in_specs=[SMEM if i in smem else HBM if i in hbm else VMEM for i in range(len(operands))],
        out_specs=[HBM if i in hbm_out else VMEM for i in range(len(shapes))],
        scratch_shapes=list(scratch),
        compiler_params=pltpu.CompilerParams(vmem_limit_bytes=mib * 1024 * 1024),
        cost_estimate=pl.CostEstimate(flops=flops, transcendentals=0, bytes_accessed=moved),
    )(*operands)


def shaped(shape, dtype):
    return jax.ShapeDtypeStruct(shape, dtype)


def pack_kernel(kn, vn, kb, vb, qn, qb, kv, q, sems):
    copies = []
    for ref, out, at in ((kn, kv, 0), (vn, kv, 128), (kb, kv, 256), (vb, kv, 512), (qn, q, 0), (qb, q, 512)):
        target = out.at[:, at : at + ref.shape[1]]
        copies.append(pltpu.make_async_copy(ref, target, sems.at[len(copies)]))
    for copy in copies:
        copy.start()
    for copy in copies:
        copy.wait()


def stack_kernel(a, b, c, d, routed, biased, low, high):
    for out, i, ref in ((low, 0, a), (low, 1, b), (high, 0, c), (high, 1, d)):
        out[i] = ref[...]


def tables_kernel(place, ids_hbm, weight_hbm, narrow_hbm, broad_hbm, target, mix, own, first, second, third, *scratch):
    ids_in, weight_in, narrow, broad, sems = scratch
    copies = []
    for ref, held in ((narrow_hbm, narrow), (broad_hbm, broad), (ids_hbm, ids_in), (weight_hbm, weight_in)):
        copies.append(pltpu.make_async_copy(ref, held, sems.at[len(copies)]))
    for copy in copies:
        copy.start()
    for copy in copies:
        copy.wait()
    ids = jnp.concatenate([ids_in[...]] * 4, axis=1)
    weight = jnp.concatenate([weight_in[...].astype(BF).astype(F32)] * 4, axis=1)
    expert = lax.broadcasted_iota(jnp.int32, (128, 128), 0)
    column = lax.broadcasted_iota(jnp.int32, (128, 128), 1)
    named = jnp.zeros((128, 128), F32)
    for k in range(4):
        named = named + jnp.where(expert == ids[k : k + 1, :], 1.0, 0.0)
    earlier = jnp.where((expert < 32) & (expert < column % 32), 1.0, 0.0).astype(BF)
    before = jnp.dot(named.astype(BF), earlier, preferred_element_type=F32)
    row = lax.broadcasted_iota(jnp.int32, (1024, 128), 0)
    total = jnp.zeros((1024, 128), F32)
    for k in range(4):
        slot = jnp.sum(jnp.where(expert == ids[k : k + 1, :], before, 0.0), axis=0, keepdims=True)
        start = ids[k : k + 1, :] * 8 + slot.astype(jnp.int32) * 4 + column[:1] // 32
        target[k : k + 1, :] = start
        total = total + jnp.where(row == start, weight[k : k + 1, :], 0.0)
    mix[...] = total.T.astype(BF)


    z, y, c = place[0], place[1], place[2]
    here = z * 4 + y

    def put(out, at, early, late):
        back_y = jnp.where(c == 0, early, late)
        back_z = jnp.where(c == 0, late, early)
        chip = ((z + 4 - back_z) % 4) * 4 + (y + 4 - back_y) % 4
        block = pl.multiple_of(chip * 256 + c * 128, 128)
        ahead = chip > here
        for row, gates in ((0, narrow), (4, broad)):
            piece = gates[:, pl.ds(block, 128)] * (-LOG2E)
            out[row : row + gates.shape[0], at : at + 128] = jnp.where(ahead, MASKED, piece)

    put(own, 0, 0, 0)
    for i in range(1, 4):
        put(first, (i - 1) * 128, ORDER[i], 0)
    for i in range(4):
        put(second, i * 128, ORDER[i % 2], 1 if i < 2 else 3)
        put(second, 512 + i * 128, ORDER[2 + i % 2], 1 if i < 2 else 3)
        put(third, i * 128, ORDER[i], 2)


def project_kernel(place, own, other, narrow, broad, *refs):
    outs, total, attn = refs[:4], *refs[4:]
    a, b = own[:, 1024:], other[:, 1024:].astype(F32)
    b = b + pltpu.roll(b, 120, 1) + pltpu.roll(b, 112, 1)
    top = jnp.maximum(a, b)
    wa, wb = jnp.exp2(a - top), jnp.exp2(b - top)
    joined = wa + wb
    wa, wb = wa / joined, wb / joined
    for h in range(6):
        lo, size = (h * 128, 128) if h < 4 else (512 + (h - 4) * 256, 256)
        value = own[:, lo : lo + size] * wa[:, h : h + 1] + other[:, lo : lo + size].astype(F32) * wb[:, h : h + 1]
        attn[:, lo : lo + size] = value.astype(BF)
    for at in range(0, 4096, 1024):
        part = jnp.dot(attn[:, :512], narrow[:, at : at + 1024], preferred_element_type=F32)
        part = part + jnp.dot(attn[:, 512:], broad[:, at : at + 1024], preferred_element_type=F32)
        total[:, at : at + 1024] = part
    for k in range(4):
        outs[k][...] = total[pl.ds(((place[3] + k) % 4) * 32, 32), :].astype(BF)


def dispatch_kernel(place, p0, p1, p2, p3, residual, gain, target, stream_out, normed_out, out, stream_held, rows, sems):
    mixture = p0[...].astype(F32) + p1[...].astype(F32) + p2[...].astype(F32) + p3[...].astype(F32)
    stream = residual[pl.ds(place[3] * 32, 32), :].astype(F32) + mixture
    stream_held[...] = stream
    copies = [pltpu.make_async_copy(stream_held, stream_out, sems.at[4])]
    copies[0].start()
    scale = lax.rsqrt(jnp.mean(stream * stream, axis=1, keepdims=True) + EPSILON)
    normed = (stream * scale * gain[...]).astype(BF)
    normed_out[...] = normed
    cut = jnp.concatenate([normed[:, g * 1024 : (g + 1) * 1024] for g in range(4)], axis=0)
    row = lax.broadcasted_iota(jnp.int32, (256, 128), 0)
    for at in range(0, 1024, 256):
        pick = row + at == target[0:1, :]
        for k in range(1, 4):
            pick = pick | (row + at == target[k : k + 1, :])
        rows[at : at + 256, :] = jnp.dot(pick.astype(F32).astype(BF), cut, preferred_element_type=F32).astype(BF)
        part = pl.ds(at, 256)
        copies.append(pltpu.make_async_copy(rows.at[part], out.at[part], sems.at[at // 256]))
        copies[-1].start()
    for copy in copies:
        copy.wait()


def fetch(pairs, sems):
    copies = [pltpu.make_async_copy(ref, held, sems.at[i]) for i, (ref, held) in enumerate(pairs)]
    for copy in copies:
        copy.start()
    return copies


def silu(v):
    return v / (1.0 + jnp.exp(-v))


def shared_kernel(n0, n1, n2, n3, gate_hbm, up_hbm, down_hbm, o0, o1, o2, o3, x, gate, up, down, sems):
    pairs = [(n, x.at[pl.ds(k * 32, 32)]) for k, n in enumerate((n0, n1, n2, n3))]
    fetched = fetch(pairs + [(gate_hbm, gate), (up_hbm, up), (down_hbm, down)], sems)
    for copy in fetched[:5]:
        copy.wait()
    x = x[...]
    g = jnp.dot(x, gate[...], preferred_element_type=F32)
    fetched[5].wait()
    u = jnp.dot(x, up[...], preferred_element_type=F32)
    fetched[6].wait()
    hidden = (silu(g) * u).astype(BF)
    for at in range(0, 4096, 1024):
        part = jnp.dot(hidden, down[:, at : at + 1024], preferred_element_type=F32).astype(BF)
        for k, out in enumerate((o0, o1, o2, o3)):
            out[:, at : at + 1024] = part[k * 32 : (k + 1) * 32]


def expert_kernel(inbound, gate_hbm, up_hbm, down_hbm, out, x, rows_out, gate, up, down, weight_sems, sems):
    pairs = []
    for g in range(4):
        part = pl.ds(g * 1024, 1024)
        pairs += [(ref.at[0, part], held.at[part]) for ref, held in ((gate_hbm, gate), (up_hbm, up))]
    fetched = fetch(pairs + [(down_hbm.at[0], down)], weight_sems)
    i = lax.broadcasted_iota(jnp.int32, (256, 256), 0)
    j = lax.broadcasted_iota(jnp.int32, (256, 256), 1)
    order = (j == ((i % 64) // 2) * 8 + (i % 2) * 4 + i // 64).astype(F32).astype(BF)
    back = (i == ((j % 64) // 2) * 8 + (j % 2) * 4 + j // 64).astype(F32).astype(BF)
    for b in range(4):
        rows = jnp.dot(order, inbound[b * 256 : (b + 1) * 256, :], preferred_element_type=F32).astype(BF)
        for g in range(4):
            x[b * 64 : (b + 1) * 64, g * 1024 : (g + 1) * 1024] = rows[g * 64 : (g + 1) * 64]
    gated, upped = jnp.zeros((256, 256), F32), jnp.zeros((256, 256), F32)
    for g in range(4):
        lo, hi = g * 1024, (g + 1) * 1024
        fetched[2 * g].wait()
        fetched[2 * g + 1].wait()
        gated = gated + jnp.dot(x[:, lo:hi], gate[lo:hi], preferred_element_type=F32)
        upped = upped + jnp.dot(x[:, lo:hi], up[lo:hi], preferred_element_type=F32)
    fetched[8].wait()
    hidden = (silu(gated) * upped).astype(BF)
    for g in range(4):
        part = jnp.dot(hidden, down[:, g * 1024 : (g + 1) * 1024], preferred_element_type=F32)
        x[:, g * 1024 : (g + 1) * 1024] = part.astype(BF)
    copies = []
    for b in range(4):
        rows = jnp.concatenate([x[b * 64 : (b + 1) * 64, g * 1024 : (g + 1) * 1024] for g in range(4)], axis=0)
        part = pl.ds(b * 256, 256)
        rows_out[part, :] = jnp.dot(back, rows, preferred_element_type=F32).astype(BF)
        copies.append(pltpu.make_async_copy(rows_out.at[part], out.at[part], sems.at[b]))
        copies[-1].start()
    for copy in copies:
        copy.wait()


def fold_kernel(stream_hbm, s0, s1, s2, s3, out, stream, shared, sems):
    pairs = [(s, shared.at[k]) for k, s in enumerate((s0, s1, s2, s3))]
    fetched = fetch([(stream_hbm, stream)] + pairs, sems)
    for copy in fetched:
        copy.wait()
    total = stream[...]
    for k in range(4):
        total = total + shared[k].astype(F32)
    out[...] = total


def combine_kernel(returned, mix, base, out):
    routed = jnp.dot(mix[...], returned[...], preferred_element_type=F32)
    for g in range(4):
        lo, hi = g * 1024, (g + 1) * 1024
        out[:, lo:hi] = (base[:, lo:hi] + routed[g * 32 : (g + 1) * 32]).astype(BF)


def attend_kernel(counts, first, last, *refs):
    at = 0

    def take(n):
        nonlocal at
        at += n
        return refs[at - n : at]

    q_own, q_other, core = take(3)
    tiles, planes = [], []
    for n, own_block in counts:
        tiles.append((take(n), take(1)[0], own_block))
        if first and not own_block:
            planes.append(tiles[-1][0][0])
    if not first:
        m_in, l_in, an_in, ab_in = take(4)
    if last:
        own_out, send_out = take(2)
    else:
        m_out, l_out, an_out, ab_out = take(4)

    def keys(ref, lo, hi):
        value = ref[1, :, lo:hi] if any(ref is p for p in planes) else ref[..., lo:hi]
        return value.reshape(-1, hi - lo)

    results = {}
    for group, size, heads, lo, per in (("n", NARROW_SIZE, 4, 0, 2 if last else 4), ("b", BROAD_SIZE, 2, 256, 2)):
        count = per * 128
        scale = size**-0.5 * LOG2E
        base = 0 if group == "n" else 4
        row_base = 0 if group == "n" else 1024
        loaded = []
        for arrays, bias, own_block in tiles:
            k = jnp.concatenate([keys(r, lo, lo + size) for r in arrays], axis=0)
            v = jnp.concatenate([keys(r, lo + size, lo + 2 * size) for r in arrays], axis=0)
            loaded.append((k, v, bias, own_block))
        for side, q_ref in ((0, q_own), (1, q_other)):
            for h0 in range(0, heads, per):
                col = (0 if group == "n" else 512) + h0 * size
                q = jnp.concatenate([q_ref[:, col + i * size : col + (i + 1) * size] for i in range(per)], axis=0)
                rows = row_base + side * heads * 128 + h0 * 128
                arow = rows - row_base
                scores = []
                for k, v, bias, own_block in loaded:
                    s = lax.dot_general(q, k, (((1,), (1,)), ((), ())), preferred_element_type=F32) * scale
                    n = k.shape[0]
                    b = bias[base + h0 : base + h0 + per, :]
                    s = (s.reshape(per, 128, n) + b[:, None, :]).reshape(count, n)
                    if own_block:
                        qi = lax.broadcasted_iota(jnp.int32, (count, n), 0) % 128
                        ki = lax.broadcasted_iota(jnp.int32, (count, n), 1)
                        offset = 0 if side == 0 else 128 * (1 - 2 * core[0])
                        s = jnp.where(ki <= qi + offset, s, MASKED)
                    scores.append(s)
                m = functools.reduce(jnp.maximum, [jnp.max(s, axis=1, keepdims=True) for s in scores])
                if not first:
                    m_old = m_in[pl.ds(rows, count), :][:, :1]
                    m = jnp.maximum(m, m_old)
                l = jnp.zeros((count, 1), F32)
                acc = jnp.zeros((count, size), F32)
                for s, (k, v, bias, own_block) in zip(scores, loaded):
                    p = jnp.exp2(s - m)
                    l = l + jnp.sum(p, axis=1, keepdims=True)
                    acc = acc + jnp.dot(p.astype(BF), v, preferred_element_type=F32)
                if not first:
                    a_in = an_in if group == "n" else ab_in
                    factor = jnp.exp2(m_old - m)
                    l = l + l_in[pl.ds(rows, count), :][:, :1] * factor
                    acc = acc + a_in[pl.ds(arow, count), :] * factor
                if last:
                    out = own_out if side == 0 else send_out
                    o = acc / l
                    lse = m + jnp.log2(l)
                    for i in range(per):
                        out[:, col + i * size : col + (i + 1) * size] = o[i * 128 : (i + 1) * 128].astype(out.dtype)
                        results[(side, base + h0 + i)] = lse[i * 128 : (i + 1) * 128]
                else:
                    a_out = an_out if group == "n" else ab_out
                    m_out[pl.ds(rows, count), :] = jnp.broadcast_to(m, (count, 128))
                    l_out[pl.ds(rows, count), :] = jnp.broadcast_to(l, (count, 128))
                    a_out[pl.ds(arow, count), :] = acc
    if last:
        lane = lax.broadcasted_iota(jnp.int32, (128, 128), 1)
        for side, out in ((0, own_out), (1, send_out)):
            stats = jnp.zeros((128, 128), F32)
            for h in range(6):
                stats = jnp.where(lane % 8 == h, results[(side, h)], stats)
            if side == 1:
                high = stats.astype(BF).astype(F32)
                middle = (stats - high).astype(BF).astype(F32)
                stats = jnp.where(lane < 8, high, jnp.where(lane < 16, middle, stats - high - middle))
            out[:, 1024:1152] = stats.astype(out.dtype)


def attend(q_own, q_other, core, tiles, state, last):
    counts = tuple((len(arrays), own_block) for arrays, _, own_block in tiles)
    operands = [q_own, q_other, core]
    n_keys = 0
    for arrays, bias, _ in tiles:
        operands += list(arrays) + [bias]
        n_keys += bias.shape[1]
    specs = [VMEM] * len(operands)
    specs[2] = SMEM
    if state is not None:
        operands += list(state)
        specs += [VMEM] * 4
    if last:
        shapes = [jax.ShapeDtypeStruct((128, 1152), F32), jax.ShapeDtypeStruct((128, 1152), BF)]
    else:
        shapes = [
            jax.ShapeDtypeStruct((1536, 128), F32),
            jax.ShapeDtypeStruct((1536, 128), F32),
            jax.ShapeDtypeStruct((1024, 128), F32),
            jax.ShapeDtypeStruct((512, 256), F32),
        ]
    return pl.pallas_call(
        functools.partial(attend_kernel, counts, state is None, last),
        out_shape=shapes,
        in_specs=specs,
        out_specs=[VMEM] * len(shapes),
        compiler_params=pltpu.CompilerParams(vmem_limit_bytes=24 * 1024 * 1024),
        cost_estimate=pl.CostEstimate(
            flops=4 * n_keys * 256 * 1024, transcendentals=n_keys * 1536, bytes_accessed=4 * 1024 * 1024
        ),
    )(*operands)


def local(
    query_narrow,
    key_narrow,
    value_narrow,
    gates_narrow,
    query_broad,
    key_broad,
    value_broad,
    gates_broad,
    project_narrow,
    project_broad,
    residual,
    norm_gain,
    route_ids,
    route_weight,
    expert_gate,
    expert_up,
    expert_down,
    shared_gate,
    shared_up,
    shared_down,
):
    z, y, c, t = (lax.axis_index(n).astype(jnp.int32) for n in ("z", "y", "c", "tp"))

    own_kv, q_own = call(
        pack_kernel,
        (key_narrow, value_narrow, key_broad, value_broad, query_narrow, query_broad),
        [shaped((128, 768), BF), shaped((128, 1024), BF)],
        hbm=range(6),
        scratch=[pltpu.SemaphoreType.DMA((6,))],
        moved=0,
    )
    place = jnp.stack([z, y, c, t])
    q_other = swap_core(q_own)
    line = {}
    for k in (2, 1, 3):
        line[k] = turn(own_kv, k, 0)
    target, mix, own_bias, bias_1, bias_2, bias_3 = call(
        tables_kernel,
        (place, route_ids.T, route_weight.T, gates_narrow.T, gates_broad.T),
        [shaped((4, 128), jnp.int32), shaped((128, 1024), BF)] + [shaped((8, n), F32) for n in (128, 384, 1024, 512)],
        smem=(0,),
        hbm=(1, 2, 3, 4),
        scratch=[
            pltpu.VMEM((4, 32), jnp.int32),
            pltpu.VMEM((4, 32), F32),
            pltpu.VMEM((4, 4096), F32),
            pltpu.VMEM((2, 4096), F32),
            pltpu.SemaphoreType.DMA((4,)),
        ],
    )
    low, high = call(
        stack_kernel,
        [own_kv] + [line[k] for k in ORDER[1:]] + [target, own_bias],
        [shaped((2, 128, 768), BF)] * 2,
    )
    low_back = turn(low, 1, 1)
    high_ahead = turn(high, 3, 1)
    low_ahead = turn(low, 3, 1)
    high_back = turn(high, 1, 1)
    low_far = turn(low_back, 1, 1)
    high_far = turn(high_ahead, 3, 1)

    core = c.reshape(1)
    first_tiles = [((own_kv,), own_bias, True), ((low, high), bias_1, False)]
    state = attend(q_own, q_other, core, first_tiles, None, False)
    second_tiles = [((low_back, low_ahead, high_back, high_ahead), bias_2, False)]
    state = attend(q_own, q_other, core, second_tiles, state, False)
    own_part, send_part = attend(q_own, q_other, core, [((low_far, high_far), bias_3, False)], state, True)
    other_part = swap_core(send_part)

    p0, p1, p2, p3 = call(
        project_kernel,
        (place, own_part, other_part, project_narrow, project_broad),
        [shaped((32, 4096), BF)] * 4,
        smem=(0,),
        scratch=[pltpu.VMEM((128, 4096), F32), pltpu.VMEM((128, 1024), BF)],
        flops=2 * 128 * 1024 * 4096,
    )
    p2 = shift(p2, "tp", 2)
    p1 = shift(p1, "tp", 1)
    p3 = shift(p3, "tp", 3)

    stream, normed, outbound = call(
        dispatch_kernel,
        (place, p0, p1, p2, p3, residual, norm_gain.reshape(1, -1), target),
        [pltpu.HBM((32, 4096), F32), shaped((32, 4096), BF), pltpu.HBM((1024, 1024), BF)],
        smem=(0,),
        hbm_out=(0, 2),
        scratch=[pltpu.VMEM((32, 4096), F32), pltpu.VMEM((1024, 1024), BF), pltpu.SemaphoreType.DMA((5,))],
        flops=2 * 1024 * 128 * 1024,
    )
    every = SP + ("tp",)
    inbound = lax.all_to_all(outbound.reshape(128, 8, 1024), every, 0, 0, tiled=True)

    n1 = shift(normed, "tp", 1)
    n2 = shift(normed, "tp", 2)
    n3 = shift(normed, "tp", 3)
    s0, s1, s2, s3 = call(
        shared_kernel,
        (normed, n1, n2, n3, shared_gate, shared_up, shared_down),
        [shaped((32, 4096), BF)] * 4,
        hbm=range(7),
        scratch=[
            pltpu.VMEM((128, 4096), BF),
            pltpu.VMEM((4096, 256), BF),
            pltpu.VMEM((4096, 256), BF),
            pltpu.VMEM((256, 4096), BF),
            pltpu.SemaphoreType.DMA((7,)),
        ],
        mib=20,
        flops=2 * 128 * 4096 * 768,
    )
    s1 = shift(s1, "tp", 3)
    s2 = shift(s2, "tp", 2)
    s3 = shift(s3, "tp", 1)

    (result,) = call(
        expert_kernel,
        (inbound.reshape(1024, 1024), expert_gate, expert_up, expert_down),
        [pltpu.HBM((1024, 1024), BF)],
        hbm=(1, 2, 3),
        hbm_out=(0,),
        scratch=[
            pltpu.VMEM((256, 4096), BF),
            pltpu.VMEM((1024, 1024), BF),
            pltpu.VMEM((4096, 256), BF),
            pltpu.VMEM((4096, 256), BF),
            pltpu.VMEM((256, 4096), BF),
            pltpu.SemaphoreType.DMA((9,)),
            pltpu.SemaphoreType.DMA((4,)),
        ],
        mib=20,
        flops=2 * 256 * 4096 * 768,
    )
    returned = lax.all_to_all(result.reshape(128, 8, 1024), every, 0, 0, tiled=True)
    (base,) = call(
        fold_kernel,
        (stream, s0, s1, s2, s3),
        [shaped((32, 4096), F32)],
        hbm=range(5),
        scratch=[pltpu.VMEM((32, 4096), F32), pltpu.VMEM((4, 32, 4096), BF), pltpu.SemaphoreType.DMA((5,))],
    )
    (out,) = call(
        combine_kernel,
        (returned.reshape(1024, 1024), mix, base),
        [shaped((32, 4096), BF)],
        flops=2 * 128 * 1024 * 1024,
    )
    return out


def solution(mesh):
    mesh = Mesh(mesh.devices.reshape(4, 4, 2, 4), ("z", "y", "c", "tp"))
    every = SP + ("tp",)
    placed = (
        P(SP, "tp"),
        P(SP, "tp"),
        P(SP, "tp"),
        P(None, "tp"),
        P(SP, "tp"),
        P(SP, "tp"),
        P(SP, "tp"),
        P(None, "tp"),
        P("tp", None),
        P("tp", None),
        P(SP, None),
        P(),
        P(every, None),
        P(every, None),
        P(every, None, None),
        P(every, None, None),
        P(every, None, None),
        P(None, "tp"),
        P(None, "tp"),
        P("tp", None),
    )

    return jax.shard_map(local, mesh=mesh, in_specs=placed, out_specs=P(every, None), check_vma=False)
```

```python
import functools

import jax
import jax.numpy as jnp
from jax import lax
from jax.experimental import pallas as pl
from jax.experimental.pallas import tpu as pltpu
from jax.sharding import Mesh
from jax.sharding import PartitionSpec as P


SP = ("z", "y", "c")
NARROW_SIZE = 128
BROAD_SIZE = 256
LOG2E = 1.4426950408889634
MASKED = -1e30
EPSILON = 1e-06
ORDER = (0, 1, 3, 2)
VMEM = pl.BlockSpec(memory_space=pltpu.VMEM)
SMEM = pl.BlockSpec(memory_space=pltpu.SMEM)
HBM = pl.BlockSpec(memory_space=pltpu.HBM)
BF = jnp.bfloat16
F32 = jnp.float32


def shift(x, axis, k):
    return lax.ppermute(x, axis, [(i, (i + k) % 4) for i in range(4)])


def swap_core(x):
    return lax.ppermute(x, "c", [(0, 1), (1, 0)])


def turn(x, k, phase):
    pairs = []
    for z in range(4):
        for y in range(4):
            for c in range(2):
                to_z, to_y = (z, (y + k) % 4) if c == phase else ((z + k) % 4, y)
                pairs.append(((z * 4 + y) * 2 + c, (to_z * 4 + to_y) * 2 + c))
    return lax.ppermute(x, SP, pairs)


def call(kernel, operands, shapes, smem=(), hbm=(), hbm_out=(), scratch=(), mib=16, flops=0, moved=2**21):
    operands = [
        pltpu.with_memory_space_constraint(x, pltpu.HBM) if i in hbm else x for i, x in enumerate(operands)
    ]
    return pl.pallas_call(
        kernel,
        out_shape=shapes,
        in_specs=[SMEM if i in smem else HBM if i in hbm else VMEM for i in range(len(operands))],
        out_specs=[HBM if i in hbm_out else VMEM for i in range(len(shapes))],
        scratch_shapes=list(scratch),
        compiler_params=pltpu.CompilerParams(vmem_limit_bytes=mib * 1024 * 1024),
        cost_estimate=pl.CostEstimate(flops=flops, transcendentals=0, bytes_accessed=moved),
    )(*operands)


def shaped(shape, dtype):
    return jax.ShapeDtypeStruct(shape, dtype)


def pack_kernel(kn, vn, kb, vb, qn, qb, kv, q, sems):
    copies = []
    for ref, out, at in ((kn, kv, 0), (vn, kv, 128), (kb, kv, 256), (vb, kv, 512), (qn, q, 0), (qb, q, 512)):
        target = out.at[:, at : at + ref.shape[1]]
        copies.append(pltpu.make_async_copy(ref, target, sems.at[len(copies)]))
    for copy in copies:
        copy.start()
    for copy in copies:
        copy.wait()


def stack_kernel(a, b, c, d, routed, biased, low, high):
    for out, i, ref in ((low, 0, a), (low, 1, b), (high, 0, c), (high, 1, d)):
        out[i] = ref[...]


def tables_kernel(place, ids_hbm, weight_hbm, narrow_hbm, broad_hbm, target, mix, own, first, second, third, fourth, *scratch):
    ids_in, weight_in, narrow, broad, sems = scratch
    copies = []
    for ref, held in ((narrow_hbm, narrow), (broad_hbm, broad), (ids_hbm, ids_in), (weight_hbm, weight_in)):
        copies.append(pltpu.make_async_copy(ref, held, sems.at[len(copies)]))
    for copy in copies:
        copy.start()
    for copy in copies:
        copy.wait()
    ids = jnp.concatenate([ids_in[...]] * 4, axis=1)
    weight = jnp.concatenate([weight_in[...].astype(BF).astype(F32)] * 4, axis=1)
    expert = lax.broadcasted_iota(jnp.int32, (128, 128), 0)
    column = lax.broadcasted_iota(jnp.int32, (128, 128), 1)
    named = jnp.zeros((128, 128), F32)
    for k in range(4):
        named = named + jnp.where(expert == ids[k : k + 1, :], 1.0, 0.0)
    earlier = jnp.where((expert < 32) & (expert < column % 32), 1.0, 0.0).astype(BF)
    before = jnp.dot(named.astype(BF), earlier, preferred_element_type=F32)
    row = lax.broadcasted_iota(jnp.int32, (1024, 128), 0)
    total = jnp.zeros((1024, 128), F32)
    for k in range(4):
        slot = jnp.sum(jnp.where(expert == ids[k : k + 1, :], before, 0.0), axis=0, keepdims=True)
        start = ids[k : k + 1, :] * 8 + slot.astype(jnp.int32) * 4 + column[:1] // 32
        target[k : k + 1, :] = start
        total = total + jnp.where(row == start, weight[k : k + 1, :], 0.0)
    mix[...] = total.T.astype(BF)


    z, y, c = place[0], place[1], place[2]
    here = z * 4 + y

    def put(out, at, early, late):
        back_y = jnp.where(c == 0, early, late)
        back_z = jnp.where(c == 0, late, early)
        chip = ((z + 4 - back_z) % 4) * 4 + (y + 4 - back_y) % 4
        block = pl.multiple_of(chip * 256 + c * 128, 128)
        ahead = chip > here
        for row, gates in ((0, narrow), (4, broad)):
            piece = gates[:, pl.ds(block, 128)] * (-LOG2E)
            out[row : row + gates.shape[0], at : at + 128] = jnp.where(ahead, MASKED, piece)

    put(own, 0, 0, 0)
    for i in range(1, 4):
        put(first, (i - 1) * 128, ORDER[i], 0)
    for i in range(4):
        put(second, i * 128, ORDER[i], 1 if i < 2 else 3)
        put(third, i * 128, ORDER[i], 3 if i < 2 else 1)
        put(fourth, i * 128, ORDER[i], 2)


def project_kernel(place, own, other, narrow, broad, *refs):
    outs, total, attn = refs[:4], *refs[4:]
    a, b = own[:, 1024:], other[:, 1024:].astype(F32)
    b = b + pltpu.roll(b, 120, 1) + pltpu.roll(b, 112, 1)
    top = jnp.maximum(a, b)
    wa, wb = jnp.exp2(a - top), jnp.exp2(b - top)
    joined = wa + wb
    wa, wb = wa / joined, wb / joined
    for h in range(6):
        lo, size = (h * 128, 128) if h < 4 else (512 + (h - 4) * 256, 256)
        value = own[:, lo : lo + size] * wa[:, h : h + 1] + other[:, lo : lo + size].astype(F32) * wb[:, h : h + 1]
        attn[:, lo : lo + size] = value.astype(BF)
    for at in range(0, 4096, 1024):
        part = jnp.dot(attn[:, :512], narrow[:, at : at + 1024], preferred_element_type=F32)
        part = part + jnp.dot(attn[:, 512:], broad[:, at : at + 1024], preferred_element_type=F32)
        total[:, at : at + 1024] = part
    for k in range(4):
        outs[k][...] = total[pl.ds(((place[3] + k) % 4) * 32, 32), :].astype(BF)


def dispatch_kernel(place, p0, p1, p2, p3, residual, gain, target, stream_out, normed_out, out, stream_held, rows, sems):
    mixture = p0[...].astype(F32) + p1[...].astype(F32) + p2[...].astype(F32) + p3[...].astype(F32)
    stream = residual[pl.ds(place[3] * 32, 32), :].astype(F32) + mixture
    stream_held[...] = stream
    copies = [pltpu.make_async_copy(stream_held, stream_out, sems.at[4])]
    copies[0].start()
    scale = lax.rsqrt(jnp.mean(stream * stream, axis=1, keepdims=True) + EPSILON)
    normed = (stream * scale * gain[...]).astype(BF)
    normed_out[...] = normed
    cut = jnp.concatenate([normed[:, g * 1024 : (g + 1) * 1024] for g in range(4)], axis=0)
    row = lax.broadcasted_iota(jnp.int32, (256, 128), 0)
    for at in range(0, 1024, 256):
        pick = row + at == target[0:1, :]
        for k in range(1, 4):
            pick = pick | (row + at == target[k : k + 1, :])
        rows[at : at + 256, :] = jnp.dot(pick.astype(F32).astype(BF), cut, preferred_element_type=F32).astype(BF)
        part = pl.ds(at, 256)
        copies.append(pltpu.make_async_copy(rows.at[part], out.at[part], sems.at[at // 256]))
        copies[-1].start()
    for copy in copies:
        copy.wait()


def fetch(pairs, sems):
    copies = [pltpu.make_async_copy(ref, held, sems.at[i]) for i, (ref, held) in enumerate(pairs)]
    for copy in copies:
        copy.start()
    return copies


def silu(v):
    return v / (1.0 + jnp.exp(-v))


def shared_kernel(n0, n1, n2, n3, gate_hbm, up_hbm, down_hbm, o0, o1, o2, o3, x, gate, up, down, sems):
    pairs = [(n, x.at[pl.ds(k * 32, 32)]) for k, n in enumerate((n0, n1, n2, n3))]
    fetched = fetch(pairs + [(gate_hbm, gate), (up_hbm, up), (down_hbm, down)], sems)
    for copy in fetched[:5]:
        copy.wait()
    x = x[...]
    g = jnp.dot(x, gate[...], preferred_element_type=F32)
    fetched[5].wait()
    u = jnp.dot(x, up[...], preferred_element_type=F32)
    fetched[6].wait()
    hidden = (silu(g) * u).astype(BF)
    for at in range(0, 4096, 1024):
        part = jnp.dot(hidden, down[:, at : at + 1024], preferred_element_type=F32).astype(BF)
        for k, out in enumerate((o0, o1, o2, o3)):
            out[:, at : at + 1024] = part[k * 32 : (k + 1) * 32]


def expert_kernel(inbound, gate_hbm, up_hbm, down_hbm, out, x, rows_out, gate, up, down, weight_sems, sems):
    pairs = []
    for g in range(4):
        part = pl.ds(g * 1024, 1024)
        pairs += [(ref.at[0, part], held.at[part]) for ref, held in ((gate_hbm, gate), (up_hbm, up))]
    fetched = fetch(pairs + [(down_hbm.at[0], down)], weight_sems)
    i = lax.broadcasted_iota(jnp.int32, (256, 256), 0)
    j = lax.broadcasted_iota(jnp.int32, (256, 256), 1)
    order = (j == ((i % 64) // 2) * 8 + (i % 2) * 4 + i // 64).astype(F32).astype(BF)
    back = (i == ((j % 64) // 2) * 8 + (j % 2) * 4 + j // 64).astype(F32).astype(BF)
    for b in range(4):
        rows = jnp.dot(order, inbound[b * 256 : (b + 1) * 256, :], preferred_element_type=F32).astype(BF)
        for g in range(4):
            x[b * 64 : (b + 1) * 64, g * 1024 : (g + 1) * 1024] = rows[g * 64 : (g + 1) * 64]
    gated, upped = jnp.zeros((256, 256), F32), jnp.zeros((256, 256), F32)
    for g in range(4):
        lo, hi = g * 1024, (g + 1) * 1024
        fetched[2 * g].wait()
        fetched[2 * g + 1].wait()
        gated = gated + jnp.dot(x[:, lo:hi], gate[lo:hi], preferred_element_type=F32)
        upped = upped + jnp.dot(x[:, lo:hi], up[lo:hi], preferred_element_type=F32)
    fetched[8].wait()
    hidden = (silu(gated) * upped).astype(BF)
    for g in range(4):
        part = jnp.dot(hidden, down[:, g * 1024 : (g + 1) * 1024], preferred_element_type=F32)
        x[:, g * 1024 : (g + 1) * 1024] = part.astype(BF)
    copies = []
    for b in range(4):
        rows = jnp.concatenate([x[b * 64 : (b + 1) * 64, g * 1024 : (g + 1) * 1024] for g in range(4)], axis=0)
        part = pl.ds(b * 256, 256)
        rows_out[part, :] = jnp.dot(back, rows, preferred_element_type=F32).astype(BF)
        copies.append(pltpu.make_async_copy(rows_out.at[part], out.at[part], sems.at[b]))
        copies[-1].start()
    for copy in copies:
        copy.wait()


def fold_kernel(stream_hbm, s0, s1, s2, s3, out, stream, shared, sems):
    pairs = [(s, shared.at[k]) for k, s in enumerate((s0, s1, s2, s3))]
    fetched = fetch([(stream_hbm, stream)] + pairs, sems)
    for copy in fetched:
        copy.wait()
    total = stream[...]
    for k in range(4):
        total = total + shared[k].astype(F32)
    out[...] = total


def combine_kernel(returned, mix, base, out):
    routed = jnp.dot(mix[...], returned[...], preferred_element_type=F32)
    for g in range(4):
        lo, hi = g * 1024, (g + 1) * 1024
        out[:, lo:hi] = (base[:, lo:hi] + routed[g * 32 : (g + 1) * 32]).astype(BF)


def attend_kernel(counts, first, last, *refs):
    at = 0

    def take(n):
        nonlocal at
        at += n
        return refs[at - n : at]

    q_own, q_other, core = take(3)
    tiles, planes = [], []
    for n, own_block in counts:
        tiles.append((take(n), take(1)[0], own_block))
        if first and not own_block:
            planes.append(tiles[-1][0][0])
    if not first:
        m_in, l_in, an_in, ab_in = take(4)
    if last:
        own_out, send_out = take(2)
    else:
        m_out, l_out, an_out, ab_out = take(4)

    def keys(ref, lo, hi):
        value = ref[1, :, lo:hi] if any(ref is p for p in planes) else ref[..., lo:hi]
        return value.reshape(-1, hi - lo)

    results = {}
    for group, size, heads, lo, per in (("n", NARROW_SIZE, 4, 0, 4 if first else 2), ("b", BROAD_SIZE, 2, 256, 2)):
        count = per * 128
        scale = size**-0.5 * LOG2E
        base = 0 if group == "n" else 4
        row_base = 0 if group == "n" else 1024
        loaded = []
        for arrays, bias, own_block in tiles:
            k = jnp.concatenate([keys(r, lo, lo + size) for r in arrays], axis=0)
            v = jnp.concatenate([keys(r, lo + size, lo + 2 * size) for r in arrays], axis=0)
            loaded.append((k, v, bias, own_block))
        for side, q_ref in ((0, q_own), (1, q_other)):
            for h0 in range(0, heads, per):
                col = (0 if group == "n" else 512) + h0 * size
                q = jnp.concatenate([q_ref[:, col + i * size : col + (i + 1) * size] for i in range(per)], axis=0)
                rows = row_base + side * heads * 128 + h0 * 128
                arow = rows - row_base
                scores = []
                for k, v, bias, own_block in loaded:
                    s = lax.dot_general(q, k, (((1,), (1,)), ((), ())), preferred_element_type=F32) * scale
                    n = k.shape[0]
                    b = bias[base + h0 : base + h0 + per, :]
                    s = (s.reshape(per, 128, n) + b[:, None, :]).reshape(count, n)
                    if own_block:
                        qi = lax.broadcasted_iota(jnp.int32, (count, n), 0) % 128
                        ki = lax.broadcasted_iota(jnp.int32, (count, n), 1)
                        offset = 0 if side == 0 else 128 * (1 - 2 * core[0])
                        s = jnp.where(ki <= qi + offset, s, MASKED)
                    scores.append(s)
                m = functools.reduce(jnp.maximum, [jnp.max(s, axis=1, keepdims=True) for s in scores])
                if not first:
                    m_old = m_in[pl.ds(rows, count), :][:, :1]
                    m = jnp.maximum(m, m_old)
                l = jnp.zeros((count, 1), F32)
                acc = jnp.zeros((count, size), F32)
                for s, (k, v, bias, own_block) in zip(scores, loaded):
                    p = jnp.exp2(s - m)
                    l = l + jnp.sum(p, axis=1, keepdims=True)
                    acc = acc + jnp.dot(p.astype(BF), v, preferred_element_type=F32)
                if not first:
                    a_in = an_in if group == "n" else ab_in
                    factor = jnp.exp2(m_old - m)
                    l = l + l_in[pl.ds(rows, count), :][:, :1] * factor
                    acc = acc + a_in[pl.ds(arow, count), :] * factor
                if last:
                    out = own_out if side == 0 else send_out
                    o = acc / l
                    lse = m + jnp.log2(l)
                    for i in range(per):
                        out[:, col + i * size : col + (i + 1) * size] = o[i * 128 : (i + 1) * 128].astype(out.dtype)
                        results[(side, base + h0 + i)] = lse[i * 128 : (i + 1) * 128]
                else:
                    a_out = an_out if group == "n" else ab_out
                    m_out[pl.ds(rows, count), :] = jnp.broadcast_to(m, (count, 128))
                    l_out[pl.ds(rows, count), :] = jnp.broadcast_to(l, (count, 128))
                    a_out[pl.ds(arow, count), :] = acc
    if last:
        lane = lax.broadcasted_iota(jnp.int32, (128, 128), 1)
        for side, out in ((0, own_out), (1, send_out)):
            stats = jnp.zeros((128, 128), F32)
            for h in range(6):
                stats = jnp.where(lane % 8 == h, results[(side, h)], stats)
            if side == 1:
                high = stats.astype(BF).astype(F32)
                middle = (stats - high).astype(BF).astype(F32)
                stats = jnp.where(lane < 8, high, jnp.where(lane < 16, middle, stats - high - middle))
            out[:, 1024:1152] = stats.astype(out.dtype)


def attend(q_own, q_other, core, tiles, state, last):
    counts = tuple((len(arrays), own_block) for arrays, _, own_block in tiles)
    operands = [q_own, q_other, core]
    n_keys = 0
    for arrays, bias, _ in tiles:
        operands += list(arrays) + [bias]
        n_keys += bias.shape[1]
    specs = [VMEM] * len(operands)
    specs[2] = SMEM
    if state is not None:
        operands += list(state)
        specs += [VMEM] * 4
    if last:
        shapes = [jax.ShapeDtypeStruct((128, 1152), F32), jax.ShapeDtypeStruct((128, 1152), BF)]
    else:
        shapes = [
            jax.ShapeDtypeStruct((1536, 128), F32),
            jax.ShapeDtypeStruct((1536, 128), F32),
            jax.ShapeDtypeStruct((1024, 128), F32),
            jax.ShapeDtypeStruct((512, 256), F32),
        ]
    return pl.pallas_call(
        functools.partial(attend_kernel, counts, state is None, last),
        out_shape=shapes,
        in_specs=specs,
        out_specs=[VMEM] * len(shapes),
        compiler_params=pltpu.CompilerParams(vmem_limit_bytes=24 * 1024 * 1024),
        cost_estimate=pl.CostEstimate(
            flops=4 * n_keys * 256 * 1024, transcendentals=n_keys * 1536, bytes_accessed=4 * 1024 * 1024
        ),
    )(*operands)


def local(
    query_narrow,
    key_narrow,
    value_narrow,
    gates_narrow,
    query_broad,
    key_broad,
    value_broad,
    gates_broad,
    project_narrow,
    project_broad,
    residual,
    norm_gain,
    route_ids,
    route_weight,
    expert_gate,
    expert_up,
    expert_down,
    shared_gate,
    shared_up,
    shared_down,
):
    z, y, c, t = (lax.axis_index(n).astype(jnp.int32) for n in ("z", "y", "c", "tp"))

    own_kv, q_own = call(
        pack_kernel,
        (key_narrow, value_narrow, key_broad, value_broad, query_narrow, query_broad),
        [shaped((128, 768), BF), shaped((128, 1024), BF)],
        hbm=range(6),
        scratch=[pltpu.SemaphoreType.DMA((6,))],
        moved=0,
    )
    place = jnp.stack([z, y, c, t])
    q_other = swap_core(q_own)
    line = {}
    for k in (2, 1, 3):
        line[k] = turn(own_kv, k, 0)
    target, mix, own_bias, bias_1, bias_2, bias_3, bias_4 = call(
        tables_kernel,
        (place, route_ids.T, route_weight.T, gates_narrow.T, gates_broad.T),
        [shaped((4, 128), jnp.int32), shaped((128, 1024), BF)] + [shaped((8, n), F32) for n in (128, 384, 512, 512, 512)],
        smem=(0,),
        hbm=(1, 2, 3, 4),
        scratch=[
            pltpu.VMEM((4, 32), jnp.int32),
            pltpu.VMEM((4, 32), F32),
            pltpu.VMEM((4, 4096), F32),
            pltpu.VMEM((2, 4096), F32),
            pltpu.SemaphoreType.DMA((4,)),
        ],
    )
    low, high = call(
        stack_kernel,
        [own_kv] + [line[k] for k in ORDER[1:]] + [target, own_bias],
        [shaped((2, 128, 768), BF)] * 2,
    )
    low_back = turn(low, 1, 1)
    high_ahead = turn(high, 3, 1)
    low_ahead = turn(low, 3, 1)
    high_back = turn(high, 1, 1)
    low_far = turn(low_back, 1, 1)
    high_far = turn(high_ahead, 3, 1)

    core = c.reshape(1)
    first_tiles = [((own_kv,), own_bias, True), ((low, high), bias_1, False)]
    state = attend(q_own, q_other, core, first_tiles, None, False)
    state = attend(q_own, q_other, core, [((low_back, high_ahead), bias_2, False)], state, False)
    state = attend(q_own, q_other, core, [((low_ahead, high_back), bias_3, False)], state, False)
    own_part, send_part = attend(q_own, q_other, core, [((low_far, high_far), bias_4, False)], state, True)
    other_part = swap_core(send_part)

    p0, p1, p2, p3 = call(
        project_kernel,
        (place, own_part, other_part, project_narrow, project_broad),
        [shaped((32, 4096), BF)] * 4,
        smem=(0,),
        scratch=[pltpu.VMEM((128, 4096), F32), pltpu.VMEM((128, 1024), BF)],
        flops=2 * 128 * 1024 * 4096,
    )
    p2 = shift(p2, "tp", 2)
    p1 = shift(p1, "tp", 1)
    p3 = shift(p3, "tp", 3)

    stream, normed, outbound = call(
        dispatch_kernel,
        (place, p0, p1, p2, p3, residual, norm_gain.reshape(1, -1), target),
        [pltpu.HBM((32, 4096), F32), shaped((32, 4096), BF), pltpu.HBM((1024, 1024), BF)],
        smem=(0,),
        hbm_out=(0, 2),
        scratch=[pltpu.VMEM((32, 4096), F32), pltpu.VMEM((1024, 1024), BF), pltpu.SemaphoreType.DMA((5,))],
        flops=2 * 1024 * 128 * 1024,
    )
    every = SP + ("tp",)
    inbound = lax.all_to_all(outbound.reshape(128, 8, 1024), every, 0, 0, tiled=True)

    n1 = shift(normed, "tp", 1)
    n2 = shift(normed, "tp", 2)
    n3 = shift(normed, "tp", 3)
    s0, s1, s2, s3 = call(
        shared_kernel,
        (normed, n1, n2, n3, shared_gate, shared_up, shared_down),
        [shaped((32, 4096), BF)] * 4,
        hbm=range(7),
        scratch=[
            pltpu.VMEM((128, 4096), BF),
            pltpu.VMEM((4096, 256), BF),
            pltpu.VMEM((4096, 256), BF),
            pltpu.VMEM((256, 4096), BF),
            pltpu.SemaphoreType.DMA((7,)),
        ],
        mib=20,
        flops=2 * 128 * 4096 * 768,
    )
    s1 = shift(s1, "tp", 3)
    s2 = shift(s2, "tp", 2)
    s3 = shift(s3, "tp", 1)

    (result,) = call(
        expert_kernel,
        (inbound.reshape(1024, 1024), expert_gate, expert_up, expert_down),
        [pltpu.HBM((1024, 1024), BF)],
        hbm=(1, 2, 3),
        hbm_out=(0,),
        scratch=[
            pltpu.VMEM((256, 4096), BF),
            pltpu.VMEM((1024, 1024), BF),
            pltpu.VMEM((4096, 256), BF),
            pltpu.VMEM((4096, 256), BF),
            pltpu.VMEM((256, 4096), BF),
            pltpu.SemaphoreType.DMA((9,)),
            pltpu.SemaphoreType.DMA((4,)),
        ],
        mib=20,
        flops=2 * 256 * 4096 * 768,
    )
    returned = lax.all_to_all(result.reshape(128, 8, 1024), every, 0, 0, tiled=True)
    (base,) = call(
        fold_kernel,
        (stream, s0, s1, s2, s3),
        [shaped((32, 4096), F32)],
        hbm=range(5),
        scratch=[pltpu.VMEM((32, 4096), F32), pltpu.VMEM((4, 32, 4096), BF), pltpu.SemaphoreType.DMA((5,))],
    )
    (out,) = call(
        combine_kernel,
        (returned.reshape(1024, 1024), mix, base),
        [shaped((32, 4096), BF)],
        flops=2 * 128 * 1024 * 1024,
    )
    return out


def solution(mesh):
    mesh = Mesh(mesh.devices.reshape(4, 4, 2, 4), ("z", "y", "c", "tp"))
    every = SP + ("tp",)
    placed = (
        P(SP, "tp"),
        P(SP, "tp"),
        P(SP, "tp"),
        P(None, "tp"),
        P(SP, "tp"),
        P(SP, "tp"),
        P(SP, "tp"),
        P(None, "tp"),
        P("tp", None),
        P("tp", None),
        P(SP, None),
        P(),
        P(every, None),
        P(every, None),
        P(every, None, None),
        P(every, None, None),
        P(every, None, None),
        P(None, "tp"),
        P(None, "tp"),
        P("tp", None),
    )

    return jax.shard_map(local, mesh=mesh, in_specs=placed, out_specs=P(every, None), check_vma=False)
```

```python
import functools

import jax
import jax.numpy as jnp
from jax import lax
from jax.experimental import pallas as pl
from jax.experimental.pallas import tpu as pltpu
from jax.sharding import Mesh
from jax.sharding import PartitionSpec as P


SP = ("z", "y", "c")
NARROW_SIZE = 128
BROAD_SIZE = 256
LOG2E = 1.4426950408889634
MASKED = -1e30
EPSILON = 1e-06
ORDER = (0, 1, 3, 2)
VMEM = pl.BlockSpec(memory_space=pltpu.VMEM)
SMEM = pl.BlockSpec(memory_space=pltpu.SMEM)
HBM = pl.BlockSpec(memory_space=pltpu.HBM)
BF = jnp.bfloat16
F32 = jnp.float32


def shift(x, axis, k):
    return lax.ppermute(x, axis, [(i, (i + k) % 4) for i in range(4)])


def swap_core(x):
    return lax.ppermute(x, "c", [(0, 1), (1, 0)])


def turn(x, k, phase):
    pairs = []
    for z in range(4):
        for y in range(4):
            for c in range(2):
                to_z, to_y = (z, (y + k) % 4) if c == phase else ((z + k) % 4, y)
                pairs.append(((z * 4 + y) * 2 + c, (to_z * 4 + to_y) * 2 + c))
    return lax.ppermute(x, SP, pairs)


def call(kernel, operands, shapes, smem=(), hbm=(), hbm_out=(), scratch=(), mib=16, flops=0, moved=2**21):
    operands = [
        pltpu.with_memory_space_constraint(x, pltpu.HBM) if i in hbm else x for i, x in enumerate(operands)
    ]
    return pl.pallas_call(
        kernel,
        out_shape=shapes,
        in_specs=[SMEM if i in smem else HBM if i in hbm else VMEM for i in range(len(operands))],
        out_specs=[HBM if i in hbm_out else VMEM for i in range(len(shapes))],
        scratch_shapes=list(scratch),
        compiler_params=pltpu.CompilerParams(vmem_limit_bytes=mib * 1024 * 1024),
        cost_estimate=pl.CostEstimate(flops=flops, transcendentals=0, bytes_accessed=moved),
    )(*operands)


def shaped(shape, dtype):
    return jax.ShapeDtypeStruct(shape, dtype)


def pack_kernel(kn, vn, kb, vb, qn, qb, kv, q, sems):
    copies = []
    for ref, out, at in ((kn, kv, 0), (vn, kv, 128), (kb, kv, 256), (vb, kv, 512), (qn, q, 0), (qb, q, 512)):
        target = out.at[:, at : at + ref.shape[1]]
        copies.append(pltpu.make_async_copy(ref, target, sems.at[len(copies)]))
    for copy in copies:
        copy.start()
    for copy in copies:
        copy.wait()


def stack_kernel(a, b, c, d, routed, biased, low, high):
    for out, i, ref in ((low, 0, a), (low, 1, b), (high, 0, c), (high, 1, d)):
        out[i] = ref[...]


def tables_kernel(place, ids_hbm, weight_hbm, narrow_hbm, broad_hbm, target, mix, own, first, second, third, fourth, *scratch):
    ids_in, weight_in, narrow, broad, sems = scratch
    copies = []
    for ref, held in ((narrow_hbm, narrow), (broad_hbm, broad), (ids_hbm, ids_in), (weight_hbm, weight_in)):
        copies.append(pltpu.make_async_copy(ref, held, sems.at[len(copies)]))
    for copy in copies:
        copy.start()
    for copy in copies:
        copy.wait()
    ids = jnp.concatenate([ids_in[...]] * 4, axis=1)
    weight = jnp.concatenate([weight_in[...].astype(BF).astype(F32)] * 4, axis=1)
    expert = lax.broadcasted_iota(jnp.int32, (128, 128), 0)
    column = lax.broadcasted_iota(jnp.int32, (128, 128), 1)
    named = jnp.zeros((128, 128), F32)
    for k in range(4):
        named = named + jnp.where(expert == ids[k : k + 1, :], 1.0, 0.0)
    earlier = jnp.where((expert < 32) & (expert < column % 32), 1.0, 0.0).astype(BF)
    before = jnp.dot(named.astype(BF), earlier, preferred_element_type=F32)
    row = lax.broadcasted_iota(jnp.int32, (1024, 128), 0)
    total = jnp.zeros((1024, 128), F32)
    for k in range(4):
        slot = jnp.sum(jnp.where(expert == ids[k : k + 1, :], before, 0.0), axis=0, keepdims=True)
        start = ids[k : k + 1, :] * 8 + slot.astype(jnp.int32) * 4 + column[:1] // 32
        target[k : k + 1, :] = start
        total = total + jnp.where(row == start, weight[k : k + 1, :], 0.0)
    mix[...] = total.T.astype(BF)


    z, y, c = place[0], place[1], place[2]
    here = z * 4 + y

    def put(out, at, early, late):
        back_y = jnp.where(c == 0, early, late)
        back_z = jnp.where(c == 0, late, early)
        chip = ((z + 4 - back_z) % 4) * 4 + (y + 4 - back_y) % 4
        block = pl.multiple_of(chip * 256 + c * 128, 128)
        ahead = chip > here
        for row, gates in ((0, narrow), (4, broad)):
            piece = gates[:, pl.ds(block, 128)] * (-LOG2E)
            out[row : row + gates.shape[0], at : at + 128] = jnp.where(ahead, MASKED, piece)

    put(own, 0, 0, 0)
    for i in range(1, 4):
        put(first, (i - 1) * 128, ORDER[i], 0)
    for i in range(4):
        put(second, i * 128, ORDER[i], 1 if i < 2 else 3)
        put(third, i * 128, ORDER[i], 3 if i < 2 else 1)
        put(fourth, i * 128, ORDER[i], 2)


def project_kernel(place, own, other, narrow, broad, *refs):
    outs, total, attn = refs[:4], *refs[4:]
    a, b = own[:, 1024:], other[:, 1024:].astype(F32)
    b = b + pltpu.roll(b, 120, 1) + pltpu.roll(b, 112, 1)
    top = jnp.maximum(a, b)
    wa, wb = jnp.exp2(a - top), jnp.exp2(b - top)
    joined = wa + wb
    wa, wb = wa / joined, wb / joined
    for h in range(6):
        lo, size = (h * 128, 128) if h < 4 else (512 + (h - 4) * 256, 256)
        value = own[:, lo : lo + size] * wa[:, h : h + 1] + other[:, lo : lo + size].astype(F32) * wb[:, h : h + 1]
        attn[:, lo : lo + size] = value.astype(BF)
    for at in range(0, 4096, 1024):
        part = jnp.dot(attn[:, :512], narrow[:, at : at + 1024], preferred_element_type=F32)
        part = part + jnp.dot(attn[:, 512:], broad[:, at : at + 1024], preferred_element_type=F32)
        total[:, at : at + 1024] = part
    for k in range(4):
        outs[k][...] = total[pl.ds(((place[3] + k) % 4) * 32, 32), :].astype(BF)


def dispatch_kernel(place, p0, p1, p2, p3, residual, gain, target, stream_out, normed_out, out, stream_held, rows, sems):
    mixture = p0[...].astype(F32) + p1[...].astype(F32) + p2[...].astype(F32) + p3[...].astype(F32)
    stream = residual[pl.ds(place[3] * 32, 32), :].astype(F32) + mixture
    stream_held[...] = stream
    copies = [pltpu.make_async_copy(stream_held, stream_out, sems.at[4])]
    copies[0].start()
    scale = lax.rsqrt(jnp.mean(stream * stream, axis=1, keepdims=True) + EPSILON)
    normed = (stream * scale * gain[...]).astype(BF)
    normed_out[...] = normed
    cut = jnp.concatenate([normed[:, g * 1024 : (g + 1) * 1024] for g in range(4)], axis=0)
    row = lax.broadcasted_iota(jnp.int32, (512, 128), 0)
    for at in range(0, 1024, 512):
        pick = row + at == target[0:1, :]
        for k in range(1, 4):
            pick = pick | (row + at == target[k : k + 1, :])
        rows[at : at + 512, :] = jnp.dot(pick.astype(F32).astype(BF), cut, preferred_element_type=F32).astype(BF)
        part = pl.ds(at, 512)
        copies.append(pltpu.make_async_copy(rows.at[part], out.at[part], sems.at[at // 512]))
        copies[-1].start()
    for copy in copies:
        copy.wait()


def fetch(pairs, sems):
    copies = [pltpu.make_async_copy(ref, held, sems.at[i]) for i, (ref, held) in enumerate(pairs)]
    for copy in copies:
        copy.start()
    return copies


def silu(v):
    return v / (1.0 + jnp.exp(-v))


def shared_kernel(n0, n1, n2, n3, gate_hbm, up_hbm, down_hbm, o0, o1, o2, o3, x, gate, up, down, sems):
    pairs = [(n, x.at[pl.ds(k * 32, 32)]) for k, n in enumerate((n0, n1, n2, n3))]
    fetched = fetch(pairs + [(gate_hbm, gate), (up_hbm, up), (down_hbm, down)], sems)
    for copy in fetched[:5]:
        copy.wait()
    x = x[...]
    g = jnp.dot(x, gate[...], preferred_element_type=F32)
    fetched[5].wait()
    u = jnp.dot(x, up[...], preferred_element_type=F32)
    fetched[6].wait()
    hidden = (silu(g) * u).astype(BF)
    for at in range(0, 4096, 1024):
        part = jnp.dot(hidden, down[:, at : at + 1024], preferred_element_type=F32).astype(BF)
        for k, out in enumerate((o0, o1, o2, o3)):
            out[:, at : at + 1024] = part[k * 32 : (k + 1) * 32]


def expert_kernel(inbound, gate_hbm, up_hbm, down_hbm, out, x, rows_out, gate, up, down, weight_sems, sems):
    pairs = []
    for g in range(4):
        part = pl.ds(g * 1024, 1024)
        pairs += [(ref.at[0, part], held.at[part]) for ref, held in ((gate_hbm, gate), (up_hbm, up))]
    fetched = fetch(pairs + [(down_hbm.at[0], down)], weight_sems)
    i = lax.broadcasted_iota(jnp.int32, (256, 256), 0)
    j = lax.broadcasted_iota(jnp.int32, (256, 256), 1)
    order = (j == ((i % 64) // 2) * 8 + (i % 2) * 4 + i // 64).astype(F32).astype(BF)
    back = (i == ((j % 64) // 2) * 8 + (j % 2) * 4 + j // 64).astype(F32).astype(BF)
    for b in range(4):
        rows = jnp.dot(order, inbound[b * 256 : (b + 1) * 256, :], preferred_element_type=F32).astype(BF)
        for g in range(4):
            x[b * 64 : (b + 1) * 64, g * 1024 : (g + 1) * 1024] = rows[g * 64 : (g + 1) * 64]
    gated, upped = jnp.zeros((256, 256), F32), jnp.zeros((256, 256), F32)
    for g in range(4):
        lo, hi = g * 1024, (g + 1) * 1024
        fetched[2 * g].wait()
        fetched[2 * g + 1].wait()
        gated = gated + jnp.dot(x[:, lo:hi], gate[lo:hi], preferred_element_type=F32)
        upped = upped + jnp.dot(x[:, lo:hi], up[lo:hi], preferred_element_type=F32)
    fetched[8].wait()
    hidden = (silu(gated) * upped).astype(BF)
    for g in range(4):
        part = jnp.dot(hidden, down[:, g * 1024 : (g + 1) * 1024], preferred_element_type=F32)
        x[:, g * 1024 : (g + 1) * 1024] = part.astype(BF)
    copies = []
    for b in range(4):
        rows = jnp.concatenate([x[b * 64 : (b + 1) * 64, g * 1024 : (g + 1) * 1024] for g in range(4)], axis=0)
        part = pl.ds(b * 256, 256)
        rows_out[part, :] = jnp.dot(back, rows, preferred_element_type=F32).astype(BF)
        copies.append(pltpu.make_async_copy(rows_out.at[part], out.at[part], sems.at[b]))
        copies[-1].start()
    for copy in copies:
        copy.wait()


def fold_kernel(stream_hbm, s0, s1, s2, s3, out, stream, shared, sems):
    pairs = [(s, shared.at[k]) for k, s in enumerate((s0, s1, s2, s3))]
    fetched = fetch([(stream_hbm, stream)] + pairs, sems)
    for copy in fetched:
        copy.wait()
    total = stream[...]
    for k in range(4):
        total = total + shared[k].astype(F32)
    out[...] = total


def combine_kernel(returned, mix, base, out):
    routed = jnp.dot(mix[...], returned[...], preferred_element_type=F32)
    for g in range(4):
        lo, hi = g * 1024, (g + 1) * 1024
        out[:, lo:hi] = (base[:, lo:hi] + routed[g * 32 : (g + 1) * 32]).astype(BF)


def attend_kernel(counts, first, last, *refs):
    at = 0

    def take(n):
        nonlocal at
        at += n
        return refs[at - n : at]

    q_own, q_other, core = take(3)
    tiles, planes = [], []
    for n, own_block in counts:
        tiles.append((take(n), take(1)[0], own_block))
        if first and not own_block:
            planes.append(tiles[-1][0][0])
    if not first:
        m_in, l_in, an_in, ab_in = take(4)
    if last:
        own_out, send_out = take(2)
    else:
        m_out, l_out, an_out, ab_out = take(4)

    def keys(ref, lo, hi):
        value = ref[1, :, lo:hi] if any(ref is p for p in planes) else ref[..., lo:hi]
        return value.reshape(-1, hi - lo)

    results = {}
    for group, size, heads, lo, per in (("n", NARROW_SIZE, 4, 0, 4 if first else 2), ("b", BROAD_SIZE, 2, 256, 2)):
        count = per * 128
        scale = size**-0.5 * LOG2E
        base = 0 if group == "n" else 4
        row_base = 0 if group == "n" else 1024
        loaded = []
        for arrays, bias, own_block in tiles:
            k = jnp.concatenate([keys(r, lo, lo + size) for r in arrays], axis=0)
            v = jnp.concatenate([keys(r, lo + size, lo + 2 * size) for r in arrays], axis=0)
            loaded.append((k, v, bias, own_block))
        for side, q_ref in ((0, q_own), (1, q_other)):
            for h0 in range(0, heads, per):
                col = (0 if group == "n" else 512) + h0 * size
                q = jnp.concatenate([q_ref[:, col + i * size : col + (i + 1) * size] for i in range(per)], axis=0)
                rows = row_base + side * heads * 128 + h0 * 128
                arow = rows - row_base
                scores = []
                for k, v, bias, own_block in loaded:
                    s = lax.dot_general(q, k, (((1,), (1,)), ((), ())), preferred_element_type=F32) * scale
                    n = k.shape[0]
                    b = bias[base + h0 : base + h0 + per, :]
                    s = (s.reshape(per, 128, n) + b[:, None, :]).reshape(count, n)
                    if own_block:
                        qi = lax.broadcasted_iota(jnp.int32, (count, n), 0) % 128
                        ki = lax.broadcasted_iota(jnp.int32, (count, n), 1)
                        offset = 0 if side == 0 else 128 * (1 - 2 * core[0])
                        s = jnp.where(ki <= qi + offset, s, MASKED)
                    scores.append(s)
                m = functools.reduce(jnp.maximum, [jnp.max(s, axis=1, keepdims=True) for s in scores])
                if not first:
                    m_old = m_in[pl.ds(rows, count), :][:, :1]
                    m = jnp.maximum(m, m_old)
                l = jnp.zeros((count, 1), F32)
                acc = jnp.zeros((count, size), F32)
                for s, (k, v, bias, own_block) in zip(scores, loaded):
                    p = jnp.exp2(s - m)
                    l = l + jnp.sum(p, axis=1, keepdims=True)
                    acc = acc + jnp.dot(p.astype(BF), v, preferred_element_type=F32)
                if not first:
                    a_in = an_in if group == "n" else ab_in
                    factor = jnp.exp2(m_old - m)
                    l = l + l_in[pl.ds(rows, count), :][:, :1] * factor
                    acc = acc + a_in[pl.ds(arow, count), :] * factor
                if last:
                    out = own_out if side == 0 else send_out
                    o = acc / l
                    lse = m + jnp.log2(l)
                    for i in range(per):
                        out[:, col + i * size : col + (i + 1) * size] = o[i * 128 : (i + 1) * 128].astype(out.dtype)
                        results[(side, base + h0 + i)] = lse[i * 128 : (i + 1) * 128]
                else:
                    a_out = an_out if group == "n" else ab_out
                    m_out[pl.ds(rows, count), :] = jnp.broadcast_to(m, (count, 128))
                    l_out[pl.ds(rows, count), :] = jnp.broadcast_to(l, (count, 128))
                    a_out[pl.ds(arow, count), :] = acc
    if last:
        lane = lax.broadcasted_iota(jnp.int32, (128, 128), 1)
        for side, out in ((0, own_out), (1, send_out)):
            stats = jnp.zeros((128, 128), F32)
            for h in range(6):
                stats = jnp.where(lane % 8 == h, results[(side, h)], stats)
            if side == 1:
                high = stats.astype(BF).astype(F32)
                middle = (stats - high).astype(BF).astype(F32)
                stats = jnp.where(lane < 8, high, jnp.where(lane < 16, middle, stats - high - middle))
            out[:, 1024:1152] = stats.astype(out.dtype)


def attend(q_own, q_other, core, tiles, state, last):
    counts = tuple((len(arrays), own_block) for arrays, _, own_block in tiles)
    operands = [q_own, q_other, core]
    n_keys = 0
    for arrays, bias, _ in tiles:
        operands += list(arrays) + [bias]
        n_keys += bias.shape[1]
    specs = [VMEM] * len(operands)
    specs[2] = SMEM
    if state is not None:
        operands += list(state)
        specs += [VMEM] * 4
    if last:
        shapes = [jax.ShapeDtypeStruct((128, 1152), F32), jax.ShapeDtypeStruct((128, 1152), BF)]
    else:
        shapes = [
            jax.ShapeDtypeStruct((1536, 128), F32),
            jax.ShapeDtypeStruct((1536, 128), F32),
            jax.ShapeDtypeStruct((1024, 128), F32),
            jax.ShapeDtypeStruct((512, 256), F32),
        ]
    return pl.pallas_call(
        functools.partial(attend_kernel, counts, state is None, last),
        out_shape=shapes,
        in_specs=specs,
        out_specs=[VMEM] * len(shapes),
        compiler_params=pltpu.CompilerParams(vmem_limit_bytes=24 * 1024 * 1024),
        cost_estimate=pl.CostEstimate(
            flops=4 * n_keys * 256 * 1024, transcendentals=n_keys * 1536, bytes_accessed=4 * 1024 * 1024
        ),
    )(*operands)


def local(
    query_narrow,
    key_narrow,
    value_narrow,
    gates_narrow,
    query_broad,
    key_broad,
    value_broad,
    gates_broad,
    project_narrow,
    project_broad,
    residual,
    norm_gain,
    route_ids,
    route_weight,
    expert_gate,
    expert_up,
    expert_down,
    shared_gate,
    shared_up,
    shared_down,
):
    z, y, c, t = (lax.axis_index(n).astype(jnp.int32) for n in ("z", "y", "c", "tp"))

    own_kv, q_own = call(
        pack_kernel,
        (key_narrow, value_narrow, key_broad, value_broad, query_narrow, query_broad),
        [shaped((128, 768), BF), shaped((128, 1024), BF)],
        hbm=range(6),
        scratch=[pltpu.SemaphoreType.DMA((6,))],
        moved=0,
    )
    place = jnp.stack([z, y, c, t])
    q_other = swap_core(q_own)
    line = {}
    for k in (2, 1, 3):
        line[k] = turn(own_kv, k, 0)
    target, mix, own_bias, bias_1, bias_2, bias_3, bias_4 = call(
        tables_kernel,
        (place, route_ids.T, route_weight.T, gates_narrow.T, gates_broad.T),
        [shaped((4, 128), jnp.int32), shaped((128, 1024), BF)] + [shaped((8, n), F32) for n in (128, 384, 512, 512, 512)],
        smem=(0,),
        hbm=(1, 2, 3, 4),
        scratch=[
            pltpu.VMEM((4, 32), jnp.int32),
            pltpu.VMEM((4, 32), F32),
            pltpu.VMEM((4, 4096), F32),
            pltpu.VMEM((2, 4096), F32),
            pltpu.SemaphoreType.DMA((4,)),
        ],
    )
    low, high = call(
        stack_kernel,
        [own_kv] + [line[k] for k in ORDER[1:]] + [target, own_bias],
        [shaped((2, 128, 768), BF)] * 2,
    )
    low_back = turn(low, 1, 1)
    high_ahead = turn(high, 3, 1)
    low_ahead = turn(low, 3, 1)
    high_back = turn(high, 1, 1)
    low_far = turn(low_back, 1, 1)
    high_far = turn(high_ahead, 3, 1)

    core = c.reshape(1)
    first_tiles = [((own_kv,), own_bias, True), ((low, high), bias_1, False)]
    state = attend(q_own, q_other, core, first_tiles, None, False)
    state = attend(q_own, q_other, core, [((low_back, high_ahead), bias_2, False)], state, False)
    state = attend(q_own, q_other, core, [((low_ahead, high_back), bias_3, False)], state, False)
    own_part, send_part = attend(q_own, q_other, core, [((low_far, high_far), bias_4, False)], state, True)
    other_part = swap_core(send_part)

    p0, p1, p2, p3 = call(
        project_kernel,
        (place, own_part, other_part, project_narrow, project_broad),
        [shaped((32, 4096), BF)] * 4,
        smem=(0,),
        scratch=[pltpu.VMEM((128, 4096), F32), pltpu.VMEM((128, 1024), BF)],
        flops=2 * 128 * 1024 * 4096,
    )
    p2 = shift(p2, "tp", 2)
    p1 = shift(p1, "tp", 1)
    p3 = shift(p3, "tp", 3)

    stream, normed, outbound = call(
        dispatch_kernel,
        (place, p0, p1, p2, p3, residual, norm_gain.reshape(1, -1), target),
        [pltpu.HBM((32, 4096), F32), shaped((32, 4096), BF), pltpu.HBM((1024, 1024), BF)],
        smem=(0,),
        hbm_out=(0, 2),
        scratch=[pltpu.VMEM((32, 4096), F32), pltpu.VMEM((1024, 1024), BF), pltpu.SemaphoreType.DMA((5,))],
        flops=2 * 1024 * 128 * 1024,
    )
    every = SP + ("tp",)
    inbound = lax.all_to_all(outbound.reshape(128, 8, 1024), every, 0, 0, tiled=True)

    n1 = shift(normed, "tp", 1)
    n2 = shift(normed, "tp", 2)
    n3 = shift(normed, "tp", 3)
    s0, s1, s2, s3 = call(
        shared_kernel,
        (normed, n1, n2, n3, shared_gate, shared_up, shared_down),
        [shaped((32, 4096), BF)] * 4,
        hbm=range(7),
        scratch=[
            pltpu.VMEM((128, 4096), BF),
            pltpu.VMEM((4096, 256), BF),
            pltpu.VMEM((4096, 256), BF),
            pltpu.VMEM((256, 4096), BF),
            pltpu.SemaphoreType.DMA((7,)),
        ],
        mib=20,
        flops=2 * 128 * 4096 * 768,
    )
    s1 = shift(s1, "tp", 3)
    s2 = shift(s2, "tp", 2)
    s3 = shift(s3, "tp", 1)

    (result,) = call(
        expert_kernel,
        (inbound.reshape(1024, 1024), expert_gate, expert_up, expert_down),
        [pltpu.HBM((1024, 1024), BF)],
        hbm=(1, 2, 3),
        hbm_out=(0,),
        scratch=[
            pltpu.VMEM((256, 4096), BF),
            pltpu.VMEM((1024, 1024), BF),
            pltpu.VMEM((4096, 256), BF),
            pltpu.VMEM((4096, 256), BF),
            pltpu.VMEM((256, 4096), BF),
            pltpu.SemaphoreType.DMA((9,)),
            pltpu.SemaphoreType.DMA((4,)),
        ],
        mib=20,
        flops=2 * 256 * 4096 * 768,
    )
    returned = lax.all_to_all(result.reshape(128, 8, 1024), every, 0, 0, tiled=True)
    (base,) = call(
        fold_kernel,
        (stream, s0, s1, s2, s3),
        [shaped((32, 4096), F32)],
        hbm=range(5),
        scratch=[pltpu.VMEM((32, 4096), F32), pltpu.VMEM((4, 32, 4096), BF), pltpu.SemaphoreType.DMA((5,))],
    )
    (out,) = call(
        combine_kernel,
        (returned.reshape(1024, 1024), mix, base),
        [shaped((32, 4096), BF)],
        flops=2 * 128 * 1024 * 1024,
    )
    return out


def solution(mesh):
    mesh = Mesh(mesh.devices.reshape(4, 4, 2, 4), ("z", "y", "c", "tp"))
    every = SP + ("tp",)
    placed = (
        P(SP, "tp"),
        P(SP, "tp"),
        P(SP, "tp"),
        P(None, "tp"),
        P(SP, "tp"),
        P(SP, "tp"),
        P(SP, "tp"),
        P(None, "tp"),
        P("tp", None),
        P("tp", None),
        P(SP, None),
        P(),
        P(every, None),
        P(every, None),
        P(every, None, None),
        P(every, None, None),
        P(every, None, None),
        P(None, "tp"),
        P(None, "tp"),
        P("tp", None),
    )

    return jax.shard_map(local, mesh=mesh, in_specs=placed, out_specs=P(every, None), check_vma=False)
```
